32 devices in a mesh: grp: 2 (over y), ep: 4 (over z), tp: 4 (over x, core).
Axes of the slice: x: 2, y: 2, z: 4, core: 2. Of those that a mesh axis runs over, the one named last changes fastest.
Arguments:
- query_rows: bfloat16 [1536, 2048], P(('grp', 'ep'), 'tp'), parts along dimension 0, may hold values from -100 to 100
- projected_keys: bfloat16 [1536, 512], P(('grp', 'ep'), 'tp'), parts along dimension 0, may hold values from -100 to 100
- projected_values: bfloat16 [1536, 512], P(('grp', 'ep'), 'tp'), parts along dimension 0, may hold values from -6 to 6
- query_gain: float32 [128], replicated, may hold values from 0.3 to 6.5
- key_norm_gain: float32 [128], replicated, may hold values from 0.3 to 6.5
- out_proj: bfloat16 [2048, 2048], P('tp'), may hold values from -4 to 4
- mix_tokens: bfloat16 [4096, 2048], P(('grp', 'ep', 'tp')), parts along dimension 0, may hold values from -150 to 150
- norm_gain: float32 [2048], replicated, may hold values from 0.1 to 1.9
- expert_ids: int32 [4096, 2], P(('grp', 'ep', 'tp')), parts along dimension 0, may hold values from 0 to 3, all different within a row; in each aligned block of 128 rows (0 to 127, 128 to 255, ...) at most 96 rows name the same one
- expert_score: float32 [4096, 2], P(('grp', 'ep', 'tp')), parts along dimension 0, may hold values from -6 to 6
- gate_proj: bfloat16 [4, 2048, 2048], P('ep', None, 'tp'), may hold values from -0.125 to 0.125
- up_proj: bfloat16 [4, 2048, 2048], P('ep', None, 'tp'), may hold values from -0.125 to 0.125
- down_proj: bfloat16 [4, 2048, 2048], P('ep', 'tp'), may hold values from -0.125 to 0.125
Outputs:
- mixed_rows: bfloat16 [1536, 2048], P(('grp', 'ep', 'tp')), parts along dimension 0
- expert_out: bfloat16 [4096, 2048], P(('grp', 'ep', 'tp')), parts along dimension 0
The draws below stay inside these ranges and needn't reach their ends.
There are 2 independent parts, one for each index of `grp`. The reference program is written for one: setup_inputs(seed, part) draws one part's arguments, and reference() takes and returns one part's arrays. A program takes and returns all parts, laid end to end along the dimension named above; an argument that names none is the same for every part. Nothing has to cross between parts.
Inputs may be any that keep to these rules, and one draw needn't show every extreme that they name: `expert_ids`: each row names 2 different experts. Within the rows of one device (aligned blocks of 128 rows) no expert is named more than 96 times, and in every draw some device names some expert exactly 96 times.
All inputs are finite; a program needn't handle non-finite values.
Results may differ from the reference program's by a relative error of at most 0.014.
The reference program's roundings to bfloat16 on the way count: a program that leaves them out, or rounds other values in their place, can miss the bound.
Values may be sent and summed in bfloat16 or wider, within the bound.
A program may use at most 128 MiB of HBM per device.

```python
import math
import jax
import jax.numpy as jnp
import numpy as np
from jax import lax

D = 2048
HEAD_SIZE = 128
QUERY_HEADS = 16
KEY_VALUE_HEADS = 4
GRID_W = 64
FFE = 2048
TOPK = 2
TOK_B_DEV = 128
EXPERTS = 4
ATTENTION_TOKENS = 768
TOKENS_B = 2048
CAP = 96
N_TP = 4


def attention_pair(key):
    folded = jax.random.fold_in(key, 11)
    keys_by_head = jax.random.split(folded, 4)
    query_matrix = jnp.clip(jax.random.normal(keys_by_head[0], (ATTENTION_TOKENS, QUERY_HEADS, HEAD_SIZE), jnp.float32), -5.0, 5.0)
    query_matrix = query_matrix * jnp.exp(jax.random.uniform(keys_by_head[1], (ATTENTION_TOKENS, QUERY_HEADS, 1), jnp.float32) * math.log(10.0))
    key_value_pairs = jnp.clip(jax.random.normal(keys_by_head[2], (ATTENTION_TOKENS, KEY_VALUE_HEADS, HEAD_SIZE), jnp.float32), -5.0, 5.0)
    key_value_pairs = key_value_pairs * jnp.exp(jax.random.uniform(keys_by_head[3], (ATTENTION_TOKENS, KEY_VALUE_HEADS, 1), jnp.float32) * math.log(10.0))
    query_matrix = jnp.clip(query_matrix, -100.0, 100.0).reshape(ATTENTION_TOKENS, QUERY_HEADS * HEAD_SIZE)
    key_value_pairs = jnp.clip(key_value_pairs, -100.0, 100.0).reshape(ATTENTION_TOKENS, KEY_VALUE_HEADS * HEAD_SIZE)
    return (query_matrix, key_value_pairs)


def draw_query_rows(key, part):
    return attention_pair(key)[0].astype(jnp.bfloat16)


def draw_projected_keys(key, part):
    return attention_pair(key)[1].astype(jnp.bfloat16)


def gain_draw(key):
    return jnp.clip(1.0 + 0.18 * jax.random.normal(key, (HEAD_SIZE,), jnp.float32), 0.3, 1.9)


def draw_query_gain(key, part):
    return gain_draw(jax.random.fold_in(key, 21))


def draw_key_norm_gain(key, part):
    return gain_draw(jax.random.fold_in(key, 22))


def draw_mix_tokens(key, part):
    keys_by_head = jax.random.split(jax.random.fold_in(key, 31), 3)
    row_scale = jnp.exp(jax.random.uniform(keys_by_head[1], (TOKENS_B, 1), jnp.float32) * math.log(10.0))
    col_scale = jnp.exp(jax.random.uniform(keys_by_head[2], (1, D), jnp.float32, math.log(0.3), math.log(3.0)))
    entries = jnp.clip(jax.random.normal(keys_by_head[0], (TOKENS_B, D), jnp.float32), -5.0, 5.0)
    return jnp.clip(entries * row_scale * col_scale, -150.0, 150.0).astype(jnp.bfloat16)


def level_of(stream_key, shape, shards, low, largest):
    level, own = 1.0, jax.random.fold_in(stream_key, 6)
    for axis_at, parts in shards:
        draws = jnp.exp(jax.random.uniform(jax.random.fold_in(own, axis_at), (parts,), jnp.float32, low / len(shards), largest / len(shards)))
        level = level * jnp.repeat(draws, shape[axis_at] // parts).reshape([-1 if axis == axis_at else 1 for axis in range(len(shape))])
    return level


def routed_block(stream_key, own, number, rows, count, top, most, lean):
    order = jax.random.permutation(stream_key, count)
    packed, usual = shares(count, rows * top, most, lean, True), shares(count, rows * top, most, lean, False)
    places = jnp.arange(count)

    def named(sizes, rotation):
        used = int((sizes > 0).sum())
        fixed = max(1, used // 4)
        moved = fixed + (places - fixed + rotation * (used - fixed)) % max(1, count - fixed)
        return jnp.zeros((count,), jnp.int32).at[order[jnp.where(places < fixed, places, moved)]].set(jnp.asarray(sizes, jnp.int32))

    sizes = jnp.where(number % 4 == 0, named(packed, number // 4), named(usual, number - number // 4 - 1))
    mixed = jax.random.permutation(jax.random.fold_in(own, 3), count)
    source_of, sink = mixed[0:count // 2 * 2:2], mixed[1:count // 2 * 2:2]
    room = jnp.minimum(sizes[source_of] - 1, most - sizes[sink]) // 2
    room = jnp.where((source_of == order[0]) | (sink == order[0]) | (sizes[sink] == 0), 0, jnp.maximum(room, 0))
    moved = jax.random.randint(jax.random.fold_in(own, 4), (count // 2,), 0, 1 << 20) % (room + 1)
    sizes = sizes.at[source_of].add(-moved).at[sink].add(moved)
    labels = jnp.searchsorted(jnp.cumsum(sizes), jnp.arange(rows * top), side="right").astype(jnp.int32)
    listing = labels.reshape(top, rows).T
    listing = listing[jax.random.permutation(jax.random.fold_in(own, 1), rows)]
    rotation = jax.random.randint(jax.random.fold_in(own, 2), (rows, 1), 0, top)
    return jnp.take_along_axis(listing, (jnp.arange(top)[None, :] + rotation) % top, axis=1)


def shares(amount, total, reach, slope, full):
    loads = [(1 << 20) // math.isqrt(rank ** slope) + 1 for rank in range(1, amount + 1)]
    largest = reach if full else min(reach, max(-(-total // amount), total * loads[0] // sum(loads)))
    least = 1 if total - largest >= amount - 1 else 0
    given, rest = [largest] + [least] * (amount - 1), total - largest - least * (amount - 1)
    while rest > 0:
        candidates = [i for i in range(1, amount) if given[i] < largest] or [i for i in range(1, amount) if given[i] < reach]
        pool, remaining = sum([loads[i] for i in candidates]), rest
        for i in candidates:
            extra = min(reach - given[i], max(1, remaining * loads[i] // pool), rest)
            given[i] = given[i] + extra
            rest = rest - extra
    return np.array(given)


def gaussian(stream_key, dims, deviation, bound, cuts=(), kind=jnp.bfloat16):
    result = deviation * jax.random.normal(stream_key, dims, jnp.float32)
    if cuts:
        result = result * level_of(stream_key, dims, cuts, -0.22, 0.18)
    return jnp.clip(result, -bound, bound).astype(kind)


def setup_inputs(seed: int = 0, part: int = 0) -> dict:
    keys = jax.random.split(jax.random.key(seed), 14)
    part_splits = jax.random.split(jax.random.fold_in(keys[13], part), 14)
    query_rows = draw_query_rows(jax.random.fold_in(jax.random.fold_in(keys[13], part), 71), part)
    projected_keys = draw_projected_keys(jax.random.fold_in(jax.random.fold_in(keys[13], part), 71), part)
    projected_values = gaussian(part_splits[2], (ATTENTION_TOKENS, KEY_VALUE_HEADS * HEAD_SIZE), 1.0, 6.0, ((0, 4), (1, 4)))
    query_gain = draw_query_gain(jax.random.fold_in(keys[13], 71), part)
    key_norm_gain = draw_key_norm_gain(jax.random.fold_in(keys[13], 71), part)
    out_proj = gaussian(keys[5], (QUERY_HEADS * HEAD_SIZE, D), (max(1, QUERY_HEADS * HEAD_SIZE // 1024)) ** -0.5, 4.0, ((0, 4),))
    mix_tokens = draw_mix_tokens(jax.random.fold_in(jax.random.fold_in(keys[13], part), 71), part)
    norm_gain = jnp.clip(1.0 + 0.18 * jax.random.normal(keys[7], (D,), jnp.float32), 0.1, 1.9)
    expert_ids_keys = jax.random.split(jax.random.fold_in(part_splits[8], 1), TOKENS_B // TOK_B_DEV)
    expert_ids_turns = jax.random.permutation(jax.random.fold_in(part_splits[8], 3), TOKENS_B // TOK_B_DEV)
    expert_ids = jax.vmap(lambda own, number: routed_block(jax.random.fold_in(part_splits[8], 2), own, number, TOK_B_DEV, EXPERTS, TOPK, CAP, 2))(expert_ids_keys, expert_ids_turns).reshape((TOKENS_B, TOPK))
    expert_score = gaussian(part_splits[9], (TOKENS_B, TOPK), 1.5, 6.0, ((0, 16),), jnp.float32)
    gate_proj = gaussian(keys[10], (EXPERTS, D, FFE), D ** -0.5, 0.125, ((0, 4), (2, 4)))
    up_proj = gaussian(keys[11], (EXPERTS, D, FFE), D ** -0.5, 0.125, ((0, 4), (2, 4)))
    down_proj = gaussian(keys[12], (EXPERTS, FFE, D), FFE ** -0.5, 0.125, ((0, 4), (1, 4)))
    return {"query_rows": query_rows, "projected_keys": projected_keys, "projected_values": projected_values, "query_gain": query_gain, "key_norm_gain": key_norm_gain, "out_proj": out_proj, "mix_tokens": mix_tokens, "norm_gain": norm_gain, "expert_ids": expert_ids, "expert_score": expert_score, "gate_proj": gate_proj, "up_proj": up_proj, "down_proj": down_proj}


EPS = 1e-06
THETA = 10000.0

def head_norm(vectors, gain):
    return vectors * lax.rsqrt(lax.optimization_barrier(jnp.mean(vectors * vectors, axis=-1, keepdims=True)) + EPS) * gain

def rotate_grid(vectors, token_positions):
    length, heads, head_dim = vectors.shape
    quarter = head_dim // 4
    freqs = 1.0 / THETA ** (jnp.arange(quarter, dtype=jnp.float32) * 4.0 / head_dim)
    grid_row = (token_positions // GRID_W).astype(jnp.float32)
    grid_col = (token_positions % GRID_W).astype(jnp.float32)
    angles = jnp.stack([grid_row[:, None] * freqs, grid_col[:, None] * freqs], axis=1)
    cosine = jnp.cos(angles)[:, None]
    sine = jnp.sin(angles)[:, None]
    halves = vectors.reshape(length, heads, 2, 2, quarter)
    first = halves[..., 0, :]
    second = halves[..., 1, :]
    turned = jnp.stack([first * cosine - second * sine, second * cosine + first * sine], axis=-2)
    return turned.reshape(length, heads, head_dim)

def prepare_inputs(raw_rows, gain, heads, token_positions):
    length = raw_rows.shape[0]
    vectors = raw_rows.astype(jnp.float32).reshape(length, heads, HEAD_SIZE)
    return rotate_grid(head_norm(vectors, gain), token_positions).astype(jnp.bfloat16)

def reference(query_rows, projected_keys, projected_values, query_gain, key_norm_gain, out_proj, mix_tokens, norm_gain, expert_ids, expert_score, gate_proj, up_proj, down_proj):
    token_total = query_rows.shape[0]
    token_positions = jnp.arange(token_total, dtype=jnp.int32)
    queries_per_group = QUERY_HEADS // KEY_VALUE_HEADS
    query_matrix = prepare_inputs(query_rows, query_gain, QUERY_HEADS, token_positions)
    keys_expanded = prepare_inputs(projected_keys, key_norm_gain, KEY_VALUE_HEADS, token_positions).astype(jnp.float32)
    values_expanded = projected_values.reshape(token_total, KEY_VALUE_HEADS, HEAD_SIZE).astype(jnp.float32)
    rows_per_block = math.gcd(token_total, 256)
    blocked_queries = query_matrix.reshape(token_total // rows_per_block, rows_per_block, KEY_VALUE_HEADS, queries_per_group, HEAD_SIZE)

    def attend(query_block):
        scores = jnp.einsum('tkgd,skd->kgts', query_block.astype(jnp.float32), keys_expanded) * HEAD_SIZE ** (-0.5)
        top_score = lax.optimization_barrier(jnp.max(scores, axis=-1, keepdims=True))
        probs = jnp.exp(scores - top_score)
        prob_total = lax.optimization_barrier(jnp.sum(probs, axis=-1))
        rounded = lax.optimization_barrier(probs.astype(jnp.bfloat16)).astype(jnp.float32)
        summed = jnp.einsum('kgts,skd->tkgd', rounded, values_expanded)
        return (summed / jnp.transpose(prob_total, (2, 0, 1))[..., None]).astype(jnp.bfloat16)
    heads_out = lax.map(attend, blocked_queries).reshape(token_total, QUERY_HEADS * HEAD_SIZE)
    group_width = QUERY_HEADS * HEAD_SIZE // N_TP
    mixed = jnp.zeros((token_total, D), jnp.float32)
    for group_index in range(N_TP):
        lower = group_index * group_width
        partial_value = jnp.dot(heads_out[:, lower:lower + group_width], out_proj[lower:lower + group_width], preferred_element_type=jnp.float32)
        mixed = mixed + lax.optimization_barrier(partial_value.astype(jnp.bfloat16)).astype(jnp.float32)
    mixed_rows = mixed.astype(jnp.bfloat16)
    count_b = mix_tokens.shape[0]
    blocks = count_b // TOK_B_DEV
    values_b = mix_tokens.astype(jnp.float32)
    normed = (values_b * lax.rsqrt(lax.optimization_barrier(jnp.mean(values_b * values_b, axis=-1, keepdims=True)) + EPS) * norm_gain).astype(jnp.bfloat16)
    flat = expert_ids.reshape(blocks, TOK_B_DEV * TOPK)
    onehot = (flat[..., None] == jnp.arange(EXPERTS, dtype=jnp.int32)).astype(jnp.int32)
    slots = lax.optimization_barrier(jnp.sum((jnp.cumsum(onehot, axis=1) - onehot) * onehot, axis=-1))
    owners = jnp.arange(blocks, dtype=jnp.int32)[:, None]
    places = ((flat * blocks + owners) * CAP + slots).reshape(count_b, TOPK).astype(jnp.int32)
    buffer = jnp.zeros((EXPERTS * blocks * CAP, D), jnp.bfloat16)
    for route_slot in range(TOPK):
        buffer = buffer.at[places[:, route_slot]].set(normed)
    stacked = buffer.reshape(EXPERTS, blocks * CAP, D)
    hidden_width = FFE // N_TP

    def run_expert(operands):
        expert_in, gate_w, up_w, down_w = operands
        gate_out = jnp.dot(expert_in, gate_w, preferred_element_type=jnp.float32)
        up_out = jnp.dot(expert_in, up_w, preferred_element_type=jnp.float32)
        active = (jax.nn.silu(gate_out) * up_out).astype(jnp.bfloat16)
        summed = jnp.zeros((expert_in.shape[0], D), jnp.float32)
        for group_index in range(N_TP):
            lower = group_index * hidden_width
            partial_value = jnp.dot(active[:, lower:lower + hidden_width], down_w[lower:lower + hidden_width], preferred_element_type=jnp.float32)
            summed = summed + lax.optimization_barrier(partial_value.astype(jnp.bfloat16)).astype(jnp.float32)
        return summed.astype(jnp.bfloat16)
    results = lax.map(run_expert, (stacked, gate_proj, up_proj, down_proj)).reshape(EXPERTS * blocks * CAP, D)
    first_weight = jax.nn.sigmoid(expert_score[:, 0] - expert_score[:, 1])
    combined = first_weight[:, None] * results[places[:, 0]].astype(jnp.float32) + (1.0 - first_weight)[:, None] * results[places[:, 1]].astype(jnp.float32)
    return (mixed_rows, combined.astype(jnp.bfloat16))
```

```python
import functools
import math

import jax
import jax.numpy as jnp
import numpy as np
from jax import lax
from jax.experimental import pallas as pl
from jax.experimental.pallas import tpu as pltpu
from jax.sharding import PartitionSpec as P

GRID_W = 64


MESH = pl.DeviceIdType.MESH
EPS = 1e-06
THETA = 10000.0


def head_norm(vectors, gain):
    return vectors * lax.rsqrt(jnp.mean(vectors * vectors, axis=-1, keepdims=True) + EPS) * gain


def rotate_grid(vectors, token_positions):
    length, heads, head_dim = vectors.shape
    quarter = head_dim // 4
    freqs = 1.0 / THETA ** (jnp.arange(quarter, dtype=jnp.float32) * 4.0 / head_dim)
    grid_row = (token_positions // GRID_W).astype(jnp.float32)
    grid_col = (token_positions % GRID_W).astype(jnp.float32)
    angles = jnp.stack([grid_row[:, None] * freqs, grid_col[:, None] * freqs], axis=1)
    cosine = jnp.cos(angles)[:, None]
    sine = jnp.sin(angles)[:, None]
    halves = vectors.reshape(length, heads, 2, 2, quarter)
    first = halves[..., 0, :]
    second = halves[..., 1, :]
    turned = jnp.stack([first * cosine - second * sine, second * cosine + first * sine], axis=-2)
    return turned.reshape(length, heads, head_dim)


def prepare_inputs(raw_rows, gain, heads, token_positions):
    length = raw_rows.shape[0]
    head_dim = gain.shape[0]
    vectors = raw_rows.astype(jnp.float32).reshape(length, heads, head_dim)
    return rotate_grid(head_norm(vectors, gain), token_positions).astype(jnp.bfloat16)


def mixer_prepare(query_rows, projected_keys, projected_values, query_gain, key_norm_gain):
    length = query_rows.shape[0]
    head_dim = query_gain.shape[0]
    kv_heads = projected_keys.shape[1] // head_dim
    q_heads = query_rows.shape[1] // head_dim
    token_positions = lax.axis_index("ep") * length + jnp.arange(length, dtype=jnp.int32)
    query_matrix = prepare_inputs(query_rows, query_gain, q_heads, token_positions).reshape(
        length, q_heads * head_dim
    )
    keys_turned = prepare_inputs(projected_keys, key_norm_gain, kv_heads, token_positions).reshape(
        length, kv_heads * head_dim
    )
    return query_matrix, jnp.concatenate([keys_turned, projected_values], axis=1)


def attend_plain(query_matrix, own_pair, head_dim):
    length = query_matrix.shape[0]
    kv_heads = own_pair.shape[1] // (2 * head_dim)
    q_heads = query_matrix.shape[1] // head_dim
    queries_per_group = q_heads // kv_heads
    query_matrix = query_matrix.reshape(length, kv_heads, queries_per_group, head_dim)
    score_scale = head_dim ** (-0.5)
    initial = (
        jnp.full((kv_heads, queries_per_group, length), -1e30, jnp.float32),
        jnp.zeros((kv_heads, queries_per_group, length), jnp.float32),
        jnp.zeros((length, kv_heads, queries_per_group, head_dim), jnp.float32),
    )
    width = kv_heads * head_dim
    pair = lax.all_gather(own_pair, "ep", axis=0, tiled=True)
    key_piece = pair[:, :width]
    value_piece = pair[:, width:]
    piece_rows = key_piece.shape[0]
    step_rows = math.gcd(piece_rows, 1024)

    def one_block(block_index, running):
        run_max, run_sum, run_acc = running
        offset = block_index * step_rows
        key_block = lax.dynamic_slice_in_dim(key_piece, offset, step_rows, 0).reshape(
            step_rows, kv_heads, head_dim
        )
        value_block = lax.dynamic_slice_in_dim(value_piece, offset, step_rows, 0).reshape(
            step_rows, kv_heads, head_dim
        )
        scores = (
            jnp.einsum(
                "tkgd,skd->kgts", query_matrix, key_block, preferred_element_type=jnp.float32
            )
            * score_scale
        )
        new_max = jnp.maximum(run_max, jnp.max(scores, axis=-1))
        factor = jnp.exp(run_max - new_max)
        weights = jnp.exp(scores - new_max[..., None])
        run_sum = run_sum * factor + jnp.sum(weights, axis=-1)
        update = jnp.einsum(
            "kgts,skd->tkgd",
            weights.astype(jnp.bfloat16),
            value_block,
            preferred_element_type=jnp.float32,
        )
        run_acc = run_acc * jnp.transpose(factor, (2, 0, 1))[..., None] + update
        return (new_max, run_sum, run_acc)

    run_max, run_sum, run_acc = lax.fori_loop(0, piece_rows // step_rows, one_block, initial)
    return (
        (run_acc / jnp.transpose(run_sum, (2, 0, 1))[..., None])
        .astype(jnp.bfloat16)
        .reshape(length, q_heads * head_dim)
    )


def flip(index, bits):
    result, place = 0, 1
    for _ in range(8):
        mine = (index // place) % 2
        result = result + place * ((1 - mine) if bits & place else mine)
        place *= 2
    return result


def exchange_plain(outgoing, gate_proj, up_proj, down_proj):
    rows_in = lax.all_gather(
        lax.all_to_all(outgoing, "ep", split_axis=0, concat_axis=0, tiled=True),
        "tp",
        axis=0,
        tiled=True,
    )
    gate_out = jnp.einsum("secd,edf->secf", rows_in, gate_proj, preferred_element_type=jnp.float32)
    up_out = jnp.einsum("secd,edf->secf", rows_in, up_proj, preferred_element_type=jnp.float32)
    active = (jax.nn.silu(gate_out) * up_out).astype(jnp.bfloat16)
    summed = lax.psum_scatter(
        jnp.einsum("secf,efd->secd", active, down_proj, preferred_element_type=jnp.float32).astype(
            jnp.bfloat16
        ),
        "tp",
        scatter_dimension=0,
        tiled=True,
    )
    return lax.all_to_all(summed, "ep", split_axis=0, concat_axis=0, tiled=True)


def plain_halves(
    query_rows,
    projected_keys,
    projected_values,
    query_gain,
    key_norm_gain,
    out_proj,
    mix_tokens,
    norm_gain,
    expert_ids,
    expert_score,
    gate_proj,
    up_proj,
    down_proj,
):
    length, model_dim = mix_tokens.shape
    top_count = expert_ids.shape[1]
    local_experts = gate_proj.shape[0]
    expert_axis = lax.axis_size("ep")
    experts_all = expert_axis * local_experts
    capacity = length * top_count * 3 // (2 * experts_all)
    values_b = mix_tokens.astype(jnp.float32)
    normed = (
        values_b
        * lax.rsqrt(jnp.mean(values_b * values_b, axis=-1, keepdims=True) + EPS)
        * norm_gain
    ).astype(jnp.bfloat16)
    flat = expert_ids.reshape(length * top_count)
    onehot = (flat[:, None] == jnp.arange(experts_all, dtype=jnp.int32)).astype(jnp.int32)
    slots = jnp.sum((jnp.cumsum(onehot, axis=0) - onehot) * onehot, axis=1)
    target = flat * capacity + slots
    placed = (target[:, None] == jnp.arange(experts_all * capacity, dtype=jnp.int32)).astype(
        jnp.int32
    )
    placed = jnp.sum(placed.reshape(length, top_count, experts_all * capacity), axis=1).astype(
        jnp.bfloat16
    )
    outgoing = jnp.einsum("re,rd->ed", placed, normed, preferred_element_type=jnp.float32).astype(
        jnp.bfloat16
    )
    outgoing = outgoing.reshape(expert_axis, local_experts, capacity, model_dim)
    lanes = lax.axis_size("tp")
    head_dim = query_gain.shape[0]
    queries, pair = mixer_prepare(
        query_rows, projected_keys, projected_values, query_gain, key_norm_gain
    )
    heads_out = attend_plain(queries, pair, head_dim)
    returned = exchange_plain(outgoing, gate_proj, up_proj, down_proj)
    head_partial = jnp.dot(heads_out, out_proj, preferred_element_type=jnp.float32).astype(
        jnp.bfloat16
    )
    pieces = lax.all_to_all(
        head_partial.reshape(lanes, -1, head_partial.shape[1]),
        "tp",
        split_axis=0,
        concat_axis=0,
        tiled=True,
    )
    mixed_rows = jnp.sum(pieces.astype(jnp.float32), axis=0).astype(jnp.bfloat16)
    results = returned.reshape(experts_all * capacity, model_dim)
    first_weight = jax.nn.sigmoid(expert_score[:, 0] - expert_score[:, 1])
    picks = target.reshape(length, top_count)
    chosen = [
        jnp.dot(
            (picks[:, k : k + 1] == jnp.arange(experts_all * capacity, dtype=jnp.int32)).astype(
                jnp.bfloat16
            ),
            results,
            preferred_element_type=jnp.float32,
        )
        for k in range(2)
    ]
    combined = first_weight[:, None] * chosen[0] + (1.0 - first_weight)[:, None] * chosen[1]
    return (mixed_rows, combined.astype(jnp.bfloat16))


ORDER = (
    "A10", "A11", "A31", "B31", "B11", "A30", "C31", "KV0",
    "D31", "B00", "A20", "A21", "KV1", "B30", "C00", "C30",
    "D30", "B10", "E31", "KV2", "D00", "B21", "C21", "E30",
    "D21", "B20", "B01", "ATT0", "C10", "C01", "D10", "C20",
    "ATT1", "E00", "E21", "D20", "ATT2", "ATT3", "E10", "D01",
    "C11", "D11", "E20", "E01", "CMB0", "OUTP", "MX0", "E11",
    "CMB2", "CMB3", "MX1", "CMB1",
)
VMEM_LIMIT = 58 * 1024 * 1024
SENDS = ((1, 1), (1, 0), (3, 1), (3, 0), (2, 0), (2, 1))


def fused_kernel(
    steps,
    order,
    tokens_ref,
    ids_ref,
    score_ref,
    ngain_ref,
    gate_hbm,
    up_hbm,
    down_hbm,
    proj_hbm,
    query_hbm,
    key_hbm,
    value_hbm,
    qgain_ref,
    kgain_ref,
    cos_hbm,
    sin_hbm,
    mixed_ref,
    expert_ref,
    gate_ref,
    up_ref,
    down_ref,
    proj_ref,
    query_ref,
    keyraw_ref,
    cos_ref,
    sin_ref,
    tok_ref,
    norm_ref,
    outb,
    rows,
    act,
    part,
    from_core,
    to_x,
    from_x,
    total,
    back,
    acc,
    lut,
    kv,
    heads_ref,
    pm,
    fc,
    to_xm,
    from_xm,
    hsem,
    zs,
    zr,
    xs,
    xr,
    cs,
    cr,
    ps,
    pr,
    qs,
    qr,
    bs,
    br,
    ks,
    kr,
    ms,
    mr,
):
    me = lax.axis_index("ep")
    lane = lax.axis_index("tp")
    peers = [flip(me, k) for k in range(steps)]
    core, across = flip(lane, 1), flip(lane, 2)
    cap, width = outb.shape[1], outb.shape[2]
    half = cap // 2
    hidden = gate_ref.shape[1]
    length = query_ref.shape[0]
    dim = keyraw_ref.shape[1]
    count = tok_ref.shape[0]
    tile = math.gcd(hidden, 256)
    tile_out = math.gcd(width, 512)
    f32, b16 = jnp.float32, jnp.bfloat16

    offset = pl.multiple_of(me * length, 16)
    loads = [
        pltpu.make_async_copy(s, d, hsem.at[i])
        for i, (s, d) in enumerate(
            [
                (tokens_ref, tok_ref),
                (key_hbm, keyraw_ref),
                (value_hbm, kv.at[0, 1]),
                (cos_hbm.at[pl.ds(offset, length)], cos_ref),
                (sin_hbm.at[pl.ds(offset, length)], sin_ref),
                (query_hbm, query_ref),
                (gate_hbm, gate_ref),
                (up_hbm, up_ref),
                (down_hbm, down_ref),
                (proj_hbm, proj_ref),
            ]
        )
    ]
    for load in loads:
        load.start()

    barrier = pltpu.get_barrier_semaphore()
    friends = [{"ep": peers[k], "tp": lane} for k in range(1, steps)]
    friends += [{"ep": me, "tp": core}, {"ep": me, "tp": across}]
    for friend in friends:
        pl.semaphore_signal(barrier, inc=1, device_id=friend, device_id_type=MESH)

    def remote(src, dst, send, recv, ep_to, tp_to):
        return pltpu.make_async_remote_copy(
            src_ref=src,
            dst_ref=dst,
            send_sem=send,
            recv_sem=recv,
            device_id={"ep": ep_to, "tp": tp_to},
            device_id_type=MESH,
        )

    def piece(h):
        return pl.ds(h * half, half)

    units = [(k, h) for k in range(steps) for h in range(2)]
    z_in, x_in, c_in, c_out, x_out, z_out = {}, {}, {}, {}, {}, {}
    for k, h in units:
        n = 2 * k + h
        if k:
            z_in[k, h] = remote(
                outb.at[k, piece(h)], rows.at[k, h, 0], zs.at[n], zr.at[n], peers[k], lane
            )
            z_out[k, h] = remote(
                total.at[k, h], back.at[k, piece(h)], bs.at[n], br.at[n], peers[k], lane
            )
        x_in[k, h] = remote(rows.at[k, h, 0], rows.at[k, h, 1], xs.at[n], xr.at[n], me, across)
        c_in[k, h] = remote(
            rows.at[k, h, pl.ds(0, 2)], rows.at[k, h, pl.ds(2, 2)], cs.at[n], cr.at[n], me, core
        )
        c_out[k, h] = remote(
            part.at[k, h, pl.ds(2, 2)], from_core.at[k, h], ps.at[n], pr.at[n], me, core
        )
        x_out[k, h] = remote(to_x.at[k, h], from_x.at[k, h], qs.at[n], qr.at[n], me, across)
    kv_near = remote(kv.at[0], kv.at[1], ks.at[0], kr.at[0], peers[1], lane)
    kv_mid = remote(kv.at[pl.ds(0, 2)], kv.at[pl.ds(2, 2)], ks.at[1], kr.at[1], peers[3], lane)
    kv_far = remote(kv.at[pl.ds(2, 2)], kv.at[pl.ds(2, 2)], ks.at[2], kr.at[2], peers[1], lane)
    inner = (me == 1) | (me == 2)
    m_core = [
        remote(pm.at[core], fc.at[0], ms.at[0], mr.at[0], me, core),
        remote(pm.at[flip(core, 2)], fc.at[1], ms.at[1], mr.at[1], me, core),
    ]
    m_x = remote(to_xm, from_xm, ms.at[2], mr.at[2], me, across)

    token_row = lax.broadcasted_iota(jnp.int32, (count, count), 0)
    token_col = lax.broadcasted_iota(jnp.int32, (count, count), 1)
    earlier = (token_row < token_col).astype(b16)
    first, second = ids_ref[0:1, :], ids_ref[1:2, :]
    weight = 1.0 / (1.0 + jnp.exp(score_ref[1:2, :] - score_ref[0:1, :]))
    table_row = lax.broadcasted_iota(jnp.int32, (8, count), 0)
    named = jnp.zeros((8, count), f32)
    scale = jnp.zeros((8, count), f32)
    for k in range(steps):
        one, two = first == peers[k], second == peers[k]
        here = jnp.where(one | two, 1.0, 0.0)
        named = jnp.where(table_row == k, here, named)
        value = jnp.where(one, weight, 0.0) + jnp.where(two, 1.0 - weight, 0.0)
        scale = jnp.where(table_row == k, value, scale)
    rank = jnp.dot(named.astype(b16), earlier, preferred_element_type=f32)
    place = jnp.where(named > 0.5, rank, -1.0)
    rest = jnp.zeros((count - 16, count), f32)
    lut[...] = jnp.transpose(jnp.concatenate([place, scale, rest], axis=0))

    loads[0].wait()
    values = tok_ref[...].astype(f32)
    norm_ref[...] = (
        values
        * lax.rsqrt(jnp.mean(values * values, axis=-1, keepdims=True) + EPS)
        * ngain_ref[...]
    ).astype(b16)

    slot = lax.broadcasted_iota(jnp.int32, (cap, count), 0).astype(f32)

    def dispatch(k):
        chosen = (slot == place[k : k + 1, :]).astype(b16)
        picked = jnp.dot(chosen, norm_ref[...], preferred_element_type=f32).astype(b16)
        if k:
            outb[k] = picked
        else:
            rows[0, 0, 0] = picked[:half]
            rows[0, 1, 0] = picked[half:]

    sent = {SENDS[0][0], 0}
    dispatch(SENDS[0][0])
    dispatch(0)
    pl.semaphore_wait(barrier, len(friends))
    z_in[SENDS[0]].start()
    for h in range(2):
        x_in[0, h].start()
    for k, h in SENDS[1:]:
        if k not in sent:
            sent.add(k)
            dispatch(k)
        z_in[k, h].start()

    turn_lane = lax.broadcasted_iota(jnp.int32, (length, dim), 1)
    leading = (turn_lane // (dim // 4)) % 2 == 0

    def turned(raw, gain):
        vectors = raw.astype(f32)
        vectors = (
            vectors
            * lax.rsqrt(jnp.mean(vectors * vectors, axis=-1, keepdims=True) + EPS)
            * gain[...]
        )
        other = jnp.where(
            leading,
            pltpu.roll(vectors, dim - dim // 4, 1),
            pltpu.roll(vectors, dim // 4, 1),
        )
        return (vectors * cos_ref[...] + other * sin_ref[...]).astype(b16)

    def stage_a(k, h):
        z_in[k, h].wait_recv()
        x_in[k, h].start()

    def stage_b(k, h):
        x_in[k, h].wait_recv()
        c_in[k, h].start()

    def stage_c(k, h):
        c_in[k, h].wait_recv()

        @pl.loop(0, hidden // tile)
        def _(i):
            cols = pl.ds(pl.multiple_of(i * tile, tile), tile)
            block = rows[k, h].reshape(4 * half, width)
            gate = jnp.dot(block, gate_ref[:, cols], preferred_element_type=f32)
            up = jnp.dot(block, up_ref[:, cols], preferred_element_type=f32)
            act[:, cols] = (gate / (1.0 + jnp.exp(-gate)) * up).astype(b16)

        @pl.loop(0, width // tile_out)
        def _(i):
            cols = pl.ds(pl.multiple_of(i * tile_out, tile_out), tile_out)
            summed = jnp.dot(act[...], down_ref[:, cols], preferred_element_type=f32)
            part[k, h, :, :, cols] = summed.astype(b16).reshape(4, half, tile_out)

        c_out[k, h].start()

    def stage_d(k, h):
        c_out[k, h].wait_recv()
        to_x[k, h] = (part[k, h, 1].astype(f32) + from_core[k, h, 1].astype(f32)).astype(b16)
        x_out[k, h].start()

    def stage_e(k, h):
        x_out[k, h].wait_recv()
        summed = (
            part[k, h, 0].astype(f32) + from_core[k, h, 0].astype(f32) + from_x[k, h].astype(f32)
        ).astype(b16)
        if k == 0:
            back[0, piece(h)] = summed
        else:
            total[k, h] = summed
            z_out[k, h].start()

    def stage_kv0():
        loads[1].wait()
        loads[2].wait()
        loads[3].wait()
        loads[4].wait()
        kv[0, 0] = turned(keyraw_ref[...], kgain_ref)
        kv_near.start()

    def stage_kv1():
        kv_near.wait_recv()

        @pl.when(inner)
        def _():
            kv_mid.start()

    def stage_kv2():
        @pl.when(inner)
        def _():
            kv_mid.wait_recv()
            kv_far.start()

    def stage_att(head):
        if head == 0:
            loads[5].wait()

            @pl.when(jnp.logical_not(inner))
            def _():
                kv_far.wait_recv()

        cols = slice(head * dim, (head + 1) * dim)
        held = steps * length
        queries = turned(query_ref[:, cols], qgain_ref)
        keys = kv[:, 0].reshape(held, dim)
        scores = (
            lax.dot_general(
                queries, keys, (((1,), (1,)), ((), ())), preferred_element_type=f32
            )
            * dim ** (-0.5)
        )
        probs = jnp.exp(scores - jnp.max(scores, axis=-1, keepdims=True))
        amount = jnp.sum(probs, axis=-1, keepdims=True)
        summed = jnp.dot(
            probs.astype(b16), kv[:, 1].reshape(held, dim), preferred_element_type=f32
        )
        heads_ref[:, cols] = (summed / amount).astype(b16)

    def stage_outp():
        loads[9].wait()

        @pl.loop(0, width // tile_out)
        def _(i):
            cols = pl.ds(pl.multiple_of(i * tile_out, tile_out), tile_out)
            summed = jnp.dot(heads_ref[...], proj_ref[:, cols], preferred_element_type=f32)
            pm[:, :, cols] = summed.astype(b16).reshape(4, length // 4, tile_out)

        for copy in m_core:
            copy.start()

    def stage_mx(step):
        if step == 0:
            for copy in m_core:
                copy.wait_recv()
            to_xm[...] = (pm[across].astype(f32) + fc[1].astype(f32)).astype(b16)
            m_x.start()
        else:
            m_x.wait_recv()
            mixed_ref[...] = (
                pm[lane].astype(f32) + fc[0].astype(f32) + from_xm[...].astype(f32)
            ).astype(b16)

    combined = []

    def stage_cmb(k):
        if k > 0:
            for h in range(2):
                z_out[k, h].wait_recv()
        spot = lax.broadcasted_iota(jnp.int32, (count, cap), 1).astype(f32)
        chosen = (spot == lut[:, k : k + 1]).astype(b16)
        scaled = lut[:, 8 + k : 9 + k]
        opening, closing = not combined, len(combined) == steps - 1
        combined.append(k)

        @pl.loop(0, width // tile_out)
        def _(i):
            cols = pl.ds(pl.multiple_of(i * tile_out, tile_out), tile_out)
            found = scaled * jnp.dot(chosen, back[k, :, cols], preferred_element_type=f32)
            if not opening:
                found = acc[:, cols] + found
            if closing:
                expert_ref[:, cols] = found.astype(b16)
            else:
                acc[:, cols] = found

    stages = {"A": stage_a, "B": stage_b, "C": stage_c, "D": stage_d, "E": stage_e}
    loaded = False
    for name in order:
        if name[0] == "C" and name[1] != "M" and not loaded:
            loaded = True
            for n in (6, 7, 8):
                loads[n].wait()
        if name.startswith("KV"):
            (stage_kv0, stage_kv1, stage_kv2)[int(name[2])]()
        elif name.startswith("ATT"):
            stage_att(int(name[3]))
        elif name == "OUTP":
            stage_outp()
        elif name.startswith("MX"):
            stage_mx(int(name[2]))
        elif name.startswith("CMB"):
            stage_cmb(int(name[3]))
        else:
            stages[name[0]](int(name[1]), int(name[2]))

    for unit in units:
        for table in (z_in, x_in, c_in, c_out, x_out, z_out):
            if unit in table:
                table[unit].wait_send()
    kv_near.wait_send()

    @pl.when(inner)
    def _():
        kv_mid.wait_send()
        kv_far.wait_send()

    for copy in m_core:
        copy.wait_send()
    m_x.wait_send()


def deliver_kernel(mixed_in, expert_in, mixed_out, expert_out, mixed_held, expert_held, sems):
    pairs = []
    for source, held, target, pieces in (
        (expert_in, expert_held, expert_out, 4),
        (mixed_in, mixed_held, mixed_out, 1),
    ):
        size = source.shape[0] // pieces
        for n in range(pieces):
            spot = pl.ds(n * size, size)
            at = len(pairs)
            pairs.append(
                (
                    pltpu.make_async_copy(source.at[spot], held.at[spot], sems.at[0, at]),
                    pltpu.make_async_copy(held.at[spot], target.at[spot], sems.at[1, at]),
                )
            )
    for fetch, _ in pairs:
        fetch.start()
    for fetch, store in pairs:
        fetch.wait()
        store.start()
    for _, store in pairs:
        store.wait()


def turn_tables(held, dim):
    quarter = dim // 4
    freqs = 1.0 / THETA ** (np.arange(quarter) * 4.0 / dim)
    spots = np.arange(held)
    tables = []
    for place in (spots // GRID_W, spots % GRID_W):
        angles = place[:, None] * freqs
        tables.append((np.cos(angles), np.sin(angles)))
    cosine = np.concatenate([tables[0][0]] * 2 + [tables[1][0]] * 2, axis=1)
    sine = np.concatenate(
        [-tables[0][1], tables[0][1], -tables[1][1], tables[1][1]], axis=1
    )
    return jnp.asarray(cosine, jnp.float32), jnp.asarray(sine, jnp.float32)


def fused(
    query_rows,
    projected_keys,
    projected_values,
    query_gain,
    key_norm_gain,
    out_proj,
    mix_tokens,
    norm_gain,
    expert_ids,
    expert_score,
    gate_proj,
    up_proj,
    down_proj,
):
    steps, lanes = lax.axis_size("ep"), lax.axis_size("tp")
    count, width = mix_tokens.shape
    cap = count * expert_ids.shape[1] * 3 // (2 * steps)
    half = cap // 2
    hidden = gate_proj.shape[2]
    length, dim = projected_keys.shape
    kind = jnp.bfloat16
    cosine, sine = turn_tables(steps * length, dim)
    vmem = pl.BlockSpec(memory_space=pltpu.VMEM)
    anywhere = pl.BlockSpec(memory_space=pltpu.HBM)
    units = 2 * steps
    mixed, expert = pl.pallas_call(
        functools.partial(fused_kernel, steps, ORDER),
        out_shape=(
            jax.ShapeDtypeStruct((length // lanes, width), kind),
            jax.ShapeDtypeStruct((count, width), kind),
        ),
        in_specs=[anywhere]
        + [vmem] * 3
        + [anywhere] * 7
        + [vmem] * 2
        + [anywhere] * 2,
        out_specs=(vmem, vmem),
        scratch_shapes=[
            pltpu.VMEM((width, hidden), kind),
            pltpu.VMEM((width, hidden), kind),
            pltpu.VMEM((hidden, width), kind),
            pltpu.VMEM(out_proj.shape, kind),
            pltpu.VMEM(query_rows.shape, kind),
            pltpu.VMEM((length, dim), kind),
            pltpu.VMEM((length, dim), jnp.float32),
            pltpu.VMEM((length, dim), jnp.float32),
            pltpu.VMEM((count, width), kind),
            pltpu.VMEM((count, width), kind),
            pltpu.VMEM((steps, cap, width), kind),
            pltpu.VMEM((steps, 2, 4, half, width), kind),
            pltpu.VMEM((4 * half, hidden), kind),
            pltpu.VMEM((steps, 2, 4, half, width), kind),
            pltpu.VMEM((steps, 2, 2, half, width), kind),
            pltpu.VMEM((steps, 2, half, width), kind),
            pltpu.VMEM((steps, 2, half, width), kind),
            pltpu.VMEM((steps, 2, half, width), kind),
            pltpu.VMEM((steps, cap, width), kind),
            pltpu.VMEM((count, width), jnp.float32),
            pltpu.VMEM((count, count), jnp.float32),
            pltpu.VMEM((steps, 2, length, dim), kind),
            pltpu.VMEM(query_rows.shape, kind),
            pltpu.VMEM((lanes, length // lanes, width), kind),
            pltpu.VMEM((2, length // lanes, width), kind),
            pltpu.VMEM((length // lanes, width), kind),
            pltpu.VMEM((length // lanes, width), kind),
            pltpu.SemaphoreType.DMA((10,)),
        ]
        + [pltpu.SemaphoreType.DMA((units,))] * 12
        + [pltpu.SemaphoreType.DMA((3,))] * 4,
        compiler_params=pltpu.CompilerParams(
            collective_id=0, has_side_effects=True, vmem_limit_bytes=VMEM_LIMIT
        ),
    )(
        mix_tokens,
        expert_ids.T,
        expert_score.T,
        norm_gain.reshape(1, width),
        gate_proj.reshape(gate_proj.shape[1:]),
        up_proj.reshape(up_proj.shape[1:]),
        down_proj.reshape(down_proj.shape[1:]),
        out_proj,
        query_rows,
        projected_keys,
        projected_values,
        query_gain.reshape(1, dim),
        key_norm_gain.reshape(1, dim),
        cosine,
        sine,
    )
    return pl.pallas_call(
        deliver_kernel,
        out_shape=(
            jax.ShapeDtypeStruct(mixed.shape, kind),
            jax.ShapeDtypeStruct(expert.shape, kind),
        ),
        in_specs=[anywhere] * 2,
        out_specs=(anywhere, anywhere),
        scratch_shapes=[
            pltpu.VMEM(mixed.shape, kind),
            pltpu.VMEM(expert.shape, kind),
            pltpu.SemaphoreType.DMA((2, 5)),
        ],
    )(mixed, expert)


def fits_fused(query_rows, projected_keys, query_gain, mix_tokens, expert_ids, gate_proj):
    steps, lanes = lax.axis_size("ep"), lax.axis_size("tp")
    count, width = mix_tokens.shape
    length, dim = projected_keys.shape
    local_experts, _, hidden = gate_proj.shape
    cap = count * expert_ids.shape[1] * 3 // (2 * steps)
    blocks = 20 * steps * cap * width * 2 + 4 * width * hidden * 2
    return (
        lanes == 4
        and steps == 4
        and local_experts == 1
        and expert_ids.shape[1] == 2
        and dim == query_gain.shape[0]
        and dim % 128 == 0
        and length % 64 == 0
        and length <= 256
        and count == 128
        and cap % 32 == 0
        and blocks < 48 * 1024 * 1024
    )


def local(
    query_rows,
    projected_keys,
    projected_values,
    query_gain,
    key_norm_gain,
    out_proj,
    mix_tokens,
    norm_gain,
    expert_ids,
    expert_score,
    gate_proj,
    up_proj,
    down_proj,
):
    simple = fits_fused(
        query_rows, projected_keys, query_gain, mix_tokens, expert_ids, gate_proj
    )
    return (fused if simple else plain_halves)(
        query_rows,
        projected_keys,
        projected_values,
        query_gain,
        key_norm_gain,
        out_proj,
        mix_tokens,
        norm_gain,
        expert_ids,
        expert_score,
        gate_proj,
        up_proj,
        down_proj,
    )


def solution(mesh):
    in_specs = (
        P(("grp", "ep"), "tp"),
        P(("grp", "ep"), "tp"),
        P(("grp", "ep"), "tp"),
        P(),
        P(),
        P("tp", None),
        P(("grp", "ep", "tp"), None),
        P(),
        P(("grp", "ep", "tp"), None),
        P(("grp", "ep", "tp"), None),
        P("ep", None, "tp"),
        P("ep", None, "tp"),
        P("ep", "tp", None),
    )
    out_specs = (P(("grp", "ep", "tp"), None), P(("grp", "ep", "tp"), None))
    return jax.shard_map(local, mesh=mesh, in_specs=in_specs, out_specs=out_specs, check_vma=False)
```

```python
import functools
import math

import jax
import jax.numpy as jnp
import numpy as np
from jax import lax
from jax.experimental import pallas as pl
from jax.experimental.pallas import tpu as pltpu
from jax.sharding import PartitionSpec as P

GRID_W = 64


MESH = pl.DeviceIdType.MESH
EPS = 1e-06
THETA = 10000.0


def head_norm(vectors, gain):
    return vectors * lax.rsqrt(jnp.mean(vectors * vectors, axis=-1, keepdims=True) + EPS) * gain


def rotate_grid(vectors, token_positions):
    length, heads, head_dim = vectors.shape
    quarter = head_dim // 4
    freqs = 1.0 / THETA ** (jnp.arange(quarter, dtype=jnp.float32) * 4.0 / head_dim)
    grid_row = (token_positions // GRID_W).astype(jnp.float32)
    grid_col = (token_positions % GRID_W).astype(jnp.float32)
    angles = jnp.stack([grid_row[:, None] * freqs, grid_col[:, None] * freqs], axis=1)
    cosine = jnp.cos(angles)[:, None]
    sine = jnp.sin(angles)[:, None]
    halves = vectors.reshape(length, heads, 2, 2, quarter)
    first = halves[..., 0, :]
    second = halves[..., 1, :]
    turned = jnp.stack([first * cosine - second * sine, second * cosine + first * sine], axis=-2)
    return turned.reshape(length, heads, head_dim)


def prepare_inputs(raw_rows, gain, heads, token_positions):
    length = raw_rows.shape[0]
    head_dim = gain.shape[0]
    vectors = raw_rows.astype(jnp.float32).reshape(length, heads, head_dim)
    return rotate_grid(head_norm(vectors, gain), token_positions).astype(jnp.bfloat16)


def mixer_prepare(query_rows, projected_keys, projected_values, query_gain, key_norm_gain):
    length = query_rows.shape[0]
    head_dim = query_gain.shape[0]
    kv_heads = projected_keys.shape[1] // head_dim
    q_heads = query_rows.shape[1] // head_dim
    token_positions = lax.axis_index("ep") * length + jnp.arange(length, dtype=jnp.int32)
    query_matrix = prepare_inputs(query_rows, query_gain, q_heads, token_positions).reshape(
        length, q_heads * head_dim
    )
    keys_turned = prepare_inputs(projected_keys, key_norm_gain, kv_heads, token_positions).reshape(
        length, kv_heads * head_dim
    )
    return query_matrix, jnp.concatenate([keys_turned, projected_values], axis=1)


def attend_plain(query_matrix, own_pair, head_dim):
    length = query_matrix.shape[0]
    kv_heads = own_pair.shape[1] // (2 * head_dim)
    q_heads = query_matrix.shape[1] // head_dim
    queries_per_group = q_heads // kv_heads
    query_matrix = query_matrix.reshape(length, kv_heads, queries_per_group, head_dim)
    score_scale = head_dim ** (-0.5)
    initial = (
        jnp.full((kv_heads, queries_per_group, length), -1e30, jnp.float32),
        jnp.zeros((kv_heads, queries_per_group, length), jnp.float32),
        jnp.zeros((length, kv_heads, queries_per_group, head_dim), jnp.float32),
    )
    width = kv_heads * head_dim
    pair = lax.all_gather(own_pair, "ep", axis=0, tiled=True)
    key_piece = pair[:, :width]
    value_piece = pair[:, width:]
    piece_rows = key_piece.shape[0]
    step_rows = math.gcd(piece_rows, 1024)

    def one_block(block_index, running):
        run_max, run_sum, run_acc = running
        offset = block_index * step_rows
        key_block = lax.dynamic_slice_in_dim(key_piece, offset, step_rows, 0).reshape(
            step_rows, kv_heads, head_dim
        )
        value_block = lax.dynamic_slice_in_dim(value_piece, offset, step_rows, 0).reshape(
            step_rows, kv_heads, head_dim
        )
        scores = (
            jnp.einsum(
                "tkgd,skd->kgts", query_matrix, key_block, preferred_element_type=jnp.float32
            )
            * score_scale
        )
        new_max = jnp.maximum(run_max, jnp.max(scores, axis=-1))
        factor = jnp.exp(run_max - new_max)
        weights = jnp.exp(scores - new_max[..., None])
        run_sum = run_sum * factor + jnp.sum(weights, axis=-1)
        update = jnp.einsum(
            "kgts,skd->tkgd",
            weights.astype(jnp.bfloat16),
            value_block,
            preferred_element_type=jnp.float32,
        )
        run_acc = run_acc * jnp.transpose(factor, (2, 0, 1))[..., None] + update
        return (new_max, run_sum, run_acc)

    run_max, run_sum, run_acc = lax.fori_loop(0, piece_rows // step_rows, one_block, initial)
    return (
        (run_acc / jnp.transpose(run_sum, (2, 0, 1))[..., None])
        .astype(jnp.bfloat16)
        .reshape(length, q_heads * head_dim)
    )


def flip(index, bits):
    result, place = 0, 1
    for _ in range(8):
        mine = (index // place) % 2
        result = result + place * ((1 - mine) if bits & place else mine)
        place *= 2
    return result


def exchange_plain(outgoing, gate_proj, up_proj, down_proj):
    rows_in = lax.all_gather(
        lax.all_to_all(outgoing, "ep", split_axis=0, concat_axis=0, tiled=True),
        "tp",
        axis=0,
        tiled=True,
    )
    gate_out = jnp.einsum("secd,edf->secf", rows_in, gate_proj, preferred_element_type=jnp.float32)
    up_out = jnp.einsum("secd,edf->secf", rows_in, up_proj, preferred_element_type=jnp.float32)
    active = (jax.nn.silu(gate_out) * up_out).astype(jnp.bfloat16)
    summed = lax.psum_scatter(
        jnp.einsum("secf,efd->secd", active, down_proj, preferred_element_type=jnp.float32).astype(
            jnp.bfloat16
        ),
        "tp",
        scatter_dimension=0,
        tiled=True,
    )
    return lax.all_to_all(summed, "ep", split_axis=0, concat_axis=0, tiled=True)


def plain_halves(
    query_rows,
    projected_keys,
    projected_values,
    query_gain,
    key_norm_gain,
    out_proj,
    mix_tokens,
    norm_gain,
    expert_ids,
    expert_score,
    gate_proj,
    up_proj,
    down_proj,
):
    length, model_dim = mix_tokens.shape
    top_count = expert_ids.shape[1]
    local_experts = gate_proj.shape[0]
    expert_axis = lax.axis_size("ep")
    experts_all = expert_axis * local_experts
    capacity = length * top_count * 3 // (2 * experts_all)
    values_b = mix_tokens.astype(jnp.float32)
    normed = (
        values_b
        * lax.rsqrt(jnp.mean(values_b * values_b, axis=-1, keepdims=True) + EPS)
        * norm_gain
    ).astype(jnp.bfloat16)
    flat = expert_ids.reshape(length * top_count)
    onehot = (flat[:, None] == jnp.arange(experts_all, dtype=jnp.int32)).astype(jnp.int32)
    slots = jnp.sum((jnp.cumsum(onehot, axis=0) - onehot) * onehot, axis=1)
    target = flat * capacity + slots
    placed = (target[:, None] == jnp.arange(experts_all * capacity, dtype=jnp.int32)).astype(
        jnp.int32
    )
    placed = jnp.sum(placed.reshape(length, top_count, experts_all * capacity), axis=1).astype(
        jnp.bfloat16
    )
    outgoing = jnp.einsum("re,rd->ed", placed, normed, preferred_element_type=jnp.float32).astype(
        jnp.bfloat16
    )
    outgoing = outgoing.reshape(expert_axis, local_experts, capacity, model_dim)
    lanes = lax.axis_size("tp")
    head_dim = query_gain.shape[0]
    queries, pair = mixer_prepare(
        query_rows, projected_keys, projected_values, query_gain, key_norm_gain
    )
    heads_out = attend_plain(queries, pair, head_dim)
    returned = exchange_plain(outgoing, gate_proj, up_proj, down_proj)
    head_partial = jnp.dot(heads_out, out_proj, preferred_element_type=jnp.float32).astype(
        jnp.bfloat16
    )
    pieces = lax.all_to_all(
        head_partial.reshape(lanes, -1, head_partial.shape[1]),
        "tp",
        split_axis=0,
        concat_axis=0,
        tiled=True,
    )
    mixed_rows = jnp.sum(pieces.astype(jnp.float32), axis=0).astype(jnp.bfloat16)
    results = returned.reshape(experts_all * capacity, model_dim)
    first_weight = jax.nn.sigmoid(expert_score[:, 0] - expert_score[:, 1])
    picks = target.reshape(length, top_count)
    chosen = [
        jnp.dot(
            (picks[:, k : k + 1] == jnp.arange(experts_all * capacity, dtype=jnp.int32)).astype(
                jnp.bfloat16
            ),
            results,
            preferred_element_type=jnp.float32,
        )
        for k in range(2)
    ]
    combined = first_weight[:, None] * chosen[0] + (1.0 - first_weight)[:, None] * chosen[1]
    return (mixed_rows, combined.astype(jnp.bfloat16))


ORDER = (
    "SEND", "BO0", "RF0", "CO0", "RF1", "DO0", "AF00", "BO1", "AF10",
    "AF01", "AF11", "BF00", "BF10", "KV0", "CF00", "AF02", "CF10", "Y0",
    "AF12", "Y2", "BF11", "BF01", "DF00", "BF02", "CO1", "Y1", "CF11",
    "BF12", "DF10", "KV1", "BN0", "CF01", "DO1", "EF00", "CF12", "CF02",
    "DF12", "EF10", "DF11", "KV2", "BN1", "GF00", "CN0", "DF01", "GF10",
    "EF12", "DF02", "BN2", "BO2", "CN2", "EF11", "DN0", "GF12", "CN1",
    "EO1", "EF01", "ATT0", "DN2", "ATT1", "GF11", "CO2", "EF02", "DN1",
    "ATT2", "EN0", "GF01", "GF02", "DO2", "EO0", "EN2", "ATT3", "OUTP",
    "EN1", "MX0", "EO2", "CMBO", "CMBN", "CMBF", "MX1",
)
SENDS = (
    ("F", 0), ("X", 0), ("X", 1), ("F", 1), ("X", 2),
    ("N", 0), ("X", 3), ("N", 1), ("F", 2), ("F", 3), ("N", 2),
)
VMEM_LIMIT = 58 * 1024 * 1024


def fused_kernel(
    steps,
    tokens_ref,
    ids_ref,
    score_ref,
    ngain_ref,
    gate_hbm,
    up_hbm,
    down_hbm,
    proj_hbm,
    query_hbm,
    key_hbm,
    value_hbm,
    qgain_ref,
    kgain_ref,
    cos_hbm,
    sin_hbm,
    mixed_ref,
    expert_ref,
    gate_ref,
    up_ref,
    down_ref,
    proj_ref,
    query_ref,
    keyraw_ref,
    cos_ref,
    sin_ref,
    tok_ref,
    norm_ref,
    outf,
    scl,
    sc,
    orows,
    nrows,
    frows,
    act,
    part,
    from_core,
    to_x,
    from_x,
    total,
    fres,
    comb,
    oback,
    nback,
    fback,
    acc,
    lut,
    kv,
    heads_ref,
    pm,
    fc,
    to_xm,
    from_xm,
    hsem,
    near_s,
    near_r,
    far_s,
    far_r,
    rel_s,
    rel_r,
    xs,
    xr,
    cs,
    cr,
    ps,
    pr,
    qs,
    qr,
    nb_s,
    nb_r,
    fo_s,
    fo_r,
    fb_s,
    fb_r,
    sc_s,
    sc_r,
    ks,
    kr,
    ms,
    mr,
):
    me = lax.axis_index("ep")
    lane = lax.axis_index("tp")
    peers = [flip(me, k) for k in range(steps)]
    core, across = flip(lane, 1), flip(lane, 2)
    inner = ((me + 1) // 2) % 2
    outer = 1 - inner
    gate_at = 2 - me // 2
    sources = [3 - me, flip(3 - me, 1)]
    blocks, _, size, width = orows.shape
    wide = blocks - 1
    hidden = gate_ref.shape[1]
    length = query_ref.shape[0]
    dim = keyraw_ref.shape[1]
    count = tok_ref.shape[0]
    tile = math.gcd(hidden, 256)
    tile_out = math.gcd(width, 512)
    f32, b16 = jnp.float32, jnp.bfloat16

    offset = pl.multiple_of(me * length, 16)
    loads = [
        pltpu.make_async_copy(s, d, hsem.at[i])
        for i, (s, d) in enumerate(
            [
                (tokens_ref, tok_ref),
                (key_hbm, keyraw_ref),
                (value_hbm, kv.at[0, 1]),
                (cos_hbm.at[pl.ds(offset, length)], cos_ref),
                (sin_hbm.at[pl.ds(offset, length)], sin_ref),
                (query_hbm, query_ref),
                (gate_hbm, gate_ref),
                (up_hbm, up_ref),
                (down_hbm, down_ref),
                (proj_hbm, proj_ref),
            ]
        )
    ]
    for load in loads:
        load.start()

    barrier = pltpu.get_barrier_semaphore()
    friends = [{"ep": peers[k], "tp": lane} for k in range(1, steps)]
    friends += [{"ep": me, "tp": core}, {"ep": me, "tp": across}]
    for friend in friends:
        pl.semaphore_signal(barrier, inc=1, device_id=friend, device_id_type=MESH)

    def remote(src, dst, send, recv, ep_to, tp_to):
        return pltpu.make_async_remote_copy(
            src_ref=src,
            dst_ref=dst,
            send_sem=send,
            recv_sem=recv,
            device_id={"ep": ep_to, "tp": tp_to},
            device_id_type=MESH,
        )

    def when_inner(body):
        pl.when(inner == 1)(body)

    def when_outer(body):
        pl.when(inner == 0)(body)

    kinds = ("O", "N", "F0", "F1")
    window = range(wide)
    number = {(c, i): n * wide + i for n, c in enumerate(kinds) for i in window}

    def rows_of(c, i):
        if c == "O":
            return orows.at[i + inner]
        if c == "N":
            return nrows.at[i]
        return frows.at[int(c[1]), i + inner]

    def x_own(p):
        return remote(orows.at[p, 0], orows.at[p, 1], xs.at[p], xr.at[p], me, across)

    near = [
        [
            remote(
                orows.at[i + outer, n],
                nrows.at[i, n],
                near_s.at[n * wide + i],
                near_r.at[n * wide + i],
                peers[1],
                lane,
            )
            for i in window
        ]
        for n in range(2)
    ]
    far = [
        remote(
            outf.at[p],
            frows.at[outer, p, 0],
            far_s.at[p],
            far_r.at[outer * blocks + p],
            gate_at,
            lane,
        )
        for p in range(blocks)
    ]
    far_in = [
        [
            remote(
                outf.at[p], frows.at[j, p, 0], far_s.at[p], far_r.at[j * blocks + p], gate_at, lane
            )
            for p in range(blocks)
        ]
        for j in range(2)
    ]
    relay = [
        [
            remote(
                frows.at[j, p, 0],
                frows.at[j, p, 0],
                rel_s.at[j * wide + p],
                rel_r.at[j * wide + p],
                peers[1],
                lane,
            )
            for p in window
        ]
        for j in range(2)
    ]
    scale_out = remote(scl, sc.at[outer], sc_s.at[0], sc_r.at[outer], gate_at, lane)
    scale_in = [remote(scl, sc.at[j], sc_s.at[0], sc_r.at[j], gate_at, lane) for j in range(2)]
    x_far, c_in, c_out, x_out = {}, {}, {}, {}
    for (c, i), u in number.items():
        held = rows_of(c, i)
        if c[0] == "F":
            at = blocks + u - 2 * wide
            x_far[c, i] = remote(held.at[0], held.at[1], xs.at[at], xr.at[at], me, across)
        c_in[c, i] = remote(
            held.at[pl.ds(0, 2)], held.at[pl.ds(2, 2)], cs.at[u], cr.at[u], me, core
        )
        c_out[c, i] = remote(
            part.at[u, pl.ds(2, 2)], from_core.at[u], ps.at[u], pr.at[u], me, core
        )
        x_out[c, i] = remote(to_x.at[u], from_x.at[u], qs.at[u], qr.at[u], me, across)
    near_back = [
        remote(total.at[wide + i], nback.at[i], nb_s.at[i], nb_r.at[i], peers[1], lane)
        for i in window
    ]
    far_over = [
        [
            remote(
                total.at[(2 + j) * wide + i],
                fres.at[j, i],
                fo_s.at[j * wide + i],
                fo_r.at[j * wide + i],
                peers[1],
                lane,
            )
            for i in window
        ]
        for j in range(2)
    ]

    def far_back(j, p):
        if p == 0:
            source = fres.at[j, 0]
        elif p == wide:
            source = total.at[(2 + j) * wide + wide - 1]
        else:
            source = comb.at[j, p - 1]
        return remote(
            source, fback.at[p], fb_s.at[j * blocks + p], fb_r.at[p], sources[j], lane
        )

    kv_near = remote(kv.at[0], kv.at[1], ks.at[0], kr.at[0], peers[1], lane)
    kv_mid = remote(kv.at[pl.ds(0, 2)], kv.at[pl.ds(2, 2)], ks.at[1], kr.at[1], peers[3], lane)
    kv_far = remote(kv.at[pl.ds(2, 2)], kv.at[pl.ds(2, 2)], ks.at[2], kr.at[2], peers[1], lane)
    m_core = [
        remote(pm.at[core], fc.at[0], ms.at[0], mr.at[0], me, core),
        remote(pm.at[flip(core, 2)], fc.at[1], ms.at[1], mr.at[1], me, core),
    ]
    m_x = remote(to_xm, from_xm, ms.at[2], mr.at[2], me, across)

    token_row = lax.broadcasted_iota(jnp.int32, (count, count), 0)
    token_col = lax.broadcasted_iota(jnp.int32, (count, count), 1)
    earlier = (token_row < token_col).astype(b16)
    first, second = ids_ref[0:1, :], ids_ref[1:2, :]
    weight = 1.0 / (1.0 + jnp.exp(score_ref[1:2, :] - score_ref[0:1, :]))
    table_row = lax.broadcasted_iota(jnp.int32, (8, count), 0)
    high = me // 2
    ends = (3 * high, 3 - 3 * high)
    middles = (1 + high, 2 - high)

    def naming(expert):
        one, two = first == expert, second == expert
        share = jnp.where(one, weight, 0.0) + jnp.where(two, 1.0 - weight, 0.0)
        return jnp.where(one | two, 1.0, 0.0), share

    named = [(naming(ends[n]), naming(middles[n])) for n in range(2)]
    counted = jnp.zeros((8, count), f32)
    parts_of = []
    for n in range(2):
        (end_one, _), (mid_one, _) = named[n]
        both = end_one * mid_one
        parts_of.append((end_one - both, mid_one - both, both))
        for r in range(3):
            counted = jnp.where(table_row == 3 * n + r, parts_of[n][r], counted)
    rank = jnp.dot(counted.astype(b16), earlier, preferred_element_type=f32)
    sums = jnp.sum(counted, axis=1, keepdims=True)
    tail, middle = float(size), float(size * (wide - 1))

    def positions(n):
        end_only, mid_only, both = parts_of[n]
        end_rank, mid_rank, both_rank = (rank[3 * n + r : 3 * n + r + 1, :] for r in range(3))
        end_sum, both_sum = sums[3 * n : 3 * n + 1, :], sums[3 * n + 2 : 3 * n + 3, :]
        extra = jnp.maximum(both_sum - middle, 0.0)
        common = tail + jnp.minimum(both_sum, middle)
        end_at, mid_at = end_rank + extra, mid_rank + extra
        spill = jnp.maximum(end_sum + extra - tail, 0.0)
        shared = both_rank < middle
        end_pos = jnp.where(
            both > 0.5,
            jnp.where(shared, tail + both_rank, both_rank - middle),
            jnp.where(end_at < tail, end_at, common + end_at - tail),
        )
        mid_pos = jnp.where(
            both > 0.5,
            tail + both_rank,
            jnp.where(
                mid_at < tail, tail + middle + mid_at, common + spill + mid_at - tail
            ),
        )
        end_pos = jnp.where(end_only + both > 0.5, end_pos, -1.0)
        mid_pos = jnp.where(mid_only + both > 0.5, mid_pos, -1.0)
        return end_pos, mid_pos, jnp.where((both > 0.5) & shared, 1.0, 0.0)

    own_end, own_mid, _ = positions(0)
    far_end, far_mid, far_shared = positions(1)
    slot = lax.broadcasted_iota(jnp.int32, (count, count), 0).astype(f32)

    def dispatch(end_pos, mid_pos):
        chosen = ((slot == end_pos) | (slot == mid_pos)).astype(b16)
        picked = jnp.dot(chosen, norm_ref[...], preferred_element_type=f32)
        return picked.astype(b16).reshape(blocks, size, width)

    loads[0].wait()
    for n in range(blocks):
        spot = pl.ds(n * size, size)
        values = tok_ref[spot, :].astype(f32)
        norm_ref[spot, :] = (
            values
            * lax.rsqrt(jnp.mean(values * values, axis=-1, keepdims=True) + EPS)
            * ngain_ref[...]
        ).astype(b16)
    outf[...] = dispatch(far_end, far_mid)
    pl.semaphore_wait(barrier, len(friends))
    far[0].start()
    orows[:, 0] = dispatch(own_end, own_mid)

    def stage_send():
        for kind, p in SENDS:
            if kind == "F" and p > 0:
                far[p].start()
            elif kind == "X":
                x_own(p).start()
            elif kind == "N":
                near[0][p].start()
        end_share, mid_share = named[1][0][1], named[1][1][1]
        rows_mid = slice(size, size * wide)
        end_scale = jnp.sum(
            jnp.where(
                slot[rows_mid] == far_end, jnp.where(far_shared > 0.5, end_share, 1.0), 0.0
            ),
            axis=1,
            keepdims=True,
        )
        mid_scale = jnp.sum(
            jnp.where(
                slot[rows_mid] == far_mid, jnp.where(far_shared > 0.5, mid_share, 1.0), 0.0
            ),
            axis=1,
            keepdims=True,
        )
        lanes_of = lax.broadcasted_iota(jnp.int32, scl.shape, 1)
        scl[...] = jnp.where(lanes_of < scl.shape[1] // 2, end_scale, mid_scale)
        scale_out.start()
        is_inner = (jnp.zeros((1, count), jnp.int32) + inner) == 1
        own_mid_at = jnp.where(own_mid < 0.0, -1.0, own_mid - tail)
        table = (
            jnp.where(is_inner, own_mid_at, own_end),
            jnp.where(is_inner, own_end, own_mid_at),
            far_end,
            jnp.where(far_shared > 0.5, -1.0, far_mid),
            jnp.where(is_inner, named[0][1][1], named[0][0][1]),
            jnp.where(is_inner, named[0][0][1], named[0][1][1]),
            jnp.where(far_shared > 0.5, 1.0, end_share),
            mid_share,
        )
        kept = jnp.zeros((8, count), f32)
        for r in range(8):
            kept = jnp.where(table_row == r, table[r], kept)
        rest = jnp.zeros((count - 8, count), f32)
        lut[...] = jnp.transpose(jnp.concatenate([kept, rest], axis=0))

    turn_lane = lax.broadcasted_iota(jnp.int32, (length, dim), 1)
    leading = (turn_lane // (dim // 4)) % 2 == 0

    def turned(raw, gain):
        vectors = raw.astype(f32)
        vectors = (
            vectors
            * lax.rsqrt(jnp.mean(vectors * vectors, axis=-1, keepdims=True) + EPS)
            * gain[...]
        )
        other = jnp.where(
            leading,
            pltpu.roll(vectors, dim - dim // 4, 1),
            pltpu.roll(vectors, dim // 4, 1),
        )
        return (vectors * cos_ref[...] + other * sin_ref[...]).astype(b16)

    arrived = (set(), set())

    def own_arrived(by_role):
        missing = [p not in arrived[r] for r, p in enumerate(by_role)]
        for r, p in enumerate(by_role):
            arrived[r].add(p)
        for r, run in ((0, when_outer), (1, when_inner)):
            if missing[r]:

                @run
                def _(p=by_role[r]):
                    x_own(p).wait_recv()

    def stage_y(i):
        own_arrived((i + 1, i))
        near[1][i].start()

    def stage_a(c, i):
        j = int(c[1])

        @when_inner
        def _():
            far_in[j][i + 1].wait_recv()
            if i + 1 < wide:
                relay[j][i + 1].start()

        @when_outer
        def _():
            relay[j][i].wait_recv()

        x_far[c, i].start()

    def stage_r(j):
        @when_inner
        def _():
            far_in[j][0].wait_recv()
            relay[j][0].start()

    def stage_b(c, i):
        if c == "O":
            own_arrived((i, i + 1))
        elif c == "N":
            near[0][i].wait_recv()
            near[1][i].wait_recv()
        else:
            x_far[c, i].wait_recv()
        c_in[c, i].start()

    def stage_c(c, i):
        c_in[c, i].wait_recv()
        u = number[c, i]
        held = rows_of(c, i)

        @pl.loop(0, hidden // tile)
        def _(n):
            cols = pl.ds(pl.multiple_of(n * tile, tile), tile)
            block = held[...].reshape(4 * size, width)
            gate = jnp.dot(block, gate_ref[:, cols], preferred_element_type=f32)
            up = jnp.dot(block, up_ref[:, cols], preferred_element_type=f32)
            act[:, cols] = (gate / (1.0 + jnp.exp(-gate)) * up).astype(b16)

        @pl.loop(0, width // tile_out)
        def _(n):
            cols = pl.ds(pl.multiple_of(n * tile_out, tile_out), tile_out)
            summed = jnp.dot(act[...], down_ref[:, cols], preferred_element_type=f32)
            part[u, :, :, cols] = summed.astype(b16).reshape(4, size, tile_out)

        c_out[c, i].start()

    def stage_d(c, i):
        c_out[c, i].wait_recv()
        u = number[c, i]
        to_x[u] = (part[u, 1].astype(f32) + from_core[u, 1].astype(f32)).astype(b16)
        x_out[c, i].start()

    def stage_e(c, i):
        x_out[c, i].wait_recv()
        u = number[c, i]
        summed = (
            part[u, 0].astype(f32) + from_core[u, 0].astype(f32) + from_x[u].astype(f32)
        ).astype(b16)
        if c == "O":
            oback[i] = summed
            return
        total[u] = summed
        if c == "N":
            near_back[i].start()
            return
        j = int(c[1])
        when_outer(far_over[j][i].start)
        if i == wide - 1:
            when_inner(far_back(j, wide).start)

    def stage_g(j, p):
        if p > 0 and j not in scaled:
            scaled.add(j)
            when_inner(scale_in[j].wait_recv)

        @when_inner
        def _():
            far_over[j][p].wait_recv()
            if p > 0:
                spot = pl.ds((p - 1) * size, size)
                end_scale = sc[j, spot, 0:1]
                mid_scale = sc[j, spot, sc.shape[2] // 2 : sc.shape[2] // 2 + 1]
                comb[j, p - 1] = (
                    end_scale * fres[j, p].astype(f32)
                    + mid_scale * total[(2 + j) * wide + p - 1].astype(f32)
                ).astype(b16)
            far_back(j, p).start()

    def stage_kv(step):
        if step == 0:
            for n in range(1, 5):
                loads[n].wait()
            kv[0, 0] = turned(keyraw_ref[...], kgain_ref)
            kv_near.start()
        elif step == 1:
            kv_near.wait_recv()
            when_inner(kv_mid.start)
        else:

            @when_inner
            def _():
                kv_mid.wait_recv()
                kv_far.start()

    def stage_att(head):
        if head == 0:
            loads[5].wait()
            when_outer(kv_far.wait_recv)
        cols = slice(head * dim, (head + 1) * dim)
        held = steps * length
        queries = turned(query_ref[:, cols], qgain_ref)
        keys = kv[:, 0].reshape(held, dim)
        scores = (
            lax.dot_general(
                queries, keys, (((1,), (1,)), ((), ())), preferred_element_type=f32
            )
            * dim ** (-0.5)
        )
        probs = jnp.exp(scores - jnp.max(scores, axis=-1, keepdims=True))
        amount = jnp.sum(probs, axis=-1, keepdims=True)
        summed = jnp.dot(
            probs.astype(b16), kv[:, 1].reshape(held, dim), preferred_element_type=f32
        )
        heads_ref[:, cols] = (summed / amount).astype(b16)

    def stage_outp():
        loads[9].wait()

        @pl.loop(0, width // tile_out)
        def _(i):
            cols = pl.ds(pl.multiple_of(i * tile_out, tile_out), tile_out)
            summed = jnp.dot(heads_ref[...], proj_ref[:, cols], preferred_element_type=f32)
            pm[:, :, cols] = summed.astype(b16).reshape(4, length // 4, tile_out)

        for copy in m_core:
            copy.start()

    def stage_mx(step):
        if step == 0:
            for copy in m_core:
                copy.wait_recv()
            to_xm[...] = (pm[across].astype(f32) + fc[1].astype(f32)).astype(b16)
            m_x.start()
        else:
            m_x.wait_recv()
            mixed_ref[...] = (
                pm[lane].astype(f32) + fc[0].astype(f32) + from_xm[...].astype(f32)
            ).astype(b16)

    combined = []
    scaled = set()

    def stage_cmb(c):
        opening, closing = not combined, len(combined) == 2
        combined.append(c)
        if c == "N":
            for i in window:
                near_back[i].wait_recv()
        if c == "F":
            for p in range(blocks):
                far_back(0, p).wait_recv()
        store = {"O": oback, "N": nback, "F": fback}[c]
        columns = {"O": (0,), "N": (1,), "F": (2, 3)}[c]
        depth = store.shape[0] * size
        spot = lax.broadcasted_iota(jnp.int32, (count, depth), 1).astype(f32)
        chosen = jnp.concatenate(
            [(spot == lut[:, r : r + 1]).astype(b16) for r in columns], axis=0
        )

        @pl.loop(0, width // tile_out)
        def _(i):
            cols = pl.ds(pl.multiple_of(i * tile_out, tile_out), tile_out)
            results = store[:, :, cols].reshape(depth, tile_out)
            picked = jnp.dot(chosen, results, preferred_element_type=f32)
            found = lut[:, 4 + columns[0] : 5 + columns[0]] * picked[:count]
            if c == "F":
                found = found + lut[:, 7:8] * picked[count:]
            if not opening:
                found = acc[:, cols] + found
            if closing:
                expert_ref[:, cols] = found.astype(b16)
            else:
                acc[:, cols] = found

    stages = {"A": stage_a, "B": stage_b, "C": stage_c, "D": stage_d, "E": stage_e}
    loaded = False
    for name in ORDER:
        if name == "SEND":
            stage_send()
        elif name[:2] == "KV":
            stage_kv(int(name[2]))
        elif name[:3] == "ATT":
            stage_att(int(name[3]))
        elif name == "OUTP":
            stage_outp()
        elif name[:2] == "MX":
            stage_mx(int(name[2]))
        elif name[:3] == "CMB":
            stage_cmb(name[3])
        elif name[0] == "Y":
            stage_y(int(name[1]))
        elif name[0] == "R":
            stage_r(int(name[2]))
        elif name[0] == "G":
            stage_g(int(name[2]), int(name[3]))
        else:
            if name[0] == "C" and not loaded:
                loaded = True
                for n in (6, 7, 8):
                    loads[n].wait()
            stages[name[0]](name[1:-1], int(name[-1]))

    for p in range(blocks):
        x_own(p).wait_send()
        far[p].wait_send()
    for table in (x_far, c_in, c_out, x_out):
        for copy in table.values():
            copy.wait_send()
    for i in window:
        near[0][i].wait_send()
        near[1][i].wait_send()
        near_back[i].wait_send()
    scale_out.wait_send()
    kv_near.wait_send()

    @when_inner
    def _():
        kv_mid.wait_send()
        kv_far.wait_send()
        for j in range(2):
            for i in window:
                relay[j][i].wait_send()
            for p in range(blocks):
                far_back(j, p).wait_send()

    @when_outer
    def _():
        for j in range(2):
            for i in window:
                far_over[j][i].wait_send()

    for copy in m_core:
        copy.wait_send()
    m_x.wait_send()


def deliver_kernel(mixed_in, expert_in, mixed_out, expert_out, mixed_held, expert_held, sems):
    pairs = []
    for source, held, target, pieces in (
        (expert_in, expert_held, expert_out, 4),
        (mixed_in, mixed_held, mixed_out, 1),
    ):
        size = source.shape[0] // pieces
        for n in range(pieces):
            spot = pl.ds(n * size, size)
            at = len(pairs)
            pairs.append(
                (
                    pltpu.make_async_copy(source.at[spot], held.at[spot], sems.at[0, at]),
                    pltpu.make_async_copy(held.at[spot], target.at[spot], sems.at[1, at]),
                )
            )
    for fetch, _ in pairs:
        fetch.start()
    for fetch, store in pairs:
        fetch.wait()
        store.start()
    for _, store in pairs:
        store.wait()


def turn_tables(held, dim):
    quarter = dim // 4
    freqs = 1.0 / THETA ** (np.arange(quarter) * 4.0 / dim)
    spots = np.arange(held)
    tables = []
    for place in (spots // GRID_W, spots % GRID_W):
        angles = place[:, None] * freqs
        tables.append((np.cos(angles), np.sin(angles)))
    cosine = np.concatenate([tables[0][0]] * 2 + [tables[1][0]] * 2, axis=1)
    sine = np.concatenate(
        [-tables[0][1], tables[0][1], -tables[1][1], tables[1][1]], axis=1
    )
    return jnp.asarray(cosine, jnp.float32), jnp.asarray(sine, jnp.float32)


def fused(
    query_rows,
    projected_keys,
    projected_values,
    query_gain,
    key_norm_gain,
    out_proj,
    mix_tokens,
    norm_gain,
    expert_ids,
    expert_score,
    gate_proj,
    up_proj,
    down_proj,
):
    steps, lanes = lax.axis_size("ep"), lax.axis_size("tp")
    count, width = mix_tokens.shape
    cap = count * expert_ids.shape[1] * 3 // (2 * steps)
    size = count - cap
    blocks = count // size
    wide = blocks - 1
    hidden = gate_proj.shape[2]
    length, dim = projected_keys.shape
    kind = jnp.bfloat16
    cosine, sine = turn_tables(steps * length, dim)
    vmem = pl.BlockSpec(memory_space=pltpu.VMEM)
    anywhere = pl.BlockSpec(memory_space=pltpu.HBM)
    units = 4 * wide
    mixed, expert = pl.pallas_call(
        functools.partial(fused_kernel, steps),
        out_shape=(
            jax.ShapeDtypeStruct((length // lanes, width), kind),
            jax.ShapeDtypeStruct((count, width), kind),
        ),
        in_specs=[anywhere]
        + [vmem] * 3
        + [anywhere] * 7
        + [vmem] * 2
        + [anywhere] * 2,
        out_specs=(vmem, vmem),
        scratch_shapes=[
            pltpu.VMEM((width, hidden), kind),
            pltpu.VMEM((width, hidden), kind),
            pltpu.VMEM((hidden, width), kind),
            pltpu.VMEM(out_proj.shape, kind),
            pltpu.VMEM(query_rows.shape, kind),
            pltpu.VMEM((length, dim), kind),
            pltpu.VMEM((length, dim), jnp.float32),
            pltpu.VMEM((length, dim), jnp.float32),
            pltpu.VMEM((count, width), kind),
            pltpu.VMEM((count, width), kind),
            pltpu.VMEM((blocks, size, width), kind),
            pltpu.VMEM((size * (wide - 1), 128), jnp.float32),
            pltpu.VMEM((2, size * (wide - 1), 128), jnp.float32),
            pltpu.VMEM((blocks, 4, size, width), kind),
            pltpu.VMEM((wide, 4, size, width), kind),
            pltpu.VMEM((2, blocks, 4, size, width), kind),
            pltpu.VMEM((4 * size, hidden), kind),
            pltpu.VMEM((units, 4, size, width), kind),
            pltpu.VMEM((units, 2, size, width), kind),
            pltpu.VMEM((units, size, width), kind),
            pltpu.VMEM((units, size, width), kind),
            pltpu.VMEM((units, size, width), kind),
            pltpu.VMEM((2, wide, size, width), kind),
            pltpu.VMEM((2, wide - 1, size, width), kind),
            pltpu.VMEM((wide, size, width), kind),
            pltpu.VMEM((wide, size, width), kind),
            pltpu.VMEM((blocks, size, width), kind),
            pltpu.VMEM((count, width), jnp.float32),
            pltpu.VMEM((count, count), jnp.float32),
            pltpu.VMEM((steps, 2, length, dim), kind),
            pltpu.VMEM(query_rows.shape, kind),
            pltpu.VMEM((lanes, length // lanes, width), kind),
            pltpu.VMEM((2, length // lanes, width), kind),
            pltpu.VMEM((length // lanes, width), kind),
            pltpu.VMEM((length // lanes, width), kind),
            pltpu.SemaphoreType.DMA((10,)),
        ]
        + [pltpu.SemaphoreType.DMA((2 * blocks,))] * 6
        + [pltpu.SemaphoreType.DMA((blocks + 2 * wide,))] * 2
        + [pltpu.SemaphoreType.DMA((units,))] * 6
        + [pltpu.SemaphoreType.DMA((2 * blocks,))] * 6
        + [pltpu.SemaphoreType.DMA((3,))] * 6,
        compiler_params=pltpu.CompilerParams(
            collective_id=0, has_side_effects=True, vmem_limit_bytes=VMEM_LIMIT
        ),
    )(
        mix_tokens,
        expert_ids.T,
        expert_score.T,
        norm_gain.reshape(1, width),
        gate_proj.reshape(gate_proj.shape[1:]),
        up_proj.reshape(up_proj.shape[1:]),
        down_proj.reshape(down_proj.shape[1:]),
        out_proj,
        query_rows,
        projected_keys,
        projected_values,
        query_gain.reshape(1, dim),
        key_norm_gain.reshape(1, dim),
        cosine,
        sine,
    )
    return pl.pallas_call(
        deliver_kernel,
        out_shape=(
            jax.ShapeDtypeStruct(mixed.shape, kind),
            jax.ShapeDtypeStruct(expert.shape, kind),
        ),
        in_specs=[anywhere] * 2,
        out_specs=(anywhere, anywhere),
        scratch_shapes=[
            pltpu.VMEM(mixed.shape, kind),
            pltpu.VMEM(expert.shape, kind),
            pltpu.SemaphoreType.DMA((2, 5)),
        ],
    )(mixed, expert)


def fits_fused(query_rows, projected_keys, query_gain, mix_tokens, expert_ids, gate_proj):
    steps, lanes = lax.axis_size("ep"), lax.axis_size("tp")
    count, width = mix_tokens.shape
    length, dim = projected_keys.shape
    local_experts, _, hidden = gate_proj.shape
    cap = count * expert_ids.shape[1] * 3 // (2 * steps)
    blocks = 20 * steps * cap * width * 2 + 4 * width * hidden * 2
    return (
        lanes == 4
        and steps == 4
        and local_experts == 1
        and expert_ids.shape[1] == 2
        and dim == query_gain.shape[0]
        and dim % 128 == 0
        and length % 64 == 0
        and length <= 256
        and count == 128
        and cap < count
        and (count - cap) % 16 == 0
        and cap % (count - cap) == 0
        and 2 * cap > count
        and blocks < 48 * 1024 * 1024
    )


def local(
    query_rows,
    projected_keys,
    projected_values,
    query_gain,
    key_norm_gain,
    out_proj,
    mix_tokens,
    norm_gain,
    expert_ids,
    expert_score,
    gate_proj,
    up_proj,
    down_proj,
):
    simple = fits_fused(
        query_rows, projected_keys, query_gain, mix_tokens, expert_ids, gate_proj
    )
    return (fused if simple else plain_halves)(
        query_rows,
        projected_keys,
        projected_values,
        query_gain,
        key_norm_gain,
        out_proj,
        mix_tokens,
        norm_gain,
        expert_ids,
        expert_score,
        gate_proj,
        up_proj,
        down_proj,
    )


def solution(mesh):
    in_specs = (
        P(("grp", "ep"), "tp"),
        P(("grp", "ep"), "tp"),
        P(("grp", "ep"), "tp"),
        P(),
        P(),
        P("tp", None),
        P(("grp", "ep", "tp"), None),
        P(),
        P(("grp", "ep", "tp"), None),
        P(("grp", "ep", "tp"), None),
        P("ep", None, "tp"),
        P("ep", None, "tp"),
        P("ep", "tp", None),
    )
    out_specs = (P(("grp", "ep", "tp"), None), P(("grp", "ep", "tp"), None))
    return jax.shard_map(local, mesh=mesh, in_specs=in_specs, out_specs=out_specs, check_vma=False)
```

```python
import functools
import math

import jax
import jax.numpy as jnp
import numpy as np
from jax import lax
from jax.experimental import pallas as pl
from jax.experimental.pallas import tpu as pltpu
from jax.sharding import PartitionSpec as P

GRID_W = 64


MESH = pl.DeviceIdType.MESH
EPS = 1e-06
THETA = 10000.0


def head_norm(vectors, gain):
    return vectors * lax.rsqrt(jnp.mean(vectors * vectors, axis=-1, keepdims=True) + EPS) * gain


def rotate_grid(vectors, token_positions):
    length, heads, head_dim = vectors.shape
    quarter = head_dim // 4
    freqs = 1.0 / THETA ** (jnp.arange(quarter, dtype=jnp.float32) * 4.0 / head_dim)
    grid_row = (token_positions // GRID_W).astype(jnp.float32)
    grid_col = (token_positions % GRID_W).astype(jnp.float32)
    angles = jnp.stack([grid_row[:, None] * freqs, grid_col[:, None] * freqs], axis=1)
    cosine = jnp.cos(angles)[:, None]
    sine = jnp.sin(angles)[:, None]
    halves = vectors.reshape(length, heads, 2, 2, quarter)
    first = halves[..., 0, :]
    second = halves[..., 1, :]
    turned = jnp.stack([first * cosine - second * sine, second * cosine + first * sine], axis=-2)
    return turned.reshape(length, heads, head_dim)


def prepare_inputs(raw_rows, gain, heads, token_positions):
    length = raw_rows.shape[0]
    head_dim = gain.shape[0]
    vectors = raw_rows.astype(jnp.float32).reshape(length, heads, head_dim)
    return rotate_grid(head_norm(vectors, gain), token_positions).astype(jnp.bfloat16)


def mixer_prepare(query_rows, projected_keys, projected_values, query_gain, key_norm_gain):
    length = query_rows.shape[0]
    head_dim = query_gain.shape[0]
    kv_heads = projected_keys.shape[1] // head_dim
    q_heads = query_rows.shape[1] // head_dim
    token_positions = lax.axis_index("ep") * length + jnp.arange(length, dtype=jnp.int32)
    query_matrix = prepare_inputs(query_rows, query_gain, q_heads, token_positions).reshape(
        length, q_heads * head_dim
    )
    keys_turned = prepare_inputs(projected_keys, key_norm_gain, kv_heads, token_positions).reshape(
        length, kv_heads * head_dim
    )
    return query_matrix, jnp.concatenate([keys_turned, projected_values], axis=1)


def attend_plain(query_matrix, own_pair, head_dim):
    length = query_matrix.shape[0]
    kv_heads = own_pair.shape[1] // (2 * head_dim)
    q_heads = query_matrix.shape[1] // head_dim
    queries_per_group = q_heads // kv_heads
    query_matrix = query_matrix.reshape(length, kv_heads, queries_per_group, head_dim)
    score_scale = head_dim ** (-0.5)
    initial = (
        jnp.full((kv_heads, queries_per_group, length), -1e30, jnp.float32),
        jnp.zeros((kv_heads, queries_per_group, length), jnp.float32),
        jnp.zeros((length, kv_heads, queries_per_group, head_dim), jnp.float32),
    )
    width = kv_heads * head_dim
    pair = lax.all_gather(own_pair, "ep", axis=0, tiled=True)
    key_piece = pair[:, :width]
    value_piece = pair[:, width:]
    piece_rows = key_piece.shape[0]
    step_rows = math.gcd(piece_rows, 1024)

    def one_block(block_index, running):
        run_max, run_sum, run_acc = running
        offset = block_index * step_rows
        key_block = lax.dynamic_slice_in_dim(key_piece, offset, step_rows, 0).reshape(
            step_rows, kv_heads, head_dim
        )
        value_block = lax.dynamic_slice_in_dim(value_piece, offset, step_rows, 0).reshape(
            step_rows, kv_heads, head_dim
        )
        scores = (
            jnp.einsum(
                "tkgd,skd->kgts", query_matrix, key_block, preferred_element_type=jnp.float32
            )
            * score_scale
        )
        new_max = jnp.maximum(run_max, jnp.max(scores, axis=-1))
        factor = jnp.exp(run_max - new_max)
        weights = jnp.exp(scores - new_max[..., None])
        run_sum = run_sum * factor + jnp.sum(weights, axis=-1)
        update = jnp.einsum(
            "kgts,skd->tkgd",
            weights.astype(jnp.bfloat16),
            value_block,
            preferred_element_type=jnp.float32,
        )
        run_acc = run_acc * jnp.transpose(factor, (2, 0, 1))[..., None] + update
        return (new_max, run_sum, run_acc)

    run_max, run_sum, run_acc = lax.fori_loop(0, piece_rows // step_rows, one_block, initial)
    return (
        (run_acc / jnp.transpose(run_sum, (2, 0, 1))[..., None])
        .astype(jnp.bfloat16)
        .reshape(length, q_heads * head_dim)
    )


def flip(index, bits):
    result, place = 0, 1
    for _ in range(8):
        mine = (index // place) % 2
        result = result + place * ((1 - mine) if bits & place else mine)
        place *= 2
    return result


def exchange_plain(outgoing, gate_proj, up_proj, down_proj):
    rows_in = lax.all_gather(
        lax.all_to_all(outgoing, "ep", split_axis=0, concat_axis=0, tiled=True),
        "tp",
        axis=0,
        tiled=True,
    )
    gate_out = jnp.einsum("secd,edf->secf", rows_in, gate_proj, preferred_element_type=jnp.float32)
    up_out = jnp.einsum("secd,edf->secf", rows_in, up_proj, preferred_element_type=jnp.float32)
    active = (jax.nn.silu(gate_out) * up_out).astype(jnp.bfloat16)
    summed = lax.psum_scatter(
        jnp.einsum("secf,efd->secd", active, down_proj, preferred_element_type=jnp.float32).astype(
            jnp.bfloat16
        ),
        "tp",
        scatter_dimension=0,
        tiled=True,
    )
    return lax.all_to_all(summed, "ep", split_axis=0, concat_axis=0, tiled=True)


def plain_halves(
    query_rows,
    projected_keys,
    projected_values,
    query_gain,
    key_norm_gain,
    out_proj,
    mix_tokens,
    norm_gain,
    expert_ids,
    expert_score,
    gate_proj,
    up_proj,
    down_proj,
):
    length, model_dim = mix_tokens.shape
    top_count = expert_ids.shape[1]
    local_experts = gate_proj.shape[0]
    expert_axis = lax.axis_size("ep")
    experts_all = expert_axis * local_experts
    capacity = length * top_count * 3 // (2 * experts_all)
    values_b = mix_tokens.astype(jnp.float32)
    normed = (
        values_b
        * lax.rsqrt(jnp.mean(values_b * values_b, axis=-1, keepdims=True) + EPS)
        * norm_gain
    ).astype(jnp.bfloat16)
    flat = expert_ids.reshape(length * top_count)
    onehot = (flat[:, None] == jnp.arange(experts_all, dtype=jnp.int32)).astype(jnp.int32)
    slots = jnp.sum((jnp.cumsum(onehot, axis=0) - onehot) * onehot, axis=1)
    target = flat * capacity + slots
    placed = (target[:, None] == jnp.arange(experts_all * capacity, dtype=jnp.int32)).astype(
        jnp.int32
    )
    placed = jnp.sum(placed.reshape(length, top_count, experts_all * capacity), axis=1).astype(
        jnp.bfloat16
    )
    outgoing = jnp.einsum("re,rd->ed", placed, normed, preferred_element_type=jnp.float32).astype(
        jnp.bfloat16
    )
    outgoing = outgoing.reshape(expert_axis, local_experts, capacity, model_dim)
    lanes = lax.axis_size("tp")
    head_dim = query_gain.shape[0]
    queries, pair = mixer_prepare(
        query_rows, projected_keys, projected_values, query_gain, key_norm_gain
    )
    heads_out = attend_plain(queries, pair, head_dim)
    returned = exchange_plain(outgoing, gate_proj, up_proj, down_proj)
    head_partial = jnp.dot(heads_out, out_proj, preferred_element_type=jnp.float32).astype(
        jnp.bfloat16
    )
    pieces = lax.all_to_all(
        head_partial.reshape(lanes, -1, head_partial.shape[1]),
        "tp",
        split_axis=0,
        concat_axis=0,
        tiled=True,
    )
    mixed_rows = jnp.sum(pieces.astype(jnp.float32), axis=0).astype(jnp.bfloat16)
    results = returned.reshape(experts_all * capacity, model_dim)
    first_weight = jax.nn.sigmoid(expert_score[:, 0] - expert_score[:, 1])
    picks = target.reshape(length, top_count)
    chosen = [
        jnp.dot(
            (picks[:, k : k + 1] == jnp.arange(experts_all * capacity, dtype=jnp.int32)).astype(
                jnp.bfloat16
            ),
            results,
            preferred_element_type=jnp.float32,
        )
        for k in range(2)
    ]
    combined = first_weight[:, None] * chosen[0] + (1.0 - first_weight)[:, None] * chosen[1]
    return (mixed_rows, combined.astype(jnp.bfloat16))


ORDER = (
    "SEND", "PRE", "BO2", "RF1", "CO2", "DO2", "AF10", "BO1", "RF0",
    "AF11", "CO1", "AF00", "AF12", "BF11", "KV0", "AF01", "BF10", "Y1",
    "Y0", "CF11", "CF10", "DF11", "KV1", "DF10", "BF12", "BF01", "BF00",
    "Y2", "EO2", "CF12", "AF02", "EF11", "DF12", "KV2", "CF01", "BN0",
    "CF00", "DF00", "DF01", "BF02", "DO1", "EF10", "EF12", "CF02", "BN1",
    "CN0", "BN2", "ATT0", "GF10", "GF11", "EF00", "ATT1", "DF02", "GF12",
    "BO0", "CN1", "DN0", "EF01", "GF00", "CN2", "DN1", "CO0", "EF02",
    "ATT2", "EO1", "DN2", "ATT3", "DO0", "EN0", "EN1", "OUTP", "GF02",
    "GF01", "EN2", "MX0", "EO0", "CMB", "MX1",
)
SENDS = (
    ("F", 0), ("F", 1), ("N", 0), ("F", 2), ("N", 1),
    ("X", 3), ("N", 2), ("F", 3), ("X", 2), ("X", 1), ("X", 0),
)
VMEM_LIMIT = 58 * 1024 * 1024


def fused_kernel(
    steps,
    tokens_hbm,
    ids_hbm,
    score_hbm,
    ngain_hbm,
    gate_hbm,
    up_hbm,
    down_hbm,
    proj_hbm,
    query_hbm,
    key_hbm,
    value_hbm,
    qgain_hbm,
    kgain_hbm,
    cos_hbm,
    sin_hbm,
    mixed_hbm,
    expert_hbm,
    ids_ref,
    score_ref,
    ngain_ref,
    qgain_ref,
    kgain_ref,
    mixed_ref,
    expert_ref,
    pick,
    gate_ref,
    up_ref,
    down_ref,
    proj_ref,
    query_ref,
    keyraw_ref,
    cos_ref,
    sin_ref,
    tok_ref,
    norm_ref,
    outf,
    scl,
    sc,
    orows,
    nrows,
    frows,
    act,
    part,
    from_core,
    to_x,
    from_x,
    total,
    fres,
    comb,
    oback,
    nback,
    fback,
    lut,
    kv,
    heads_ref,
    pm,
    fc,
    to_xm,
    from_xm,
    hsem,
    osem,
    near_s,
    near_r,
    far_s,
    far_r,
    rel_s,
    rel_r,
    xs,
    xr,
    cs,
    cr,
    ps,
    pr,
    qs,
    qr,
    nb_s,
    nb_r,
    fo_s,
    fo_r,
    fb_s,
    fb_r,
    sc_s,
    sc_r,
    ks,
    kr,
    ms,
    mr,
):
    me = lax.axis_index("ep")
    lane = lax.axis_index("tp")
    peers = [flip(me, k) for k in range(steps)]
    core, across = flip(lane, 1), flip(lane, 2)
    inner = ((me + 1) // 2) % 2
    outer = 1 - inner
    gate_at = 2 - me // 2
    sources = [3 - me, flip(3 - me, 1)]
    blocks, _, size, width = orows.shape
    wide = blocks - 1
    hidden = gate_ref.shape[1]
    length = query_ref.shape[0]
    dim = keyraw_ref.shape[1]
    count = tok_ref.shape[0]
    tile = math.gcd(hidden, 256)
    tile_out = math.gcd(width, 512)
    f32, b16 = jnp.float32, jnp.bfloat16

    offset = pl.multiple_of(me * length, 16)
    loads = [
        pltpu.make_async_copy(s, d, hsem.at[i])
        for i, (s, d) in enumerate(
            [
                (ids_hbm, ids_ref),
                (score_hbm, score_ref),
                (tokens_hbm, tok_ref),
                (ngain_hbm, ngain_ref),
                (kgain_hbm, kgain_ref),
                (key_hbm, keyraw_ref),
                (value_hbm, kv.at[0, 1]),
                (cos_hbm.at[pl.ds(offset, length)], cos_ref),
                (sin_hbm.at[pl.ds(offset, length)], sin_ref),
                (qgain_hbm, qgain_ref),
                (query_hbm, query_ref),
                (gate_hbm, gate_ref),
                (up_hbm, up_ref),
                (down_hbm, down_ref),
                (proj_hbm, proj_ref),
            ]
        )
    ]
    for load in loads:
        load.start()

    barrier = pltpu.get_barrier_semaphore()
    friends = [{"ep": peers[k], "tp": lane} for k in range(1, steps)]
    friends += [{"ep": me, "tp": core}, {"ep": me, "tp": across}]
    for friend in friends:
        pl.semaphore_signal(barrier, inc=1, device_id=friend, device_id_type=MESH)

    def remote(src, dst, send, recv, ep_to, tp_to):
        return pltpu.make_async_remote_copy(
            src_ref=src,
            dst_ref=dst,
            send_sem=send,
            recv_sem=recv,
            device_id={"ep": ep_to, "tp": tp_to},
            device_id_type=MESH,
        )

    def when_inner(body):
        pl.when(inner == 1)(body)

    def when_outer(body):
        pl.when(inner == 0)(body)

    kinds = ("O", "N", "F0", "F1")
    window = range(wide)
    number = {(c, i): n * wide + i for n, c in enumerate(kinds) for i in window}

    def rows_of(c, i):
        if c == "O":
            return orows.at[i + inner]
        if c == "N":
            return nrows.at[i]
        return frows.at[int(c[1]), i + inner]

    def x_own(p):
        return remote(orows.at[p, 0], orows.at[p, 1], xs.at[p], xr.at[p], me, across)

    near = [
        [
            remote(
                orows.at[i + outer, n],
                nrows.at[i, n],
                near_s.at[n * wide + i],
                near_r.at[n * wide + i],
                peers[1],
                lane,
            )
            for i in window
        ]
        for n in range(2)
    ]
    far = [
        remote(
            outf.at[p],
            frows.at[outer, p, 0],
            far_s.at[p],
            far_r.at[outer * blocks + p],
            gate_at,
            lane,
        )
        for p in range(blocks)
    ]
    far_in = [
        [
            remote(
                outf.at[p], frows.at[j, p, 0], far_s.at[p], far_r.at[j * blocks + p], gate_at, lane
            )
            for p in range(blocks)
        ]
        for j in range(2)
    ]
    relay = [
        [
            remote(
                frows.at[j, p, 0],
                frows.at[j, p, 0],
                rel_s.at[j * wide + p],
                rel_r.at[j * wide + p],
                peers[1],
                lane,
            )
            for p in window
        ]
        for j in range(2)
    ]
    scale_out = remote(scl, sc.at[outer], sc_s.at[0], sc_r.at[outer], gate_at, lane)
    scale_in = [remote(scl, sc.at[j], sc_s.at[0], sc_r.at[j], gate_at, lane) for j in range(2)]
    x_far, c_in, c_out, x_out = {}, {}, {}, {}
    for (c, i), u in number.items():
        held = rows_of(c, i)
        if c[0] == "F":
            at = blocks + u - 2 * wide
            x_far[c, i] = remote(held.at[0], held.at[1], xs.at[at], xr.at[at], me, across)
        c_in[c, i] = remote(
            held.at[pl.ds(0, 2)], held.at[pl.ds(2, 2)], cs.at[u], cr.at[u], me, core
        )
        c_out[c, i] = remote(
            part.at[u, pl.ds(2, 2)], from_core.at[u], ps.at[u], pr.at[u], me, core
        )
        x_out[c, i] = remote(to_x.at[u], from_x.at[u], qs.at[u], qr.at[u], me, across)
    near_back = [
        remote(total.at[wide + i], nback.at[i], nb_s.at[i], nb_r.at[i], peers[1], lane)
        for i in window
    ]
    far_over = [
        [
            remote(
                total.at[(2 + j) * wide + i],
                fres.at[j, i],
                fo_s.at[j * wide + i],
                fo_r.at[j * wide + i],
                peers[1],
                lane,
            )
            for i in window
        ]
        for j in range(2)
    ]

    def far_back(j, p):
        if p == 0:
            source = fres.at[j, 0]
        elif p == wide:
            source = total.at[(2 + j) * wide + wide - 1]
        else:
            source = comb.at[j, p - 1]
        return remote(
            source, fback.at[p], fb_s.at[j * blocks + p], fb_r.at[p], sources[j], lane
        )

    kv_near = remote(kv.at[0], kv.at[1], ks.at[0], kr.at[0], peers[1], lane)
    kv_mid = remote(kv.at[pl.ds(0, 2)], kv.at[pl.ds(2, 2)], ks.at[1], kr.at[1], peers[3], lane)
    kv_far = remote(kv.at[pl.ds(2, 2)], kv.at[pl.ds(2, 2)], ks.at[2], kr.at[2], peers[1], lane)
    m_core = [
        remote(pm.at[core], fc.at[0], ms.at[0], mr.at[0], me, core),
        remote(pm.at[flip(core, 2)], fc.at[1], ms.at[1], mr.at[1], me, core),
    ]
    m_x = remote(to_xm, from_xm, ms.at[2], mr.at[2], me, across)
    mixed_out = pltpu.make_async_copy(mixed_ref, mixed_hbm, osem.at[0])
    expert_out = [
        pltpu.make_async_copy(
            expert_ref.at[:, pl.ds(n * tile_out, tile_out)],
            expert_hbm.at[:, pl.ds(n * tile_out, tile_out)],
            osem.at[1 + n],
        )
        for n in range(width // tile_out)
    ]

    loads[0].wait()
    loads[1].wait()

    token_row = lax.broadcasted_iota(jnp.int32, (count, count), 0)
    token_col = lax.broadcasted_iota(jnp.int32, (count, count), 1)
    earlier = (token_row < token_col).astype(b16)
    first, second = ids_ref[0:1, :], ids_ref[1:2, :]
    weight = 1.0 / (1.0 + jnp.exp(score_ref[1:2, :] - score_ref[0:1, :]))
    table_row = lax.broadcasted_iota(jnp.int32, (8, count), 0)
    high = me // 2
    ends = (3 * high, 3 - 3 * high)
    middles = (1 + high, 2 - high)

    def naming(expert):
        one, two = first == expert, second == expert
        share = jnp.where(one, weight, 0.0) + jnp.where(two, 1.0 - weight, 0.0)
        return jnp.where(one | two, 1.0, 0.0), share

    named = [(naming(ends[n]), naming(middles[n])) for n in range(2)]
    counted = jnp.zeros((8, count), f32)
    parts_of = []
    for n in range(2):
        (end_one, _), (mid_one, _) = named[n]
        both = end_one * mid_one
        parts_of.append((end_one - both, mid_one - both, both))
        for r in range(3):
            counted = jnp.where(table_row == 3 * n + r, parts_of[n][r], counted)
    rank = jnp.dot(counted.astype(b16), earlier, preferred_element_type=f32)
    sums = jnp.sum(counted, axis=1, keepdims=True)
    tail, middle = float(size), float(size * (wide - 1))

    def positions(n):
        end_only, mid_only, both = parts_of[n]
        end_rank, mid_rank, both_rank = (rank[3 * n + r : 3 * n + r + 1, :] for r in range(3))
        end_sum, both_sum = sums[3 * n : 3 * n + 1, :], sums[3 * n + 2 : 3 * n + 3, :]
        extra = jnp.maximum(both_sum - middle, 0.0)
        common = tail + jnp.minimum(both_sum, middle)
        end_at, mid_at = end_rank + extra, mid_rank + extra
        spill = jnp.maximum(end_sum + extra - tail, 0.0)
        shared = both_rank < middle
        end_pos = jnp.where(
            both > 0.5,
            jnp.where(shared, tail + both_rank, both_rank - middle),
            jnp.where(end_at < tail, end_at, common + end_at - tail),
        )
        mid_pos = jnp.where(
            both > 0.5,
            tail + both_rank,
            jnp.where(
                mid_at < tail, tail + middle + mid_at, common + spill + mid_at - tail
            ),
        )
        end_pos = jnp.where(end_only + both > 0.5, end_pos, -1.0)
        mid_pos = jnp.where(mid_only + both > 0.5, mid_pos, -1.0)
        return end_pos, mid_pos, jnp.where((both > 0.5) & shared, 1.0, 0.0)

    own_end, own_mid, _ = positions(0)
    far_end, far_mid, far_shared = positions(1)
    slot = lax.broadcasted_iota(jnp.int32, (count, count), 0).astype(f32)

    def dispatch(end_pos, mid_pos):
        chosen = ((slot == end_pos) | (slot == mid_pos)).astype(b16)
        picked = jnp.dot(chosen, norm_ref[...], preferred_element_type=f32)
        return picked.astype(b16).reshape(blocks, size, width)

    loads[2].wait()
    loads[3].wait()
    for n in range(blocks):
        spot = pl.ds(n * size, size)
        values = tok_ref[spot, :].astype(f32)
        norm_ref[spot, :] = (
            values
            * lax.rsqrt(jnp.mean(values * values, axis=-1, keepdims=True) + EPS)
            * ngain_ref[...]
        ).astype(b16)
    outf[...] = dispatch(far_end, far_mid)
    pl.semaphore_wait(barrier, len(friends))
    far[0].start()
    orows[:, 0] = dispatch(own_end, own_mid)

    def stage_send():
        for kind, p in SENDS:
            if kind == "F" and p > 0:
                far[p].start()
            elif kind == "X":
                x_own(p).start()
            elif kind == "N":
                near[0][p].start()
        end_share, mid_share = named[1][0][1], named[1][1][1]
        rows_mid = slice(size, size * wide)
        end_scale = jnp.sum(
            jnp.where(
                slot[rows_mid] == far_end, jnp.where(far_shared > 0.5, end_share, 1.0), 0.0
            ),
            axis=1,
            keepdims=True,
        )
        mid_scale = jnp.sum(
            jnp.where(
                slot[rows_mid] == far_mid, jnp.where(far_shared > 0.5, mid_share, 1.0), 0.0
            ),
            axis=1,
            keepdims=True,
        )
        lanes_of = lax.broadcasted_iota(jnp.int32, scl.shape, 1)
        scl[...] = jnp.where(lanes_of < scl.shape[1] // 2, end_scale, mid_scale)
        scale_out.start()
        is_inner = (jnp.zeros((1, count), jnp.int32) + inner) == 1
        own_mid_at = jnp.where(own_mid < 0.0, -1.0, own_mid - tail)
        table = (
            jnp.where(is_inner, own_mid_at, own_end),
            jnp.where(is_inner, own_end, own_mid_at),
            far_end,
            jnp.where(far_shared > 0.5, -1.0, far_mid),
            jnp.where(is_inner, named[0][1][1], named[0][0][1]),
            jnp.where(is_inner, named[0][0][1], named[0][1][1]),
            jnp.where(far_shared > 0.5, 1.0, end_share),
            mid_share,
        )
        kept = jnp.zeros((8, count), f32)
        for r in range(8):
            kept = jnp.where(table_row == r, table[r], kept)
        rest = jnp.zeros((count - 8, count), f32)
        lut[...] = jnp.transpose(jnp.concatenate([kept, rest], axis=0))

    turn_lane = lax.broadcasted_iota(jnp.int32, (length, dim), 1)
    leading = (turn_lane // (dim // 4)) % 2 == 0

    def turned(raw, gain):
        vectors = raw.astype(f32)
        vectors = (
            vectors
            * lax.rsqrt(jnp.mean(vectors * vectors, axis=-1, keepdims=True) + EPS)
            * gain[...]
        )
        other = jnp.where(
            leading,
            pltpu.roll(vectors, dim - dim // 4, 1),
            pltpu.roll(vectors, dim // 4, 1),
        )
        return (vectors * cos_ref[...] + other * sin_ref[...]).astype(b16)

    arrived = (set(), set())
    scaled = set()

    def own_arrived(by_role):
        missing = [p not in arrived[r] for r, p in enumerate(by_role)]
        for r, p in enumerate(by_role):
            arrived[r].add(p)
        for r, run in ((0, when_outer), (1, when_inner)):
            if missing[r]:

                @run
                def _(p=by_role[r]):
                    x_own(p).wait_recv()

    def stage_y(i):
        own_arrived((i + 1, i))
        near[1][i].start()

    def stage_a(c, i):
        j = int(c[1])

        @when_inner
        def _():
            far_in[j][i + 1].wait_recv()
            if i + 1 < wide:
                relay[j][i + 1].start()

        @when_outer
        def _():
            relay[j][i].wait_recv()

        x_far[c, i].start()

    def stage_r(j):
        @when_inner
        def _():
            far_in[j][0].wait_recv()
            relay[j][0].start()

    def stage_b(c, i):
        if c == "O":
            own_arrived((i, i + 1))
        elif c == "N":
            near[0][i].wait_recv()
            near[1][i].wait_recv()
        else:
            x_far[c, i].wait_recv()
        c_in[c, i].start()

    def stage_c(c, i):
        c_in[c, i].wait_recv()
        u = number[c, i]
        held = rows_of(c, i)

        @pl.loop(0, hidden // tile)
        def _(n):
            cols = pl.ds(pl.multiple_of(n * tile, tile), tile)
            block = held[...].reshape(4 * size, width)
            gate = jnp.dot(block, gate_ref[:, cols], preferred_element_type=f32)
            up = jnp.dot(block, up_ref[:, cols], preferred_element_type=f32)
            act[:, cols] = (gate / (1.0 + jnp.exp(-gate)) * up).astype(b16)

        @pl.loop(0, width // tile_out)
        def _(n):
            cols = pl.ds(pl.multiple_of(n * tile_out, tile_out), tile_out)
            summed = jnp.dot(act[...], down_ref[:, cols], preferred_element_type=f32)
            part[u, :, :, cols] = summed.astype(b16).reshape(4, size, tile_out)

        c_out[c, i].start()

    def stage_d(c, i):
        c_out[c, i].wait_recv()
        u = number[c, i]
        to_x[u] = (part[u, 1].astype(f32) + from_core[u, 1].astype(f32)).astype(b16)
        x_out[c, i].start()

    def stage_e(c, i):
        x_out[c, i].wait_recv()
        u = number[c, i]
        summed = (
            part[u, 0].astype(f32) + from_core[u, 0].astype(f32) + from_x[u].astype(f32)
        ).astype(b16)
        if c == "O":
            oback[i] = summed
            return
        total[u] = summed
        if c == "N":
            near_back[i].start()
            return
        j = int(c[1])
        when_outer(far_over[j][i].start)
        if i == wide - 1:
            when_inner(far_back(j, wide).start)

    def stage_g(j, p):
        if p > 0 and j not in scaled:
            scaled.add(j)
            when_inner(scale_in[j].wait_recv)

        @when_inner
        def _():
            far_over[j][p].wait_recv()
            if p > 0:
                spot = pl.ds((p - 1) * size, size)
                end_scale = sc[j, spot, 0:1]
                mid_scale = sc[j, spot, sc.shape[2] // 2 : sc.shape[2] // 2 + 1]
                comb[j, p - 1] = (
                    end_scale * fres[j, p].astype(f32)
                    + mid_scale * total[(2 + j) * wide + p - 1].astype(f32)
                ).astype(b16)
            far_back(j, p).start()

    def stage_kv(step):
        if step == 0:
            for n in range(4, 9):
                loads[n].wait()
            kv[0, 0] = turned(keyraw_ref[...], kgain_ref)
            kv_near.start()
        elif step == 1:
            kv_near.wait_recv()
            when_inner(kv_mid.start)
        else:

            @when_inner
            def _():
                kv_mid.wait_recv()
                kv_far.start()

    def stage_att(head):
        if head == 0:
            loads[9].wait()
            loads[10].wait()
            when_outer(kv_far.wait_recv)
        cols = slice(head * dim, (head + 1) * dim)
        held = steps * length
        queries = turned(query_ref[:, cols], qgain_ref)
        keys = kv[:, 0].reshape(held, dim)
        scores = (
            lax.dot_general(
                queries, keys, (((1,), (1,)), ((), ())), preferred_element_type=f32
            )
            * dim ** (-0.5)
        )
        probs = jnp.exp(scores - jnp.max(scores, axis=-1, keepdims=True))
        amount = jnp.sum(probs, axis=-1, keepdims=True)
        summed = jnp.dot(
            probs.astype(b16), kv[:, 1].reshape(held, dim), preferred_element_type=f32
        )
        heads_ref[:, cols] = (summed / amount).astype(b16)

    def stage_outp():
        loads[14].wait()

        @pl.loop(0, width // tile_out)
        def _(i):
            cols = pl.ds(pl.multiple_of(i * tile_out, tile_out), tile_out)
            summed = jnp.dot(heads_ref[...], proj_ref[:, cols], preferred_element_type=f32)
            pm[:, :, cols] = summed.astype(b16).reshape(4, length // 4, tile_out)

        for copy in m_core:
            copy.start()

    def stage_mx(step):
        if step == 0:
            for copy in m_core:
                copy.wait_recv()
            to_xm[...] = (pm[across].astype(f32) + fc[1].astype(f32)).astype(b16)
            m_x.start()
        else:
            m_x.wait_recv()
            mixed_ref[...] = (
                pm[lane].astype(f32) + fc[0].astype(f32) + from_xm[...].astype(f32)
            ).astype(b16)
            mixed_out.start()

    def stage_pre():
        spot = lax.broadcasted_iota(jnp.int32, (count, count), 1).astype(f32)
        for r in range(4):
            pick[r] = (spot == lut[:, r : r + 1]).astype(b16)

    def stage_cmb():
        for i in window:
            near_back[i].wait_recv()
        for p in range(blocks):
            far_back(0, p).wait_recv()
        for n in range(width // tile_out):
            cols = slice(n * tile_out, (n + 1) * tile_out)
            found = jnp.zeros((count, tile_out), f32)
            for r, store in enumerate((oback, nback, fback, fback)):
                depth = store.shape[0] * size
                results = store[:, :, cols].reshape(depth, tile_out)
                chosen = pick[r, :, :depth]
                found += lut[:, 4 + r : 5 + r] * jnp.dot(
                    chosen, results, preferred_element_type=f32
                )
            expert_ref[:, cols] = found.astype(b16)
            expert_out[n].start()

    stages = {"A": stage_a, "B": stage_b, "C": stage_c, "D": stage_d, "E": stage_e}
    loaded = False
    for name in ORDER:
        if name == "SEND":
            stage_send()
        elif name[:2] == "KV":
            stage_kv(int(name[2]))
        elif name[:3] == "ATT":
            stage_att(int(name[3]))
        elif name == "OUTP":
            stage_outp()
        elif name[:2] == "MX":
            stage_mx(int(name[2]))
        elif name == "PRE":
            stage_pre()
        elif name == "CMB":
            stage_cmb()
        elif name[0] == "Y":
            stage_y(int(name[1]))
        elif name[0] == "R":
            stage_r(int(name[2]))
        elif name[0] == "G":
            stage_g(int(name[2]), int(name[3]))
        else:
            if name[0] == "C" and not loaded:
                loaded = True
                for n in (11, 12, 13):
                    loads[n].wait()
            stages[name[0]](name[1:-1], int(name[-1]))

    for p in range(blocks):
        x_own(p).wait_send()
        far[p].wait_send()
    for table in (x_far, c_in, c_out, x_out):
        for copy in table.values():
            copy.wait_send()
    for i in window:
        near[0][i].wait_send()
        near[1][i].wait_send()
        near_back[i].wait_send()
    scale_out.wait_send()
    kv_near.wait_send()

    @when_inner
    def _():
        kv_mid.wait_send()
        kv_far.wait_send()
        for j in range(2):
            for i in window:
                relay[j][i].wait_send()
            for p in range(blocks):
                far_back(j, p).wait_send()

    @when_outer
    def _():
        for j in range(2):
            for i in window:
                far_over[j][i].wait_send()

    for copy in m_core:
        copy.wait_send()
    m_x.wait_send()
    mixed_out.wait()
    for copy in expert_out:
        copy.wait()


def deliver_kernel(mixed_in, expert_in, mixed_out, expert_out, mixed_held, expert_held, sems):
    pairs = []
    for source, held, target, pieces in (
        (expert_in, expert_held, expert_out, 4),
        (mixed_in, mixed_held, mixed_out, 1),
    ):
        size = source.shape[0] // pieces
        for n in range(pieces):
            spot = pl.ds(n * size, size)
            at = len(pairs)
            pairs.append(
                (
                    pltpu.make_async_copy(source.at[spot], held.at[spot], sems.at[0, at]),
                    pltpu.make_async_copy(held.at[spot], target.at[spot], sems.at[1, at]),
                )
            )
    for fetch, _ in pairs:
        fetch.start()
    for fetch, store in pairs:
        fetch.wait()
        store.start()
    for _, store in pairs:
        store.wait()


def turn_tables(held, dim):
    quarter = dim // 4
    freqs = 1.0 / THETA ** (np.arange(quarter) * 4.0 / dim)
    spots = np.arange(held)
    tables = []
    for place in (spots // GRID_W, spots % GRID_W):
        angles = place[:, None] * freqs
        tables.append((np.cos(angles), np.sin(angles)))
    cosine = np.concatenate([tables[0][0]] * 2 + [tables[1][0]] * 2, axis=1)
    sine = np.concatenate(
        [-tables[0][1], tables[0][1], -tables[1][1], tables[1][1]], axis=1
    )
    return jnp.asarray(cosine, jnp.float32), jnp.asarray(sine, jnp.float32)


def fused(
    query_rows,
    projected_keys,
    projected_values,
    query_gain,
    key_norm_gain,
    out_proj,
    mix_tokens,
    norm_gain,
    expert_ids,
    expert_score,
    gate_proj,
    up_proj,
    down_proj,
):
    steps, lanes = lax.axis_size("ep"), lax.axis_size("tp")
    count, width = mix_tokens.shape
    cap = count * expert_ids.shape[1] * 3 // (2 * steps)
    size = count - cap
    blocks = count // size
    wide = blocks - 1
    hidden = gate_proj.shape[2]
    length, dim = projected_keys.shape
    kind = jnp.bfloat16
    cosine, sine = turn_tables(steps * length, dim)
    anywhere = pl.BlockSpec(memory_space=pltpu.HBM)
    units = 4 * wide
    mixed, expert = pl.pallas_call(
        functools.partial(fused_kernel, steps),
        out_shape=(
            jax.ShapeDtypeStruct((length // lanes, width), kind),
            jax.ShapeDtypeStruct((count, width), kind),
        ),
        in_specs=[anywhere] * 15,
        out_specs=(anywhere, anywhere),
        scratch_shapes=[
            pltpu.VMEM((2, count), jnp.int32),
            pltpu.VMEM((2, count), jnp.float32),
            pltpu.VMEM((1, width), jnp.float32),
            pltpu.VMEM((1, dim), jnp.float32),
            pltpu.VMEM((1, dim), jnp.float32),
            pltpu.VMEM((length // lanes, width), kind),
            pltpu.VMEM((count, width), kind),
            pltpu.VMEM((4, count, count), kind),
            pltpu.VMEM((width, hidden), kind),
            pltpu.VMEM((width, hidden), kind),
            pltpu.VMEM((hidden, width), kind),
            pltpu.VMEM(out_proj.shape, kind),
            pltpu.VMEM(query_rows.shape, kind),
            pltpu.VMEM((length, dim), kind),
            pltpu.VMEM((length, dim), jnp.float32),
            pltpu.VMEM((length, dim), jnp.float32),
            pltpu.VMEM((count, width), kind),
            pltpu.VMEM((count, width), kind),
            pltpu.VMEM((blocks, size, width), kind),
            pltpu.VMEM((size * (wide - 1), 128), jnp.float32),
            pltpu.VMEM((2, size * (wide - 1), 128), jnp.float32),
            pltpu.VMEM((blocks, 4, size, width), kind),
            pltpu.VMEM((wide, 4, size, width), kind),
            pltpu.VMEM((2, blocks, 4, size, width), kind),
            pltpu.VMEM((4 * size, hidden), kind),
            pltpu.VMEM((units, 4, size, width), kind),
            pltpu.VMEM((units, 2, size, width), kind),
            pltpu.VMEM((units, size, width), kind),
            pltpu.VMEM((units, size, width), kind),
            pltpu.VMEM((units, size, width), kind),
            pltpu.VMEM((2, wide, size, width), kind),
            pltpu.VMEM((2, wide - 1, size, width), kind),
            pltpu.VMEM((wide, size, width), kind),
            pltpu.VMEM((wide, size, width), kind),
            pltpu.VMEM((blocks, size, width), kind),
            pltpu.VMEM((count, count), jnp.float32),
            pltpu.VMEM((steps, 2, length, dim), kind),
            pltpu.VMEM(query_rows.shape, kind),
            pltpu.VMEM((lanes, length // lanes, width), kind),
            pltpu.VMEM((2, length // lanes, width), kind),
            pltpu.VMEM((length // lanes, width), kind),
            pltpu.VMEM((length // lanes, width), kind),
            pltpu.SemaphoreType.DMA((15,)),
            pltpu.SemaphoreType.DMA((1 + width // math.gcd(width, 512),)),
        ]
        + [pltpu.SemaphoreType.DMA((2 * blocks,))] * 6
        + [pltpu.SemaphoreType.DMA((blocks + 2 * wide,))] * 2
        + [pltpu.SemaphoreType.DMA((units,))] * 6
        + [pltpu.SemaphoreType.DMA((2 * blocks,))] * 6
        + [pltpu.SemaphoreType.DMA((3,))] * 6,
        compiler_params=pltpu.CompilerParams(
            collective_id=0, has_side_effects=True, vmem_limit_bytes=VMEM_LIMIT
        ),
    )(
        mix_tokens,
        expert_ids.T,
        expert_score.T,
        norm_gain.reshape(1, width),
        gate_proj.reshape(gate_proj.shape[1:]),
        up_proj.reshape(up_proj.shape[1:]),
        down_proj.reshape(down_proj.shape[1:]),
        out_proj,
        query_rows,
        projected_keys,
        projected_values,
        query_gain.reshape(1, dim),
        key_norm_gain.reshape(1, dim),
        cosine,
        sine,
    )
    return pl.pallas_call(
        deliver_kernel,
        out_shape=(
            jax.ShapeDtypeStruct(mixed.shape, kind),
            jax.ShapeDtypeStruct(expert.shape, kind),
        ),
        in_specs=[anywhere] * 2,
        out_specs=(anywhere, anywhere),
        scratch_shapes=[
            pltpu.VMEM(mixed.shape, kind),
            pltpu.VMEM(expert.shape, kind),
            pltpu.SemaphoreType.DMA((2, 5)),
        ],
    )(mixed, expert)


def fits_fused(query_rows, projected_keys, query_gain, mix_tokens, expert_ids, gate_proj):
    steps, lanes = lax.axis_size("ep"), lax.axis_size("tp")
    count, width = mix_tokens.shape
    length, dim = projected_keys.shape
    local_experts, _, hidden = gate_proj.shape
    cap = count * expert_ids.shape[1] * 3 // (2 * steps)
    blocks = 20 * steps * cap * width * 2 + 4 * width * hidden * 2
    return (
        lanes == 4
        and steps == 4
        and local_experts == 1
        and expert_ids.shape[1] == 2
        and dim == query_gain.shape[0]
        and dim % 128 == 0
        and length % 64 == 0
        and length <= 256
        and count == 128
        and cap < count
        and (count - cap) % 16 == 0
        and cap % (count - cap) == 0
        and 2 * cap > count
        and blocks < 48 * 1024 * 1024
    )


def local(
    query_rows,
    projected_keys,
    projected_values,
    query_gain,
    key_norm_gain,
    out_proj,
    mix_tokens,
    norm_gain,
    expert_ids,
    expert_score,
    gate_proj,
    up_proj,
    down_proj,
):
    simple = fits_fused(
        query_rows, projected_keys, query_gain, mix_tokens, expert_ids, gate_proj
    )
    return (fused if simple else plain_halves)(
        query_rows,
        projected_keys,
        projected_values,
        query_gain,
        key_norm_gain,
        out_proj,
        mix_tokens,
        norm_gain,
        expert_ids,
        expert_score,
        gate_proj,
        up_proj,
        down_proj,
    )


def solution(mesh):
    in_specs = (
        P(("grp", "ep"), "tp"),
        P(("grp", "ep"), "tp"),
        P(("grp", "ep"), "tp"),
        P(),
        P(),
        P("tp", None),
        P(("grp", "ep", "tp"), None),
        P(),
        P(("grp", "ep", "tp"), None),
        P(("grp", "ep", "tp"), None),
        P("ep", None, "tp"),
        P("ep", None, "tp"),
        P("ep", "tp", None),
    )
    out_specs = (P(("grp", "ep", "tp"), None), P(("grp", "ep", "tp"), None))
    return jax.shard_map(local, mesh=mesh, in_specs=in_specs, out_specs=out_specs, check_vma=False)
```

```python
import functools
import math

import jax
import jax.numpy as jnp
import numpy as np
from jax import lax
from jax.experimental import pallas as pl
from jax.experimental.pallas import tpu as pltpu
from jax.sharding import PartitionSpec as P

GRID_W = 64


MESH = pl.DeviceIdType.MESH
EPS = 1e-06
THETA = 10000.0


def head_norm(vectors, gain):
    return vectors * lax.rsqrt(jnp.mean(vectors * vectors, axis=-1, keepdims=True) + EPS) * gain


def rotate_grid(vectors, token_positions):
    length, heads, head_dim = vectors.shape
    quarter = head_dim // 4
    freqs = 1.0 / THETA ** (jnp.arange(quarter, dtype=jnp.float32) * 4.0 / head_dim)
    grid_row = (token_positions // GRID_W).astype(jnp.float32)
    grid_col = (token_positions % GRID_W).astype(jnp.float32)
    angles = jnp.stack([grid_row[:, None] * freqs, grid_col[:, None] * freqs], axis=1)
    cosine = jnp.cos(angles)[:, None]
    sine = jnp.sin(angles)[:, None]
    halves = vectors.reshape(length, heads, 2, 2, quarter)
    first = halves[..., 0, :]
    second = halves[..., 1, :]
    turned = jnp.stack([first * cosine - second * sine, second * cosine + first * sine], axis=-2)
    return turned.reshape(length, heads, head_dim)


def prepare_inputs(raw_rows, gain, heads, token_positions):
    length = raw_rows.shape[0]
    head_dim = gain.shape[0]
    vectors = raw_rows.astype(jnp.float32).reshape(length, heads, head_dim)
    return rotate_grid(head_norm(vectors, gain), token_positions).astype(jnp.bfloat16)


def mixer_prepare(query_rows, projected_keys, projected_values, query_gain, key_norm_gain):
    length = query_rows.shape[0]
    head_dim = query_gain.shape[0]
    kv_heads = projected_keys.shape[1] // head_dim
    q_heads = query_rows.shape[1] // head_dim
    token_positions = lax.axis_index("ep") * length + jnp.arange(length, dtype=jnp.int32)
    query_matrix = prepare_inputs(query_rows, query_gain, q_heads, token_positions).reshape(
        length, q_heads * head_dim
    )
    keys_turned = prepare_inputs(projected_keys, key_norm_gain, kv_heads, token_positions).reshape(
        length, kv_heads * head_dim
    )
    return query_matrix, jnp.concatenate([keys_turned, projected_values], axis=1)


def attend_plain(query_matrix, own_pair, head_dim):
    length = query_matrix.shape[0]
    kv_heads = own_pair.shape[1] // (2 * head_dim)
    q_heads = query_matrix.shape[1] // head_dim
    queries_per_group = q_heads // kv_heads
    query_matrix = query_matrix.reshape(length, kv_heads, queries_per_group, head_dim)
    score_scale = head_dim ** (-0.5)
    initial = (
        jnp.full((kv_heads, queries_per_group, length), -1e30, jnp.float32),
        jnp.zeros((kv_heads, queries_per_group, length), jnp.float32),
        jnp.zeros((length, kv_heads, queries_per_group, head_dim), jnp.float32),
    )
    width = kv_heads * head_dim
    pair = lax.all_gather(own_pair, "ep", axis=0, tiled=True)
    key_piece = pair[:, :width]
    value_piece = pair[:, width:]
    piece_rows = key_piece.shape[0]
    step_rows = math.gcd(piece_rows, 1024)

    def one_block(block_index, running):
        run_max, run_sum, run_acc = running
        offset = block_index * step_rows
        key_block = lax.dynamic_slice_in_dim(key_piece, offset, step_rows, 0).reshape(
            step_rows, kv_heads, head_dim
        )
        value_block = lax.dynamic_slice_in_dim(value_piece, offset, step_rows, 0).reshape(
            step_rows, kv_heads, head_dim
        )
        scores = (
            jnp.einsum(
                "tkgd,skd->kgts", query_matrix, key_block, preferred_element_type=jnp.float32
            )
            * score_scale
        )
        new_max = jnp.maximum(run_max, jnp.max(scores, axis=-1))
        factor = jnp.exp(run_max - new_max)
        weights = jnp.exp(scores - new_max[..., None])
        run_sum = run_sum * factor + jnp.sum(weights, axis=-1)
        update = jnp.einsum(
            "kgts,skd->tkgd",
            weights.astype(jnp.bfloat16),
            value_block,
            preferred_element_type=jnp.float32,
        )
        run_acc = run_acc * jnp.transpose(factor, (2, 0, 1))[..., None] + update
        return (new_max, run_sum, run_acc)

    run_max, run_sum, run_acc = lax.fori_loop(0, piece_rows // step_rows, one_block, initial)
    return (
        (run_acc / jnp.transpose(run_sum, (2, 0, 1))[..., None])
        .astype(jnp.bfloat16)
        .reshape(length, q_heads * head_dim)
    )


def flip(index, bits):
    result, place = 0, 1
    for _ in range(8):
        mine = (index // place) % 2
        result = result + place * ((1 - mine) if bits & place else mine)
        place *= 2
    return result


def exchange_plain(outgoing, gate_proj, up_proj, down_proj):
    rows_in = lax.all_gather(
        lax.all_to_all(outgoing, "ep", split_axis=0, concat_axis=0, tiled=True),
        "tp",
        axis=0,
        tiled=True,
    )
    gate_out = jnp.einsum("secd,edf->secf", rows_in, gate_proj, preferred_element_type=jnp.float32)
    up_out = jnp.einsum("secd,edf->secf", rows_in, up_proj, preferred_element_type=jnp.float32)
    active = (jax.nn.silu(gate_out) * up_out).astype(jnp.bfloat16)
    summed = lax.psum_scatter(
        jnp.einsum("secf,efd->secd", active, down_proj, preferred_element_type=jnp.float32).astype(
            jnp.bfloat16
        ),
        "tp",
        scatter_dimension=0,
        tiled=True,
    )
    return lax.all_to_all(summed, "ep", split_axis=0, concat_axis=0, tiled=True)


def plain_halves(
    query_rows,
    projected_keys,
    projected_values,
    query_gain,
    key_norm_gain,
    out_proj,
    mix_tokens,
    norm_gain,
    expert_ids,
    expert_score,
    gate_proj,
    up_proj,
    down_proj,
):
    length, model_dim = mix_tokens.shape
    top_count = expert_ids.shape[1]
    local_experts = gate_proj.shape[0]
    expert_axis = lax.axis_size("ep")
    experts_all = expert_axis * local_experts
    capacity = length * top_count * 3 // (2 * experts_all)
    values_b = mix_tokens.astype(jnp.float32)
    normed = (
        values_b
        * lax.rsqrt(jnp.mean(values_b * values_b, axis=-1, keepdims=True) + EPS)
        * norm_gain
    ).astype(jnp.bfloat16)
    flat = expert_ids.reshape(length * top_count)
    onehot = (flat[:, None] == jnp.arange(experts_all, dtype=jnp.int32)).astype(jnp.int32)
    slots = jnp.sum((jnp.cumsum(onehot, axis=0) - onehot) * onehot, axis=1)
    target = flat * capacity + slots
    placed = (target[:, None] == jnp.arange(experts_all * capacity, dtype=jnp.int32)).astype(
        jnp.int32
    )
    placed = jnp.sum(placed.reshape(length, top_count, experts_all * capacity), axis=1).astype(
        jnp.bfloat16
    )
    outgoing = jnp.einsum("re,rd->ed", placed, normed, preferred_element_type=jnp.float32).astype(
        jnp.bfloat16
    )
    outgoing = outgoing.reshape(expert_axis, local_experts, capacity, model_dim)
    lanes = lax.axis_size("tp")
    head_dim = query_gain.shape[0]
    queries, pair = mixer_prepare(
        query_rows, projected_keys, projected_values, query_gain, key_norm_gain
    )
    heads_out = attend_plain(queries, pair, head_dim)
    returned = exchange_plain(outgoing, gate_proj, up_proj, down_proj)
    head_partial = jnp.dot(heads_out, out_proj, preferred_element_type=jnp.float32).astype(
        jnp.bfloat16
    )
    pieces = lax.all_to_all(
        head_partial.reshape(lanes, -1, head_partial.shape[1]),
        "tp",
        split_axis=0,
        concat_axis=0,
        tiled=True,
    )
    mixed_rows = jnp.sum(pieces.astype(jnp.float32), axis=0).astype(jnp.bfloat16)
    results = returned.reshape(experts_all * capacity, model_dim)
    first_weight = jax.nn.sigmoid(expert_score[:, 0] - expert_score[:, 1])
    picks = target.reshape(length, top_count)
    chosen = [
        jnp.dot(
            (picks[:, k : k + 1] == jnp.arange(experts_all * capacity, dtype=jnp.int32)).astype(
                jnp.bfloat16
            ),
            results,
            preferred_element_type=jnp.float32,
        )
        for k in range(2)
    ]
    combined = first_weight[:, None] * chosen[0] + (1.0 - first_weight)[:, None] * chosen[1]
    return (mixed_rows, combined.astype(jnp.bfloat16))


ORDER = (
    "SEND", "RF1", "BO2", "AF10", "CO2", "RF0", "AF11", "BF10", "AF00",
    "BF11", "KV0", "PRE", "AF12", "CF11", "BO0", "AF01", "BF00", "CF10",
    "DF11", "Y0", "KV1", "CF00", "Y1", "Y2", "BF01", "DF10", "BF12",
    "CO0", "DF00", "AF02", "CF01", "BN0", "EF11", "CF12", "BN1", "CN0",
    "KV2", "EF00", "DF01", "DF12", "CN1", "EF10", "GF11", "BF02", "BN2",
    "DO2", "EF01", "BO1", "GF00", "DN0", "DN1", "CF02", "GF10", "DF02",
    "EF12", "CN2", "ATT0", "GF01", "DN2", "EN1", "CO1", "ATT1", "ATT2",
    "EF02", "ATT3", "DO0", "OUTP", "DO1", "EN2", "EN0", "GF12", "EO2",
    "GF02", "EO0", "MX0", "EO1", "CMBP", "CMB", "MX1",
)
SENDS = (
    ("X", 2), ("X", 3), ("N", 2), ("F", 0), ("F", 1),
    ("F", 2), ("N", 1), ("F", 3), ("X", 1), ("N", 0), ("X", 0),
)
SHARED_PIECE = 1
VMEM_LIMIT = 58 * 1024 * 1024


def fused_kernel(
    steps,
    tokens_hbm,
    ids_hbm,
    score_hbm,
    ngain_hbm,
    gate_hbm,
    up_hbm,
    down_hbm,
    proj_hbm,
    query_hbm,
    key_hbm,
    value_hbm,
    qgain_hbm,
    kgain_hbm,
    cos_hbm,
    sin_hbm,
    mixed_hbm,
    expert_hbm,
    ids_ref,
    score_ref,
    ngain_ref,
    qgain_ref,
    kgain_ref,
    mixed_ref,
    expert_ref,
    pick,
    gate_ref,
    up_ref,
    down_ref,
    proj_ref,
    query_ref,
    keyraw_ref,
    cos_ref,
    sin_ref,
    tok_ref,
    norm_ref,
    outf,
    scl,
    sc,
    own_scl,
    x_scl,
    near_two,
    near_got,
    own_sum,
    orows,
    nrows,
    frows,
    act,
    part,
    from_core,
    to_x,
    from_x,
    total,
    fres,
    comb,
    oback,
    nback,
    fback,
    acc,
    lut,
    kv,
    heads_ref,
    pm,
    fc,
    to_xm,
    from_xm,
    hsem,
    osem,
    near_s,
    near_r,
    far_s,
    far_r,
    rel_s,
    rel_r,
    xs,
    xr,
    cs,
    cr,
    ps,
    pr,
    qs,
    qr,
    nb_s,
    nb_r,
    fo_s,
    fo_r,
    fb_s,
    fb_r,
    sc_s,
    sc_r,
    ns_s,
    ns_r,
    ks,
    kr,
    ms,
    mr,
):
    me = lax.axis_index("ep")
    lane = lax.axis_index("tp")
    peers = [flip(me, k) for k in range(steps)]
    core, across = flip(lane, 1), flip(lane, 2)
    inner = ((me + 1) // 2) % 2
    outer = 1 - inner
    gate_at = 2 - me // 2
    sources = [3 - me, flip(3 - me, 1)]
    blocks, _, size, width = orows.shape
    wide = blocks - 1
    hidden = gate_ref.shape[1]
    length = query_ref.shape[0]
    dim = keyraw_ref.shape[1]
    count = tok_ref.shape[0]
    tile = math.gcd(hidden, 256)
    tile_out = math.gcd(width, 512)
    f32, b16 = jnp.float32, jnp.bfloat16

    offset = pl.multiple_of(me * length, 16)
    loads = [
        pltpu.make_async_copy(s, d, hsem.at[i])
        for i, (s, d) in enumerate(
            [
                (ids_hbm, ids_ref),
                (score_hbm, score_ref),
                (ngain_hbm, ngain_ref),
                (kgain_hbm, kgain_ref),
                (key_hbm, keyraw_ref),
                (value_hbm, kv.at[0, 1]),
                (cos_hbm.at[pl.ds(offset, length)], cos_ref),
                (sin_hbm.at[pl.ds(offset, length)], sin_ref),
                (qgain_hbm, qgain_ref),
                (query_hbm, query_ref),
                (gate_hbm, gate_ref),
                (up_hbm, up_ref),
                (down_hbm, down_ref),
                (proj_hbm, proj_ref),
            ]
        )
    ]
    spots = [pl.ds(n * size, size) for n in range(blocks)]
    pieces = [
        pltpu.make_async_copy(tokens_hbm.at[spot], tok_ref.at[spot], hsem.at[len(loads) + n])
        for n, spot in enumerate(spots)
    ]
    for load in loads[:3] + pieces + loads[3:]:
        load.start()

    barrier = pltpu.get_barrier_semaphore()
    friends = [{"ep": me, "tp": core}, {"ep": me, "tp": across}]
    friends += [{"ep": peers[k], "tp": lane} for k in (1, 2)]

    def greet(friend):
        pl.semaphore_signal(barrier, inc=1, device_id=friend, device_id_type=MESH)

    @pl.when(inner == 1)
    def _():
        greet({"ep": peers[3], "tp": lane})

    for friend in friends:
        greet(friend)

    def remote(src, dst, send, recv, ep_to, tp_to):
        return pltpu.make_async_remote_copy(
            src_ref=src,
            dst_ref=dst,
            send_sem=send,
            recv_sem=recv,
            device_id={"ep": ep_to, "tp": tp_to},
            device_id_type=MESH,
        )

    def when_inner(body):
        pl.when(inner == 1)(body)

    def when_outer(body):
        pl.when(inner == 0)(body)

    kinds = ("O", "N", "F0", "F1")
    window = range(wide)
    number = {(c, i): n * wide + i for n, c in enumerate(kinds) for i in window}

    def by_role(i, special, usual):
        if i == SHARED_PIECE - 1:
            when_inner(special)
            when_outer(usual)
        elif i == SHARED_PIECE:
            when_outer(special)
            when_inner(usual)
        else:
            usual()

    def rows_of(c, i):
        if c == "O":
            return orows.at[i + inner]
        if c == "N":
            return nrows.at[i]
        return frows.at[int(c[1]), i + inner]

    def x_own(p):
        return remote(orows.at[p, 0], orows.at[p, 1], xs.at[0], xr.at[p], me, across)

    near = [
        [
            remote(
                orows.at[i + outer, n],
                nrows.at[i, n],
                near_s.at[0],
                near_r.at[n * wide + i],
                peers[1],
                lane,
            )
            for i in window
        ]
        for n in range(2)
    ]
    far = [
        remote(
            outf.at[p],
            frows.at[outer, p, 0],
            far_s.at[0],
            far_r.at[outer * blocks + p],
            gate_at,
            lane,
        )
        for p in range(blocks)
    ]
    far_in = [
        [
            remote(
                outf.at[p], frows.at[j, p, 0], far_s.at[0], far_r.at[j * blocks + p], gate_at, lane
            )
            for p in range(blocks)
        ]
        for j in range(2)
    ]
    relay = [
        [
            remote(
                frows.at[j, p, 0],
                frows.at[j, p, 0],
                rel_s.at[0],
                rel_r.at[j * wide + p],
                peers[1],
                lane,
            )
            for p in window
        ]
        for j in range(2)
    ]
    scale_out = remote(scl, sc.at[outer], sc_s.at[0], sc_r.at[outer], gate_at, lane)
    scale_in = [remote(scl, sc.at[j], sc_s.at[0], sc_r.at[j], gate_at, lane) for j in range(2)]
    x_far, c_in, c_out, x_out = {}, {}, {}, {}
    for (c, i), u in number.items():
        held = rows_of(c, i)
        if c[0] == "F":
            at = blocks + u - 2 * wide
            x_far[c, i] = remote(held.at[0], held.at[1], xs.at[0], xr.at[at], me, across)
        c_in[c, i] = remote(
            held.at[pl.ds(0, 2)], held.at[pl.ds(2, 2)], cs.at[0], cr.at[u], me, core
        )
        c_out[c, i] = remote(
            part.at[u, pl.ds(2, 2)], from_core.at[u], ps.at[0], pr.at[u], me, core
        )
        x_out[c, i] = remote(to_x.at[u], from_x.at[u], qs.at[0], qr.at[u], me, across)
    near_back = [
        remote(total.at[wide + i], nback.at[i], nb_s.at[0], nb_r.at[i], peers[1], lane)
        for i in window
    ]
    near_sum = remote(near_two, near_got, ns_s.at[0], ns_r.at[0], peers[1], lane)
    own_scale = remote(own_scl, x_scl, ns_s.at[1], ns_r.at[1], me, across)
    far_over = [
        [
            remote(
                total.at[(2 + j) * wide + i],
                fres.at[j, i],
                fo_s.at[0],
                fo_r.at[j * wide + i],
                peers[1],
                lane,
            )
            for i in window
        ]
        for j in range(2)
    ]

    def far_back(j, p):
        if p == 0:
            source = fres.at[j, 0]
        elif p == wide:
            source = total.at[(2 + j) * wide + wide - 1]
        else:
            source = comb.at[j, p - 1]
        return remote(
            source, fback.at[p], fb_s.at[0], fb_r.at[p], sources[j], lane
        )

    kv_near = remote(kv.at[0], kv.at[1], ks.at[0], kr.at[0], peers[1], lane)
    kv_mid = remote(kv.at[pl.ds(0, 2)], kv.at[pl.ds(2, 2)], ks.at[1], kr.at[1], peers[3], lane)
    kv_far = remote(kv.at[pl.ds(2, 2)], kv.at[pl.ds(2, 2)], ks.at[2], kr.at[2], peers[1], lane)
    m_core = [
        remote(pm.at[core], fc.at[0], ms.at[0], mr.at[0], me, core),
        remote(pm.at[flip(core, 2)], fc.at[1], ms.at[0], mr.at[1], me, core),
    ]
    m_x = remote(to_xm, from_xm, ms.at[1], mr.at[2], me, across)
    mixed_out = pltpu.make_async_copy(mixed_ref, mixed_hbm, osem.at[0])
    expert_out = [
        pltpu.make_async_copy(
            expert_ref.at[:, pl.ds(n * tile_out, tile_out)],
            expert_hbm.at[:, pl.ds(n * tile_out, tile_out)],
            osem.at[1 + n],
        )
        for n in range(width // tile_out)
    ]

    loads[0].wait()
    loads[1].wait()

    token_row = lax.broadcasted_iota(jnp.int32, (count, count), 0)
    token_col = lax.broadcasted_iota(jnp.int32, (count, count), 1)
    earlier = (token_row < token_col).astype(b16)
    first, second = ids_ref[0:1, :], ids_ref[1:2, :]
    weight = 1.0 / (1.0 + jnp.exp(score_ref[1:2, :] - score_ref[0:1, :]))
    table_row = lax.broadcasted_iota(jnp.int32, (8, count), 0)
    high = me // 2
    ends = (3 * high, 3 - 3 * high)
    middles = (1 + high, 2 - high)

    def naming(expert):
        one, two = first == expert, second == expert
        share = jnp.where(one, weight, 0.0) + jnp.where(two, 1.0 - weight, 0.0)
        return jnp.where(one | two, 1.0, 0.0), share

    named = [(naming(ends[n]), naming(middles[n])) for n in range(2)]
    counted = jnp.zeros((8, count), f32)
    parts_of = []
    for n in range(2):
        (end_one, _), (mid_one, _) = named[n]
        both = end_one * mid_one
        parts_of.append((end_one - both, mid_one - both, both))
        for r in range(3):
            counted = jnp.where(table_row == 3 * n + r, parts_of[n][r], counted)
    rank = jnp.dot(counted.astype(b16), earlier, preferred_element_type=f32)
    sums = jnp.sum(counted, axis=1, keepdims=True)
    tail, middle = float(size), float(size * (wide - 1))

    def positions(n):
        end_only, mid_only, both = parts_of[n]
        end_rank, mid_rank, both_rank = (rank[3 * n + r : 3 * n + r + 1, :] for r in range(3))
        end_sum, both_sum = sums[3 * n : 3 * n + 1, :], sums[3 * n + 2 : 3 * n + 3, :]
        extra = jnp.maximum(both_sum - middle, 0.0)
        common = tail + jnp.minimum(both_sum, middle)
        end_at, mid_at = end_rank + extra, mid_rank + extra
        spill = jnp.maximum(end_sum + extra - tail, 0.0)
        shared = both_rank < middle
        end_pos = jnp.where(
            both > 0.5,
            jnp.where(shared, tail + both_rank, both_rank - middle),
            jnp.where(end_at < tail, end_at, common + end_at - tail),
        )
        mid_pos = jnp.where(
            both > 0.5,
            tail + both_rank,
            jnp.where(
                mid_at < tail, tail + middle + mid_at, common + spill + mid_at - tail
            ),
        )
        end_pos = jnp.where(end_only + both > 0.5, end_pos, -1.0)
        mid_pos = jnp.where(mid_only + both > 0.5, mid_pos, -1.0)
        return end_pos, mid_pos, jnp.where((both > 0.5) & shared, 1.0, 0.0)

    own_end, own_mid, own_shared = positions(0)
    far_end, far_mid, far_shared = positions(1)
    slot = lax.broadcasted_iota(jnp.int32, (count, count), 0).astype(f32)

    def dispatch(end_pos, mid_pos):
        chosen = ((slot == end_pos) | (slot == mid_pos)).astype(b16)
        picked = jnp.dot(chosen, norm_ref[...], preferred_element_type=f32)
        return picked.astype(b16).reshape(blocks, size, width)

    loads[2].wait()
    for n, spot in enumerate(spots):
        pieces[n].wait()
        values = tok_ref[spot, :].astype(f32)
        norm_ref[spot, :] = (
            values
            * lax.rsqrt(jnp.mean(values * values, axis=-1, keepdims=True) + EPS)
            * ngain_ref[...]
        ).astype(b16)
    orows[:, 0] = dispatch(own_end, own_mid)

    @when_inner
    def _():
        pl.semaphore_wait(barrier, len(friends) + 1)

    @when_outer
    def _():
        pl.semaphore_wait(barrier, len(friends))

    for kind, p in SENDS:
        if kind == "X":
            x_own(p).start()
    outf[...] = dispatch(far_end, far_mid)

    def stage_send():
        for kind, p in SENDS:
            if kind == "F":
                far[p].start()
            elif kind == "N":
                near[0][p].start()
        end_share, mid_share = named[1][0][1], named[1][1][1]
        rows_mid = slice(size, size * wide)
        end_scale = jnp.sum(
            jnp.where(
                slot[rows_mid] == far_end, jnp.where(far_shared > 0.5, end_share, 1.0), 0.0
            ),
            axis=1,
            keepdims=True,
        )
        mid_scale = jnp.sum(
            jnp.where(
                slot[rows_mid] == far_mid, jnp.where(far_shared > 0.5, mid_share, 1.0), 0.0
            ),
            axis=1,
            keepdims=True,
        )
        lanes_of = lax.broadcasted_iota(jnp.int32, scl.shape, 1)
        scl[...] = jnp.where(lanes_of < scl.shape[1] // 2, end_scale, mid_scale)
        scale_out.start()
        is_inner = (jnp.zeros((1, count), jnp.int32) + inner) == 1
        own_at = jnp.where(is_inner, own_mid, own_end)
        near_at = jnp.where(is_inner, own_end, own_mid)
        own_share = jnp.where(is_inner, named[0][1][1], named[0][0][1])
        near_share = jnp.where(is_inner, named[0][0][1], named[0][1][1])
        rows_one = slice(size * SHARED_PIECE, size * (SHARED_PIECE + 1))
        own_factor = jnp.sum(
            jnp.where(
                slot[rows_one] == own_at, jnp.where(own_shared > 0.5, own_share, 1.0), 0.0
            ),
            axis=1,
            keepdims=True,
        )
        near_factor = jnp.sum(
            jnp.where(
                slot[rows_one] == near_at, jnp.where(own_shared > 0.5, near_share, 1.0), 0.0
            ),
            axis=1,
            keepdims=True,
        )
        lanes_one = lax.broadcasted_iota(jnp.int32, own_scl.shape, 1)
        own_scl[...] = jnp.where(lanes_one < own_scl.shape[1] // 2, own_factor, near_factor)
        own_scale.start()
        nback[SHARED_PIECE - outer] = jnp.zeros((size, width), b16)
        moved = (near_at >= size * SHARED_PIECE) & (near_at < size * (SHARED_PIECE + 1))
        own_first = jnp.where(is_inner, tail, 0.0)
        own_held = jnp.where(moved, near_at, own_at)
        near_held = jnp.where(moved, -1.0, near_at)
        table = (
            jnp.where(own_held < 0.0, -1.0, own_held - own_first),
            jnp.where(near_held < 0.0, -1.0, near_held - (tail - own_first)),
            far_end,
            jnp.where(far_shared > 0.5, -1.0, far_mid),
            jnp.where(
                moved, jnp.where(own_shared > 0.5, 1.0, near_share), own_share
            ),
            near_share,
            jnp.where(far_shared > 0.5, 1.0, end_share),
            mid_share,
        )
        kept = jnp.zeros((8, count), f32)
        for r in range(8):
            kept = jnp.where(table_row == r, table[r], kept)
        rest = jnp.zeros((count - 8, count), f32)
        lut[...] = jnp.transpose(jnp.concatenate([kept, rest], axis=0))

    turn_lane = lax.broadcasted_iota(jnp.int32, (length, dim), 1)
    leading = (turn_lane // (dim // 4)) % 2 == 0

    def turned(raw, gain):
        vectors = raw.astype(f32)
        vectors = (
            vectors
            * lax.rsqrt(jnp.mean(vectors * vectors, axis=-1, keepdims=True) + EPS)
            * gain[...]
        )
        other = jnp.where(
            leading,
            pltpu.roll(vectors, dim - dim // 4, 1),
            pltpu.roll(vectors, dim // 4, 1),
        )
        return (vectors * cos_ref[...] + other * sin_ref[...]).astype(b16)

    arrived = (set(), set())
    scaled = set()

    def own_arrived(by_role):
        missing = [p not in arrived[r] for r, p in enumerate(by_role)]
        for r, p in enumerate(by_role):
            arrived[r].add(p)
        for r, run in ((0, when_outer), (1, when_inner)):
            if missing[r]:

                @run
                def _(p=by_role[r]):
                    x_own(p).wait_recv()

    def stage_y(i):
        own_arrived((i + 1, i))
        near[1][i].start()

    def stage_a(c, i):
        j = int(c[1])

        @when_inner
        def _():
            far_in[j][i + 1].wait_recv()
            if i + 1 < wide:
                relay[j][i + 1].start()

        @when_outer
        def _():
            relay[j][i].wait_recv()

        x_far[c, i].start()

    def stage_r(j):
        @when_inner
        def _():
            far_in[j][0].wait_recv()
            relay[j][0].start()

    def stage_b(c, i):
        if c == "O":
            own_arrived((i, i + 1))
        elif c == "N":
            near[0][i].wait_recv()
            near[1][i].wait_recv()
        else:
            x_far[c, i].wait_recv()
        c_in[c, i].start()

    def stage_c(c, i):
        c_in[c, i].wait_recv()
        u = number[c, i]
        held = rows_of(c, i)

        @pl.loop(0, hidden // tile)
        def _(n):
            cols = pl.ds(pl.multiple_of(n * tile, tile), tile)
            block = held[...].reshape(4 * size, width)
            gate = jnp.dot(block, gate_ref[:, cols], preferred_element_type=f32)
            up = jnp.dot(block, up_ref[:, cols], preferred_element_type=f32)
            act[:, cols] = (gate / (1.0 + jnp.exp(-gate)) * up).astype(b16)

        @pl.loop(0, width // tile_out)
        def _(n):
            cols = pl.ds(pl.multiple_of(n * tile_out, tile_out), tile_out)
            summed = jnp.dot(act[...], down_ref[:, cols], preferred_element_type=f32)
            part[u, :, :, cols] = summed.astype(b16).reshape(4, size, tile_out)

        c_out[c, i].start()

    def stage_d(c, i):
        c_out[c, i].wait_recv()
        u = number[c, i]

        def usual():
            to_x[u] = (part[u, 1].astype(f32) + from_core[u, 1].astype(f32)).astype(b16)
            x_out[c, i].start()

        def near_special():
            for n in range(2):
                near_two[n] = (
                    part[u, n].astype(f32) + from_core[u, n].astype(f32)
                ).astype(b16)
            near_sum.start()

        def own_special():
            near_sum.wait_recv()
            own_scale.wait_recv()
            half = own_scl.shape[1] // 2
            for n, factors in ((1, x_scl), (0, own_scl)):
                both = factors[:, 0:1] * (
                    part[u, n].astype(f32) + from_core[u, n].astype(f32)
                ) + factors[:, half : half + 1] * near_got[n].astype(f32)
                if n:
                    to_x[u] = both.astype(b16)
                    x_out[c, i].start()
                else:
                    own_sum[...] = both

        if c == "N":
            by_role(i, near_special, usual)
        elif c == "O":
            by_role(i, own_special, usual)
        else:
            usual()

    def stage_e(c, i):
        u = number[c, i]

        def reduced():
            x_out[c, i].wait_recv()
            return (
                part[u, 0].astype(f32)
                + from_core[u, 0].astype(f32)
                + from_x[u].astype(f32)
            ).astype(b16)

        if c == "O":

            def own_special():
                x_out[c, i].wait_recv()
                oback[i] = (own_sum[...] + from_x[u].astype(f32)).astype(b16)

            def own_usual():
                oback[i] = reduced()

            by_role(i, own_special, own_usual)
            return
        if c == "N":

            def near_usual():
                total[u] = reduced()
                near_back[i].start()

            by_role(i, lambda: None, near_usual)
            return
        total[u] = reduced()
        j = int(c[1])
        when_outer(far_over[j][i].start)
        if i == wide - 1:
            when_inner(far_back(j, wide).start)

    def stage_g(j, p):
        if p > 0 and j not in scaled:
            scaled.add(j)
            when_inner(scale_in[j].wait_recv)

        @when_inner
        def _():
            far_over[j][p].wait_recv()
            if p > 0:
                spot = pl.ds((p - 1) * size, size)
                end_scale = sc[j, spot, 0:1]
                mid_scale = sc[j, spot, sc.shape[2] // 2 : sc.shape[2] // 2 + 1]
                comb[j, p - 1] = (
                    end_scale * fres[j, p].astype(f32)
                    + mid_scale * total[(2 + j) * wide + p - 1].astype(f32)
                ).astype(b16)
            far_back(j, p).start()

    def stage_kv(step):
        if step == 0:
            for n in range(3, 8):
                loads[n].wait()
            kv[0, 0] = turned(keyraw_ref[...], kgain_ref)
            kv_near.start()
        elif step == 1:
            kv_near.wait_recv()
            when_inner(kv_mid.start)
        else:

            @when_inner
            def _():
                kv_mid.wait_recv()
                kv_far.start()

    def stage_att(head):
        if head == 0:
            loads[8].wait()
            loads[9].wait()
            when_outer(kv_far.wait_recv)
        cols = slice(head * dim, (head + 1) * dim)
        held = steps * length
        queries = turned(query_ref[:, cols], qgain_ref)
        keys = kv[:, 0].reshape(held, dim)
        scores = (
            lax.dot_general(
                queries, keys, (((1,), (1,)), ((), ())), preferred_element_type=f32
            )
            * dim ** (-0.5)
        )
        probs = jnp.exp(scores - jnp.max(scores, axis=-1, keepdims=True))
        amount = jnp.sum(probs, axis=-1, keepdims=True)
        summed = jnp.dot(
            probs.astype(b16), kv[:, 1].reshape(held, dim), preferred_element_type=f32
        )
        heads_ref[:, cols] = (summed / amount).astype(b16)

    def stage_outp():
        loads[13].wait()

        @pl.loop(0, width // tile_out)
        def _(i):
            cols = pl.ds(pl.multiple_of(i * tile_out, tile_out), tile_out)
            summed = jnp.dot(heads_ref[...], proj_ref[:, cols], preferred_element_type=f32)
            pm[:, :, cols] = summed.astype(b16).reshape(4, length // 4, tile_out)

        for copy in m_core:
            copy.start()

    def stage_mx(step):
        if step == 0:
            for copy in m_core:
                copy.wait_recv()
            to_xm[...] = (pm[across].astype(f32) + fc[1].astype(f32)).astype(b16)
            m_x.start()
        else:
            m_x.wait_recv()
            mixed_ref[...] = (
                pm[lane].astype(f32) + fc[0].astype(f32) + from_xm[...].astype(f32)
            ).astype(b16)
            mixed_out.start()

    def stage_pre():
        spot = lax.broadcasted_iota(jnp.int32, (count, count), 1).astype(f32)
        for r in range(4):
            pick[r] = (spot == lut[:, r : r + 1]).astype(b16)

    def gathered(cols, stores):
        found = 0.0
        for r, store in stores:
            depth = store.shape[0] * size
            results = store[:, :, cols].reshape(depth, tile_out)
            found += lut[:, 4 + r : 5 + r] * jnp.dot(
                pick[r, :, :depth], results, preferred_element_type=f32
            )
        return found

    def stage_cmb(last):
        if last:
            for n in range(width // tile_out):
                cols = slice(n * tile_out, (n + 1) * tile_out)
                found = acc[:, cols] + gathered(cols, ((0, oback),))
                expert_ref[:, cols] = found.astype(b16)
                expert_out[n].start()
            return
        for i in window:
            if i == SHARED_PIECE - 1:
                when_inner(near_back[i].wait_recv)
            elif i == SHARED_PIECE:
                when_outer(near_back[i].wait_recv)
            else:
                near_back[i].wait_recv()
        for p in range(blocks):
            far_back(0, p).wait_recv()

        @pl.loop(0, width // tile_out)
        def _(n):
            cols = pl.ds(pl.multiple_of(n * tile_out, tile_out), tile_out)
            acc[:, cols] = gathered(cols, ((1, nback), (2, fback), (3, fback)))

    stages = {"A": stage_a, "B": stage_b, "C": stage_c, "D": stage_d, "E": stage_e}
    loaded = False
    for name in ORDER:
        if name == "SEND":
            stage_send()
        elif name[:2] == "KV":
            stage_kv(int(name[2]))
        elif name[:3] == "ATT":
            stage_att(int(name[3]))
        elif name == "OUTP":
            stage_outp()
        elif name[:2] == "MX":
            stage_mx(int(name[2]))
        elif name == "PRE":
            stage_pre()
        elif name[:3] == "CMB":
            stage_cmb(name == "CMB")
        elif name[0] == "Y":
            stage_y(int(name[1]))
        elif name[0] == "R":
            stage_r(int(name[2]))
        elif name[0] == "G":
            stage_g(int(name[2]), int(name[3]))
        else:
            if name[0] == "C" and not loaded:
                loaded = True
                for n in (10, 11, 12):
                    loads[n].wait()
            stages[name[0]](name[1:-1], int(name[-1]))

    def all_sent(sem, like):
        pltpu.make_async_copy(like, like, sem).wait()

    def some(n):
        return total.at[pl.ds(0, n)]

    all_sent(xs.at[0], some(blocks + 2 * wide))
    all_sent(cs.at[0], from_core)
    all_sent(ps.at[0], from_core)
    all_sent(qs.at[0], some(4 * wide - 1))
    all_sent(near_s.at[0], some(2 * wide))
    all_sent(far_s.at[0], some(blocks))
    all_sent(nb_s.at[0], some(wide - 1))
    near_sum.wait_send()
    own_scale.wait_send()
    scale_out.wait_send()
    kv_near.wait_send()

    @when_inner
    def _():
        kv_mid.wait_send()
        kv_far.wait_send()
        all_sent(rel_s.at[0], some(2 * wide))
        all_sent(fb_s.at[0], some(2 * blocks))

    @when_outer
    def _():
        all_sent(fo_s.at[0], some(2 * wide))

    all_sent(ms.at[0], fc)
    m_x.wait_send()
    mixed_out.wait()
    for copy in expert_out:
        copy.wait()


def deliver_kernel(mixed_in, expert_in, mixed_out, expert_out, mixed_held, expert_held, sems):
    pairs = []
    for source, held, target, pieces in (
        (expert_in, expert_held, expert_out, 4),
        (mixed_in, mixed_held, mixed_out, 1),
    ):
        size = source.shape[0] // pieces
        for n in range(pieces):
            spot = pl.ds(n * size, size)
            at = len(pairs)
            pairs.append(
                (
                    pltpu.make_async_copy(source.at[spot], held.at[spot], sems.at[0, at]),
                    pltpu.make_async_copy(held.at[spot], target.at[spot], sems.at[1, at]),
                )
            )
    for fetch, _ in pairs:
        fetch.start()
    for fetch, store in pairs:
        fetch.wait()
        store.start()
    for _, store in pairs:
        store.wait()


def turn_tables(held, dim):
    quarter = dim // 4
    freqs = 1.0 / THETA ** (np.arange(quarter) * 4.0 / dim)
    spots = np.arange(held)
    tables = []
    for place in (spots // GRID_W, spots % GRID_W):
        angles = place[:, None] * freqs
        tables.append((np.cos(angles), np.sin(angles)))
    cosine = np.concatenate([tables[0][0]] * 2 + [tables[1][0]] * 2, axis=1)
    sine = np.concatenate(
        [-tables[0][1], tables[0][1], -tables[1][1], tables[1][1]], axis=1
    )
    return jnp.asarray(cosine, jnp.float32), jnp.asarray(sine, jnp.float32)


def fused(
    query_rows,
    projected_keys,
    projected_values,
    query_gain,
    key_norm_gain,
    out_proj,
    mix_tokens,
    norm_gain,
    expert_ids,
    expert_score,
    gate_proj,
    up_proj,
    down_proj,
):
    steps, lanes = lax.axis_size("ep"), lax.axis_size("tp")
    count, width = mix_tokens.shape
    cap = count * expert_ids.shape[1] * 3 // (2 * steps)
    size = count - cap
    blocks = count // size
    wide = blocks - 1
    hidden = gate_proj.shape[2]
    length, dim = projected_keys.shape
    kind = jnp.bfloat16
    cosine, sine = turn_tables(steps * length, dim)
    anywhere = pl.BlockSpec(memory_space=pltpu.HBM)
    units = 4 * wide
    mixed, expert = pl.pallas_call(
        functools.partial(fused_kernel, steps),
        out_shape=(
            jax.ShapeDtypeStruct((length // lanes, width), kind),
            jax.ShapeDtypeStruct((count, width), kind),
        ),
        in_specs=[anywhere] * 15,
        out_specs=(anywhere, anywhere),
        scratch_shapes=[
            pltpu.VMEM((2, count), jnp.int32),
            pltpu.VMEM((2, count), jnp.float32),
            pltpu.VMEM((1, width), jnp.float32),
            pltpu.VMEM((1, dim), jnp.float32),
            pltpu.VMEM((1, dim), jnp.float32),
            pltpu.VMEM((length // lanes, width), kind),
            pltpu.VMEM((count, width), kind),
            pltpu.VMEM((4, count, count), kind),
            pltpu.VMEM((width, hidden), kind),
            pltpu.VMEM((width, hidden), kind),
            pltpu.VMEM((hidden, width), kind),
            pltpu.VMEM(out_proj.shape, kind),
            pltpu.VMEM(query_rows.shape, kind),
            pltpu.VMEM((length, dim), kind),
            pltpu.VMEM((length, dim), jnp.float32),
            pltpu.VMEM((length, dim), jnp.float32),
            pltpu.VMEM((count, width), kind),
            pltpu.VMEM((count, width), kind),
            pltpu.VMEM((blocks, size, width), kind),
            pltpu.VMEM((size * (wide - 1), 128), jnp.float32),
            pltpu.VMEM((2, size * (wide - 1), 128), jnp.float32),
            pltpu.VMEM((size, 128), jnp.float32),
            pltpu.VMEM((size, 128), jnp.float32),
            pltpu.VMEM((2, size, width), kind),
            pltpu.VMEM((2, size, width), kind),
            pltpu.VMEM((size, width), jnp.float32),
            pltpu.VMEM((blocks, 4, size, width), kind),
            pltpu.VMEM((wide, 4, size, width), kind),
            pltpu.VMEM((2, blocks, 4, size, width), kind),
            pltpu.VMEM((4 * size, hidden), kind),
            pltpu.VMEM((units, 4, size, width), kind),
            pltpu.VMEM((units, 2, size, width), kind),
            pltpu.VMEM((units, size, width), kind),
            pltpu.VMEM((units, size, width), kind),
            pltpu.VMEM((units, size, width), kind),
            pltpu.VMEM((2, wide, size, width), kind),
            pltpu.VMEM((2, wide - 1, size, width), kind),
            pltpu.VMEM((wide, size, width), kind),
            pltpu.VMEM((wide, size, width), kind),
            pltpu.VMEM((blocks, size, width), kind),
            pltpu.VMEM((count, width), jnp.float32),
            pltpu.VMEM((count, count), jnp.float32),
            pltpu.VMEM((steps, 2, length, dim), kind),
            pltpu.VMEM(query_rows.shape, kind),
            pltpu.VMEM((lanes, length // lanes, width), kind),
            pltpu.VMEM((2, length // lanes, width), kind),
            pltpu.VMEM((length // lanes, width), kind),
            pltpu.VMEM((length // lanes, width), kind),
            pltpu.SemaphoreType.DMA((14 + blocks,)),
            pltpu.SemaphoreType.DMA((1 + width // math.gcd(width, 512),)),
        ]
        + [
            pltpu.SemaphoreType.DMA((n,))
            for n in (1, 2 * wide, 1, 2 * blocks, 1, 2 * wide)
            + (1, blocks + 2 * wide)
            + (1, units) * 3
            + (1, wide, 1, 2 * wide, 1, blocks)
            + (1, 2, 2, 2, 3, 3, 2, 3)
        ],
        compiler_params=pltpu.CompilerParams(
            collective_id=0, has_side_effects=True, vmem_limit_bytes=VMEM_LIMIT
        ),
    )(
        mix_tokens,
        expert_ids.T,
        expert_score.T,
        norm_gain.reshape(1, width),
        gate_proj.reshape(gate_proj.shape[1:]),
        up_proj.reshape(up_proj.shape[1:]),
        down_proj.reshape(down_proj.shape[1:]),
        out_proj,
        query_rows,
        projected_keys,
        projected_values,
        query_gain.reshape(1, dim),
        key_norm_gain.reshape(1, dim),
        cosine,
        sine,
    )
    return pl.pallas_call(
        deliver_kernel,
        out_shape=(
            jax.ShapeDtypeStruct(mixed.shape, kind),
            jax.ShapeDtypeStruct(expert.shape, kind),
        ),
        in_specs=[anywhere] * 2,
        out_specs=(anywhere, anywhere),
        scratch_shapes=[
            pltpu.VMEM(mixed.shape, kind),
            pltpu.VMEM(expert.shape, kind),
            pltpu.SemaphoreType.DMA((2, 5)),
        ],
    )(mixed, expert)


def fits_fused(query_rows, projected_keys, query_gain, mix_tokens, expert_ids, gate_proj):
    steps, lanes = lax.axis_size("ep"), lax.axis_size("tp")
    count, width = mix_tokens.shape
    length, dim = projected_keys.shape
    local_experts, _, hidden = gate_proj.shape
    cap = count * expert_ids.shape[1] * 3 // (2 * steps)
    blocks = 20 * steps * cap * width * 2 + 4 * width * hidden * 2
    return (
        lanes == 4
        and steps == 4
        and local_experts == 1
        and expert_ids.shape[1] == 2
        and dim == query_gain.shape[0]
        and dim % 128 == 0
        and length % 64 == 0
        and length <= 256
        and count == 128
        and cap < count
        and (count - cap) % 16 == 0
        and cap % (count - cap) == 0
        and 2 * cap > count
        and blocks < 48 * 1024 * 1024
    )


def local(
    query_rows,
    projected_keys,
    projected_values,
    query_gain,
    key_norm_gain,
    out_proj,
    mix_tokens,
    norm_gain,
    expert_ids,
    expert_score,
    gate_proj,
    up_proj,
    down_proj,
):
    simple = fits_fused(
        query_rows, projected_keys, query_gain, mix_tokens, expert_ids, gate_proj
    )
    return (fused if simple else plain_halves)(
        query_rows,
        projected_keys,
        projected_values,
        query_gain,
        key_norm_gain,
        out_proj,
        mix_tokens,
        norm_gain,
        expert_ids,
        expert_score,
        gate_proj,
        up_proj,
        down_proj,
    )


def solution(mesh):
    in_specs = (
        P(("grp", "ep"), "tp"),
        P(("grp", "ep"), "tp"),
        P(("grp", "ep"), "tp"),
        P(),
        P(),
        P("tp", None),
        P(("grp", "ep", "tp"), None),
        P(),
        P(("grp", "ep", "tp"), None),
        P(("grp", "ep", "tp"), None),
        P("ep", None, "tp"),
        P("ep", None, "tp"),
        P("ep", "tp", None),
    )
    out_specs = (P(("grp", "ep", "tp"), None), P(("grp", "ep", "tp"), None))
    return jax.shard_map(local, mesh=mesh, in_specs=in_specs, out_specs=out_specs, check_vma=False)
```

```python
import functools
import math

import jax
import jax.numpy as jnp
import numpy as np
from jax import lax
from jax.experimental import pallas as pl
from jax.experimental.pallas import tpu as pltpu
from jax.sharding import PartitionSpec as P

GRID_W = 64


MESH = pl.DeviceIdType.MESH
EPS = 1e-06
THETA = 10000.0


def head_norm(vectors, gain):
    return vectors * lax.rsqrt(jnp.mean(vectors * vectors, axis=-1, keepdims=True) + EPS) * gain


def rotate_grid(vectors, token_positions):
    length, heads, head_dim = vectors.shape
    quarter = head_dim // 4
    freqs = 1.0 / THETA ** (jnp.arange(quarter, dtype=jnp.float32) * 4.0 / head_dim)
    grid_row = (token_positions // GRID_W).astype(jnp.float32)
    grid_col = (token_positions % GRID_W).astype(jnp.float32)
    angles = jnp.stack([grid_row[:, None] * freqs, grid_col[:, None] * freqs], axis=1)
    cosine = jnp.cos(angles)[:, None]
    sine = jnp.sin(angles)[:, None]
    halves = vectors.reshape(length, heads, 2, 2, quarter)
    first = halves[..., 0, :]
    second = halves[..., 1, :]
    turned = jnp.stack([first * cosine - second * sine, second * cosine + first * sine], axis=-2)
    return turned.reshape(length, heads, head_dim)


def prepare_inputs(raw_rows, gain, heads, token_positions):
    length = raw_rows.shape[0]
    head_dim = gain.shape[0]
    vectors = raw_rows.astype(jnp.float32).reshape(length, heads, head_dim)
    return rotate_grid(head_norm(vectors, gain), token_positions).astype(jnp.bfloat16)


def mixer_prepare(query_rows, projected_keys, projected_values, query_gain, key_norm_gain):
    length = query_rows.shape[0]
    head_dim = query_gain.shape[0]
    kv_heads = projected_keys.shape[1] // head_dim
    q_heads = query_rows.shape[1] // head_dim
    token_positions = lax.axis_index("ep") * length + jnp.arange(length, dtype=jnp.int32)
    query_matrix = prepare_inputs(query_rows, query_gain, q_heads, token_positions).reshape(
        length, q_heads * head_dim
    )
    keys_turned = prepare_inputs(projected_keys, key_norm_gain, kv_heads, token_positions).reshape(
        length, kv_heads * head_dim
    )
    return query_matrix, jnp.concatenate([keys_turned, projected_values], axis=1)


def attend_plain(query_matrix, own_pair, head_dim):
    length = query_matrix.shape[0]
    kv_heads = own_pair.shape[1] // (2 * head_dim)
    q_heads = query_matrix.shape[1] // head_dim
    queries_per_group = q_heads // kv_heads
    query_matrix = query_matrix.reshape(length, kv_heads, queries_per_group, head_dim)
    score_scale = head_dim ** (-0.5)
    initial = (
        jnp.full((kv_heads, queries_per_group, length), -1e30, jnp.float32),
        jnp.zeros((kv_heads, queries_per_group, length), jnp.float32),
        jnp.zeros((length, kv_heads, queries_per_group, head_dim), jnp.float32),
    )
    width = kv_heads * head_dim
    pair = lax.all_gather(own_pair, "ep", axis=0, tiled=True)
    key_piece = pair[:, :width]
    value_piece = pair[:, width:]
    piece_rows = key_piece.shape[0]
    step_rows = math.gcd(piece_rows, 1024)

    def one_block(block_index, running):
        run_max, run_sum, run_acc = running
        offset = block_index * step_rows
        key_block = lax.dynamic_slice_in_dim(key_piece, offset, step_rows, 0).reshape(
            step_rows, kv_heads, head_dim
        )
        value_block = lax.dynamic_slice_in_dim(value_piece, offset, step_rows, 0).reshape(
            step_rows, kv_heads, head_dim
        )
        scores = (
            jnp.einsum(
                "tkgd,skd->kgts", query_matrix, key_block, preferred_element_type=jnp.float32
            )
            * score_scale
        )
        new_max = jnp.maximum(run_max, jnp.max(scores, axis=-1))
        factor = jnp.exp(run_max - new_max)
        weights = jnp.exp(scores - new_max[..., None])
        run_sum = run_sum * factor + jnp.sum(weights, axis=-1)
        update = jnp.einsum(
            "kgts,skd->tkgd",
            weights.astype(jnp.bfloat16),
            value_block,
            preferred_element_type=jnp.float32,
        )
        run_acc = run_acc * jnp.transpose(factor, (2, 0, 1))[..., None] + update
        return (new_max, run_sum, run_acc)

    run_max, run_sum, run_acc = lax.fori_loop(0, piece_rows // step_rows, one_block, initial)
    return (
        (run_acc / jnp.transpose(run_sum, (2, 0, 1))[..., None])
        .astype(jnp.bfloat16)
        .reshape(length, q_heads * head_dim)
    )


def flip(index, bits):
    result, place = 0, 1
    for _ in range(8):
        mine = (index // place) % 2
        result = result + place * ((1 - mine) if bits & place else mine)
        place *= 2
    return result


def exchange_plain(outgoing, gate_proj, up_proj, down_proj):
    rows_in = lax.all_gather(
        lax.all_to_all(outgoing, "ep", split_axis=0, concat_axis=0, tiled=True),
        "tp",
        axis=0,
        tiled=True,
    )
    gate_out = jnp.einsum("secd,edf->secf", rows_in, gate_proj, preferred_element_type=jnp.float32)
    up_out = jnp.einsum("secd,edf->secf", rows_in, up_proj, preferred_element_type=jnp.float32)
    active = (jax.nn.silu(gate_out) * up_out).astype(jnp.bfloat16)
    summed = lax.psum_scatter(
        jnp.einsum("secf,efd->secd", active, down_proj, preferred_element_type=jnp.float32).astype(
            jnp.bfloat16
        ),
        "tp",
        scatter_dimension=0,
        tiled=True,
    )
    return lax.all_to_all(summed, "ep", split_axis=0, concat_axis=0, tiled=True)


def plain_halves(
    query_rows,
    projected_keys,
    projected_values,
    query_gain,
    key_norm_gain,
    out_proj,
    mix_tokens,
    norm_gain,
    expert_ids,
    expert_score,
    gate_proj,
    up_proj,
    down_proj,
):
    length, model_dim = mix_tokens.shape
    top_count = expert_ids.shape[1]
    local_experts = gate_proj.shape[0]
    expert_axis = lax.axis_size("ep")
    experts_all = expert_axis * local_experts
    capacity = length * top_count * 3 // (2 * experts_all)
    values_b = mix_tokens.astype(jnp.float32)
    normed = (
        values_b
        * lax.rsqrt(jnp.mean(values_b * values_b, axis=-1, keepdims=True) + EPS)
        * norm_gain
    ).astype(jnp.bfloat16)
    flat = expert_ids.reshape(length * top_count)
    onehot = (flat[:, None] == jnp.arange(experts_all, dtype=jnp.int32)).astype(jnp.int32)
    slots = jnp.sum((jnp.cumsum(onehot, axis=0) - onehot) * onehot, axis=1)
    target = flat * capacity + slots
    placed = (target[:, None] == jnp.arange(experts_all * capacity, dtype=jnp.int32)).astype(
        jnp.int32
    )
    placed = jnp.sum(placed.reshape(length, top_count, experts_all * capacity), axis=1).astype(
        jnp.bfloat16
    )
    outgoing = jnp.einsum("re,rd->ed", placed, normed, preferred_element_type=jnp.float32).astype(
        jnp.bfloat16
    )
    outgoing = outgoing.reshape(expert_axis, local_experts, capacity, model_dim)
    lanes = lax.axis_size("tp")
    head_dim = query_gain.shape[0]
    queries, pair = mixer_prepare(
        query_rows, projected_keys, projected_values, query_gain, key_norm_gain
    )
    heads_out = attend_plain(queries, pair, head_dim)
    returned = exchange_plain(outgoing, gate_proj, up_proj, down_proj)
    head_partial = jnp.dot(heads_out, out_proj, preferred_element_type=jnp.float32).astype(
        jnp.bfloat16
    )
    pieces = lax.all_to_all(
        head_partial.reshape(lanes, -1, head_partial.shape[1]),
        "tp",
        split_axis=0,
        concat_axis=0,
        tiled=True,
    )
    mixed_rows = jnp.sum(pieces.astype(jnp.float32), axis=0).astype(jnp.bfloat16)
    results = returned.reshape(experts_all * capacity, model_dim)
    first_weight = jax.nn.sigmoid(expert_score[:, 0] - expert_score[:, 1])
    picks = target.reshape(length, top_count)
    chosen = [
        jnp.dot(
            (picks[:, k : k + 1] == jnp.arange(experts_all * capacity, dtype=jnp.int32)).astype(
                jnp.bfloat16
            ),
            results,
            preferred_element_type=jnp.float32,
        )
        for k in range(2)
    ]
    combined = first_weight[:, None] * chosen[0] + (1.0 - first_weight)[:, None] * chosen[1]
    return (mixed_rows, combined.astype(jnp.bfloat16))


ORDER = (
    "SEND", "RF1", "BO2", "AF10", "CO2", "RF0", "AF11", "BF10", "AF00",
    "BF11", "KV0", "PRE", "AF12", "CF11", "BO0", "AF01", "BF00", "CF10",
    "DF11", "Y0", "KV1", "CF00", "Y1", "Y2", "BF01", "DF10", "BF12",
    "CO0", "DF00", "AF02", "CF01", "BN0", "EF11", "CF12", "BN1", "CN0",
    "KV2", "EF00", "DF01", "DF12", "CN1", "EF10", "GF11", "BF02", "BN2",
    "DO2", "EF01", "BO1", "GF00", "DN0", "DN1", "CF02", "GF10", "DF02",
    "EF12", "CN2", "ATT0", "GF01", "DN2", "EN1", "CO1", "ATT1", "ATT2",
    "EF02", "ATT3", "DO0", "OUTP", "DO1", "EN2", "EN0", "GF12", "EO2",
    "GF02", "EO0", "MX0", "EO1", "CMB", "MX1",
)
SENDS = (
    ("X", 2), ("X", 3), ("N", 2), ("F", 0), ("F", 1),
    ("F", 2), ("N", 1), ("F", 3), ("X", 1), ("N", 0), ("X", 0),
)
SHARED_PIECE = 1
VMEM_LIMIT = 58 * 1024 * 1024


def fused_kernel(
    steps,
    tokens_hbm,
    ids_hbm,
    score_hbm,
    ngain_hbm,
    gate_hbm,
    up_hbm,
    down_hbm,
    proj_hbm,
    query_hbm,
    key_hbm,
    value_hbm,
    qgain_hbm,
    kgain_hbm,
    cos_hbm,
    sin_hbm,
    mixed_hbm,
    expert_hbm,
    ids_ref,
    score_ref,
    ngain_ref,
    qgain_ref,
    kgain_ref,
    mixed_ref,
    expert_ref,
    pick,
    gate_ref,
    up_ref,
    down_ref,
    proj_ref,
    query_ref,
    keyraw_ref,
    cos_ref,
    sin_ref,
    tok_ref,
    norm_ref,
    outf,
    scl,
    sc,
    own_scl,
    x_scl,
    near_two,
    near_got,
    own_sum,
    orows,
    nrows,
    frows,
    act,
    part,
    from_core,
    to_x,
    from_x,
    total,
    fres,
    comb,
    oback,
    nback,
    fback,
    lut,
    kv,
    heads_ref,
    pm,
    fc,
    to_xm,
    from_xm,
    hsem,
    osem,
    near_s,
    near_r,
    far_s,
    far_r,
    rel_s,
    rel_r,
    xs,
    xr,
    cs,
    cr,
    ps,
    pr,
    qs,
    qr,
    nb_s,
    nb_r,
    fo_s,
    fo_r,
    fb_s,
    fb_r,
    sc_s,
    sc_r,
    ns_s,
    ns_r,
    ks,
    kr,
    ms,
    mr,
):
    me = lax.axis_index("ep")
    lane = lax.axis_index("tp")
    peers = [flip(me, k) for k in range(steps)]
    core, across = flip(lane, 1), flip(lane, 2)
    inner = ((me + 1) // 2) % 2
    outer = 1 - inner
    gate_at = 2 - me // 2
    sources = [3 - me, flip(3 - me, 1)]
    blocks, _, size, width = orows.shape
    wide = blocks - 1
    hidden = gate_ref.shape[1]
    length = query_ref.shape[0]
    dim = keyraw_ref.shape[1]
    count = tok_ref.shape[0]
    tile = math.gcd(hidden, 512)
    tile_out = math.gcd(width, 512)
    f32, b16 = jnp.float32, jnp.bfloat16

    offset = pl.multiple_of(me * length, 16)
    loads = [
        pltpu.make_async_copy(s, d, hsem.at[i])
        for i, (s, d) in enumerate(
            [
                (ids_hbm, ids_ref),
                (score_hbm, score_ref),
                (ngain_hbm, ngain_ref),
                (kgain_hbm, kgain_ref),
                (key_hbm, keyraw_ref),
                (value_hbm, kv.at[0, 1]),
                (cos_hbm.at[pl.ds(offset, length)], cos_ref),
                (sin_hbm.at[pl.ds(offset, length)], sin_ref),
                (qgain_hbm, qgain_ref),
                (query_hbm, query_ref),
                (gate_hbm, gate_ref),
                (up_hbm, up_ref),
                (down_hbm, down_ref),
                (proj_hbm, proj_ref),
            ]
        )
    ]
    spots = [pl.ds(n * size, size) for n in range(blocks)]
    pieces = [
        pltpu.make_async_copy(tokens_hbm.at[spot], tok_ref.at[spot], hsem.at[len(loads) + n])
        for n, spot in enumerate(spots)
    ]
    for load in loads[:3] + pieces + loads[3:]:
        load.start()

    barrier = pltpu.get_barrier_semaphore()
    friends = [{"ep": me, "tp": core}, {"ep": me, "tp": across}]
    friends += [{"ep": peers[k], "tp": lane} for k in (1, 2)]

    def greet(friend):
        pl.semaphore_signal(barrier, inc=1, device_id=friend, device_id_type=MESH)

    @pl.when(inner == 1)
    def _():
        greet({"ep": peers[3], "tp": lane})

    for friend in friends:
        greet(friend)

    def remote(src, dst, send, recv, ep_to, tp_to):
        return pltpu.make_async_remote_copy(
            src_ref=src,
            dst_ref=dst,
            send_sem=send,
            recv_sem=recv,
            device_id={"ep": ep_to, "tp": tp_to},
            device_id_type=MESH,
        )

    def when_inner(body):
        pl.when(inner == 1)(body)

    def when_outer(body):
        pl.when(inner == 0)(body)

    kinds = ("O", "N", "F0", "F1")
    window = range(wide)
    number = {(c, i): n * wide + i for n, c in enumerate(kinds) for i in window}

    def by_role(i, special, usual):
        if i == SHARED_PIECE - 1:
            when_inner(special)
            when_outer(usual)
        elif i == SHARED_PIECE:
            when_outer(special)
            when_inner(usual)
        else:
            usual()

    def rows_of(c, i):
        if c == "O":
            return orows.at[i + inner]
        if c == "N":
            return nrows.at[i]
        return frows.at[int(c[1]), i + inner]

    def x_own(p):
        return remote(orows.at[p, 0], orows.at[p, 1], xs.at[0], xr.at[p], me, across)

    near = [
        [
            remote(
                orows.at[i + outer, n],
                nrows.at[i, n],
                near_s.at[0],
                near_r.at[n * wide + i],
                peers[1],
                lane,
            )
            for i in window
        ]
        for n in range(2)
    ]
    far = [
        remote(
            outf.at[p],
            frows.at[outer, p, 0],
            far_s.at[0],
            far_r.at[outer * blocks + p],
            gate_at,
            lane,
        )
        for p in range(blocks)
    ]
    far_in = [
        [
            remote(
                outf.at[p], frows.at[j, p, 0], far_s.at[0], far_r.at[j * blocks + p], gate_at, lane
            )
            for p in range(blocks)
        ]
        for j in range(2)
    ]
    relay = [
        [
            remote(
                frows.at[j, p, 0],
                frows.at[j, p, 0],
                rel_s.at[0],
                far_r.at[j * blocks + p],
                peers[1],
                lane,
            )
            for p in window
        ]
        for j in range(2)
    ]
    scale_out = remote(scl, sc.at[outer], sc_s.at[0], sc_r.at[outer], gate_at, lane)
    scale_in = [remote(scl, sc.at[j], sc_s.at[0], sc_r.at[j], gate_at, lane) for j in range(2)]
    x_far, c_in, c_out, x_out = {}, {}, {}, {}
    for (c, i), u in number.items():
        held = rows_of(c, i)
        if c[0] == "F":
            at = blocks + u - 2 * wide
            x_far[c, i] = remote(held.at[0], held.at[1], xs.at[0], xr.at[at], me, across)
        c_in[c, i] = remote(
            held.at[pl.ds(0, 2)], held.at[pl.ds(2, 2)], cs.at[0], cr.at[u], me, core
        )
        c_out[c, i] = remote(
            part.at[u, pl.ds(2, 2)], from_core.at[u], ps.at[0], pr.at[u], me, core
        )
        x_out[c, i] = remote(to_x.at[u], from_x.at[u], qs.at[0], qr.at[u], me, across)
    near_back = [
        remote(total.at[wide + i], nback.at[i], nb_s.at[0], nb_r.at[i], peers[1], lane)
        for i in window
    ]
    near_sum = remote(near_two, near_got, ns_s.at[0], ns_r.at[0], peers[1], lane)
    own_scale = remote(own_scl, x_scl, ns_s.at[1], ns_r.at[1], me, across)
    far_over = [
        [
            remote(
                total.at[(2 + j) * wide + i],
                fres.at[j, i],
                fo_s.at[0],
                fo_r.at[j * wide + i],
                peers[1],
                lane,
            )
            for i in window
        ]
        for j in range(2)
    ]

    def far_back(j, p):
        if p == 0:
            source = fres.at[j, 0]
        elif p == wide:
            source = total.at[(2 + j) * wide + wide - 1]
        else:
            source = comb.at[j, p - 1]
        return remote(
            source, fback.at[p], fb_s.at[0], fb_r.at[p], sources[j], lane
        )

    kv_near = remote(kv.at[0], kv.at[1], ks.at[0], kr.at[0], peers[1], lane)
    kv_mid = remote(kv.at[pl.ds(0, 2)], kv.at[pl.ds(2, 2)], ks.at[1], kr.at[1], peers[3], lane)
    kv_far = remote(kv.at[pl.ds(2, 2)], kv.at[pl.ds(2, 2)], ks.at[2], kr.at[2], peers[1], lane)
    m_core = [
        remote(pm.at[core], fc.at[0], ms.at[0], mr.at[0], me, core),
        remote(pm.at[flip(core, 2)], fc.at[1], ms.at[0], mr.at[1], me, core),
    ]
    m_x = remote(to_xm, from_xm, ms.at[1], mr.at[2], me, across)
    mixed_out = pltpu.make_async_copy(mixed_ref, mixed_hbm, osem.at[0])
    expert_out = [
        pltpu.make_async_copy(
            expert_ref.at[:, pl.ds(n * tile_out, tile_out)],
            expert_hbm.at[:, pl.ds(n * tile_out, tile_out)],
            osem.at[1 + n],
        )
        for n in range(width // tile_out)
    ]

    loads[0].wait()
    loads[1].wait()

    token_row = lax.broadcasted_iota(jnp.int32, (count, count), 0)
    token_col = lax.broadcasted_iota(jnp.int32, (count, count), 1)
    earlier = (token_row < token_col).astype(b16)
    first, second = ids_ref[0:1, :], ids_ref[1:2, :]
    weight = 1.0 / (1.0 + jnp.exp(score_ref[1:2, :] - score_ref[0:1, :]))
    table_row = lax.broadcasted_iota(jnp.int32, (8, count), 0)
    high = me // 2
    ends = (3 * high, 3 - 3 * high)
    middles = (1 + high, 2 - high)

    def naming(expert):
        one, two = first == expert, second == expert
        share = jnp.where(one, weight, 0.0) + jnp.where(two, 1.0 - weight, 0.0)
        return jnp.where(one | two, 1.0, 0.0), share

    named = [(naming(ends[n]), naming(middles[n])) for n in range(2)]
    counted = jnp.zeros((8, count), f32)
    parts_of = []
    for n in range(2):
        (end_one, _), (mid_one, _) = named[n]
        both = end_one * mid_one
        parts_of.append((end_one - both, mid_one - both, both))
        for r in range(3):
            counted = jnp.where(table_row == 3 * n + r, parts_of[n][r], counted)
    rank = jnp.dot(counted.astype(b16), earlier, preferred_element_type=f32)
    sums = jnp.sum(counted, axis=1, keepdims=True)
    tail, middle = float(size), float(size * (wide - 1))

    def positions(n):
        end_only, mid_only, both = parts_of[n]
        end_rank, mid_rank, both_rank = (rank[3 * n + r : 3 * n + r + 1, :] for r in range(3))
        end_sum, both_sum = sums[3 * n : 3 * n + 1, :], sums[3 * n + 2 : 3 * n + 3, :]
        extra = jnp.maximum(both_sum - middle, 0.0)
        common = tail + jnp.minimum(both_sum, middle)
        end_at, mid_at = end_rank + extra, mid_rank + extra
        spill = jnp.maximum(end_sum + extra - tail, 0.0)
        shared = both_rank < middle
        end_pos = jnp.where(
            both > 0.5,
            jnp.where(shared, tail + both_rank, both_rank - middle),
            jnp.where(end_at < tail, end_at, common + end_at - tail),
        )
        mid_pos = jnp.where(
            both > 0.5,
            tail + both_rank,
            jnp.where(
                mid_at < tail, tail + middle + mid_at, common + spill + mid_at - tail
            ),
        )
        end_pos = jnp.where(end_only + both > 0.5, end_pos, -1.0)
        mid_pos = jnp.where(mid_only + both > 0.5, mid_pos, -1.0)
        return end_pos, mid_pos, jnp.where((both > 0.5) & shared, 1.0, 0.0)

    own_end, own_mid, own_shared = positions(0)
    far_end, far_mid, far_shared = positions(1)
    slot = lax.broadcasted_iota(jnp.int32, (count, count), 0).astype(f32)

    def dispatch(end_pos, mid_pos):
        chosen = ((slot == end_pos) | (slot == mid_pos)).astype(b16)
        picked = jnp.dot(chosen, norm_ref[...], preferred_element_type=f32)
        return picked.astype(b16).reshape(blocks, size, width)

    loads[2].wait()
    for n, spot in enumerate(spots):
        pieces[n].wait()
        values = tok_ref[spot, :].astype(f32)
        norm_ref[spot, :] = (
            values
            * lax.rsqrt(jnp.mean(values * values, axis=-1, keepdims=True) + EPS)
            * ngain_ref[...]
        ).astype(b16)
    orows[:, 0] = dispatch(own_end, own_mid)

    @when_inner
    def _():
        pl.semaphore_wait(barrier, len(friends) + 1)

    @when_outer
    def _():
        pl.semaphore_wait(barrier, len(friends))

    for kind, p in SENDS:
        if kind == "X":
            x_own(p).start()
    outf[...] = dispatch(far_end, far_mid)

    def stage_send():
        for kind, p in SENDS:
            if kind == "F":
                far[p].start()
            elif kind == "N":
                near[0][p].start()
        end_share, mid_share = named[1][0][1], named[1][1][1]
        rows_mid = slice(size, size * wide)
        end_scale = jnp.sum(
            jnp.where(
                slot[rows_mid] == far_end, jnp.where(far_shared > 0.5, end_share, 1.0), 0.0
            ),
            axis=1,
            keepdims=True,
        )
        mid_scale = jnp.sum(
            jnp.where(
                slot[rows_mid] == far_mid, jnp.where(far_shared > 0.5, mid_share, 1.0), 0.0
            ),
            axis=1,
            keepdims=True,
        )
        lanes_of = lax.broadcasted_iota(jnp.int32, scl.shape, 1)
        scl[...] = jnp.where(lanes_of < scl.shape[1] // 2, end_scale, mid_scale)
        scale_out.start()
        is_inner = (jnp.zeros((1, count), jnp.int32) + inner) == 1
        own_at = jnp.where(is_inner, own_mid, own_end)
        near_at = jnp.where(is_inner, own_end, own_mid)
        own_share = jnp.where(is_inner, named[0][1][1], named[0][0][1])
        near_share = jnp.where(is_inner, named[0][0][1], named[0][1][1])
        rows_one = slice(size * SHARED_PIECE, size * (SHARED_PIECE + 1))
        own_factor = jnp.sum(
            jnp.where(
                slot[rows_one] == own_at, jnp.where(own_shared > 0.5, own_share, 1.0), 0.0
            ),
            axis=1,
            keepdims=True,
        )
        near_factor = jnp.sum(
            jnp.where(
                slot[rows_one] == near_at, jnp.where(own_shared > 0.5, near_share, 1.0), 0.0
            ),
            axis=1,
            keepdims=True,
        )
        lanes_one = lax.broadcasted_iota(jnp.int32, own_scl.shape, 1)
        own_scl[...] = jnp.where(lanes_one < own_scl.shape[1] // 2, own_factor, near_factor)
        own_scale.start()
        nback[SHARED_PIECE - outer] = jnp.zeros((size, width), b16)
        moved = (near_at >= size * SHARED_PIECE) & (near_at < size * (SHARED_PIECE + 1))
        own_first = jnp.where(is_inner, tail, 0.0)
        own_held = jnp.where(moved, near_at, own_at)
        near_held = jnp.where(moved, -1.0, near_at)
        table = (
            jnp.where(own_held < 0.0, -1.0, own_held - own_first),
            jnp.where(near_held < 0.0, -1.0, near_held - (tail - own_first)),
            far_end,
            jnp.where(far_shared > 0.5, -1.0, far_mid),
            jnp.where(
                moved, jnp.where(own_shared > 0.5, 1.0, near_share), own_share
            ),
            near_share,
            jnp.where(far_shared > 0.5, 1.0, end_share),
            mid_share,
        )
        kept = jnp.zeros((8, count), f32)
        for r in range(8):
            kept = jnp.where(table_row == r, table[r], kept)
        rest = jnp.zeros((count - 8, count), f32)
        lut[...] = jnp.transpose(jnp.concatenate([kept, rest], axis=0))

    turn_lane = lax.broadcasted_iota(jnp.int32, (length, dim), 1)
    leading = (turn_lane // (dim // 4)) % 2 == 0

    def turned(raw, gain):
        vectors = raw.astype(f32)
        vectors = (
            vectors
            * lax.rsqrt(jnp.mean(vectors * vectors, axis=-1, keepdims=True) + EPS)
            * gain[...]
        )
        other = jnp.where(
            leading,
            pltpu.roll(vectors, dim - dim // 4, 1),
            pltpu.roll(vectors, dim // 4, 1),
        )
        return (vectors * cos_ref[...] + other * sin_ref[...]).astype(b16)

    arrived = (set(), set())
    scaled = set()

    def own_arrived(by_role):
        missing = [p not in arrived[r] for r, p in enumerate(by_role)]
        for r, p in enumerate(by_role):
            arrived[r].add(p)
        for r, run in ((0, when_outer), (1, when_inner)):
            if missing[r]:

                @run
                def _(p=by_role[r]):
                    x_own(p).wait_recv()

    def stage_y(i):
        own_arrived((i + 1, i))
        near[1][i].start()

    def stage_a(c, i):
        j = int(c[1])

        @when_inner
        def _():
            far_in[j][i + 1].wait_recv()
            if i + 1 < wide:
                relay[j][i + 1].start()

        @when_outer
        def _():
            relay[j][i].wait_recv()

        x_far[c, i].start()

    def stage_r(j):
        @when_inner
        def _():
            far_in[j][0].wait_recv()
            relay[j][0].start()

    def stage_b(c, i):
        if c == "O":
            own_arrived((i, i + 1))
        elif c == "N":
            near[0][i].wait_recv()
            near[1][i].wait_recv()
        else:
            x_far[c, i].wait_recv()
        c_in[c, i].start()

    def stage_c(c, i):
        c_in[c, i].wait_recv()
        u = number[c, i]
        held = rows_of(c, i)

        @pl.loop(0, hidden // tile)
        def _(n):
            cols = pl.ds(pl.multiple_of(n * tile, tile), tile)
            block = held[...].reshape(4 * size, width)
            gate = jnp.dot(block, gate_ref[:, cols], preferred_element_type=f32)
            up = jnp.dot(block, up_ref[:, cols], preferred_element_type=f32)
            act[:, cols] = (gate / (1.0 + jnp.exp(-gate)) * up).astype(b16)

        @pl.loop(0, width // tile_out)
        def _(n):
            cols = pl.ds(pl.multiple_of(n * tile_out, tile_out), tile_out)
            summed = jnp.dot(act[...], down_ref[:, cols], preferred_element_type=f32)
            part[u, :, :, cols] = summed.astype(b16).reshape(4, size, tile_out)

        c_out[c, i].start()

    def stage_d(c, i):
        c_out[c, i].wait_recv()
        u = number[c, i]

        def usual():
            to_x[u] = (part[u, 1].astype(f32) + from_core[u, 1].astype(f32)).astype(b16)
            x_out[c, i].start()

        def near_special():
            for n in range(2):
                near_two[n] = (
                    part[u, n].astype(f32) + from_core[u, n].astype(f32)
                ).astype(b16)
            near_sum.start()

        def own_special():
            near_sum.wait_recv()
            own_scale.wait_recv()
            half = own_scl.shape[1] // 2
            for n, factors in ((1, x_scl), (0, own_scl)):
                both = factors[:, 0:1] * (
                    part[u, n].astype(f32) + from_core[u, n].astype(f32)
                ) + factors[:, half : half + 1] * near_got[n].astype(f32)
                if n:
                    to_x[u] = both.astype(b16)
                    x_out[c, i].start()
                else:
                    own_sum[...] = both

        if c == "N":
            by_role(i, near_special, usual)
        elif c == "O":
            by_role(i, own_special, usual)
        else:
            usual()

    def stage_e(c, i):
        u = number[c, i]

        def reduced():
            x_out[c, i].wait_recv()
            return (
                part[u, 0].astype(f32)
                + from_core[u, 0].astype(f32)
                + from_x[u].astype(f32)
            ).astype(b16)

        if c == "O":

            def own_special():
                x_out[c, i].wait_recv()
                oback[i] = (own_sum[...] + from_x[u].astype(f32)).astype(b16)

            def own_usual():
                oback[i] = reduced()

            by_role(i, own_special, own_usual)
            return
        if c == "N":

            def near_usual():
                total[u] = reduced()
                near_back[i].start()

            by_role(i, lambda: None, near_usual)
            return
        total[u] = reduced()
        j = int(c[1])
        when_outer(far_over[j][i].start)
        if i == wide - 1:
            when_inner(far_back(j, wide).start)

    def stage_g(j, p):
        if p > 0 and j not in scaled:
            scaled.add(j)
            when_inner(scale_in[j].wait_recv)

        @when_inner
        def _():
            far_over[j][p].wait_recv()
            if p > 0:
                spot = pl.ds((p - 1) * size, size)
                end_scale = sc[j, spot, 0:1]
                mid_scale = sc[j, spot, sc.shape[2] // 2 : sc.shape[2] // 2 + 1]
                comb[j, p - 1] = (
                    end_scale * fres[j, p].astype(f32)
                    + mid_scale * total[(2 + j) * wide + p - 1].astype(f32)
                ).astype(b16)
            far_back(j, p).start()

    def stage_kv(step):
        if step == 0:
            for n in range(3, 8):
                loads[n].wait()
            kv[0, 0] = turned(keyraw_ref[...], kgain_ref)
            kv_near.start()
        elif step == 1:
            kv_near.wait_recv()
            when_inner(kv_mid.start)
        else:

            @when_inner
            def _():
                kv_mid.wait_recv()
                kv_far.start()

    def stage_att(head):
        if head == 0:
            loads[8].wait()
            loads[9].wait()
            when_outer(kv_far.wait_recv)
        cols = slice(head * dim, (head + 1) * dim)
        held = steps * length
        queries = turned(query_ref[:, cols], qgain_ref)
        keys = kv[:, 0].reshape(held, dim)
        scores = (
            lax.dot_general(
                queries, keys, (((1,), (1,)), ((), ())), preferred_element_type=f32
            )
            * dim ** (-0.5)
        )
        probs = jnp.exp(scores - jnp.max(scores, axis=-1, keepdims=True))
        amount = jnp.sum(probs, axis=-1, keepdims=True)
        summed = jnp.dot(
            probs.astype(b16), kv[:, 1].reshape(held, dim), preferred_element_type=f32
        )
        heads_ref[:, cols] = (summed / amount).astype(b16)

    def stage_outp():
        loads[13].wait()

        @pl.loop(0, width // tile_out)
        def _(i):
            cols = pl.ds(pl.multiple_of(i * tile_out, tile_out), tile_out)
            summed = jnp.dot(heads_ref[...], proj_ref[:, cols], preferred_element_type=f32)
            pm[:, :, cols] = summed.astype(b16).reshape(4, length // 4, tile_out)

        for copy in m_core:
            copy.start()

    def stage_mx(step):
        if step == 0:
            for copy in m_core:
                copy.wait_recv()
            to_xm[...] = (pm[across].astype(f32) + fc[1].astype(f32)).astype(b16)
            m_x.start()
        else:
            m_x.wait_recv()
            mixed_ref[...] = (
                pm[lane].astype(f32) + fc[0].astype(f32) + from_xm[...].astype(f32)
            ).astype(b16)
            mixed_out.start()

    def stage_pre():
        spot = lax.broadcasted_iota(jnp.int32, (count, count), 1).astype(f32)
        for r in range(4):
            pick[r] = (spot == lut[:, r : r + 1]).astype(b16)

    def gathered(cols, stores):
        found = 0.0
        for r, store in stores:
            depth = store.shape[0] * size
            results = store[:, :, cols].reshape(depth, tile_out)
            found += lut[:, 4 + r : 5 + r] * jnp.dot(
                pick[r, :, :depth], results, preferred_element_type=f32
            )
        return found

    def stage_cmb():
        for i in window:
            if i == SHARED_PIECE - 1:
                when_inner(near_back[i].wait_recv)
            elif i == SHARED_PIECE:
                when_outer(near_back[i].wait_recv)
            else:
                near_back[i].wait_recv()
        for p in range(blocks):
            far_back(0, p).wait_recv()
        for n in range(width // tile_out):
            cols = slice(n * tile_out, (n + 1) * tile_out)
            found = gathered(cols, ((0, oback), (1, nback), (2, fback), (3, fback)))
            expert_ref[:, cols] = found.astype(b16)
            expert_out[n].start()

    stages = {"A": stage_a, "B": stage_b, "C": stage_c, "D": stage_d, "E": stage_e}
    loaded = False
    for name in ORDER:
        if name == "SEND":
            stage_send()
        elif name[:2] == "KV":
            stage_kv(int(name[2]))
        elif name[:3] == "ATT":
            stage_att(int(name[3]))
        elif name == "OUTP":
            stage_outp()
        elif name[:2] == "MX":
            stage_mx(int(name[2]))
        elif name == "PRE":
            stage_pre()
        elif name == "CMB":
            stage_cmb()
        elif name[0] == "Y":
            stage_y(int(name[1]))
        elif name[0] == "R":
            stage_r(int(name[2]))
        elif name[0] == "G":
            stage_g(int(name[2]), int(name[3]))
        else:
            if name[0] == "C" and not loaded:
                loaded = True
                for n in (10, 11, 12):
                    loads[n].wait()
            stages[name[0]](name[1:-1], int(name[-1]))

    def all_sent(sem, like):
        pltpu.make_async_copy(like, like, sem).wait()

    def some(n):
        return total.at[pl.ds(0, n)]

    all_sent(xs.at[0], some(blocks + 2 * wide))
    all_sent(cs.at[0], from_core)
    all_sent(ps.at[0], from_core)
    all_sent(qs.at[0], some(4 * wide - 1))
    all_sent(near_s.at[0], some(2 * wide))
    all_sent(far_s.at[0], some(blocks))
    all_sent(nb_s.at[0], some(wide - 1))
    near_sum.wait_send()
    own_scale.wait_send()
    scale_out.wait_send()
    kv_near.wait_send()

    @when_inner
    def _():
        kv_mid.wait_send()
        kv_far.wait_send()
        all_sent(rel_s.at[0], some(2 * wide))
        all_sent(fb_s.at[0], some(2 * blocks))

    @when_outer
    def _():
        all_sent(fo_s.at[0], some(2 * wide))

    all_sent(ms.at[0], fc)
    m_x.wait_send()
    mixed_out.wait()
    for copy in expert_out:
        copy.wait()


def deliver_kernel(mixed_in, expert_in, mixed_out, expert_out, mixed_held, expert_held, sems):
    pairs = []
    for source, held, target, pieces in (
        (expert_in, expert_held, expert_out, 1),
        (mixed_in, mixed_held, mixed_out, 1),
    ):
        size = source.shape[0] // pieces
        for n in range(pieces):
            spot = pl.ds(n * size, size)
            at = len(pairs)
            pairs.append(
                (
                    pltpu.make_async_copy(source.at[spot], held.at[spot], sems.at[0, at]),
                    pltpu.make_async_copy(held.at[spot], target.at[spot], sems.at[1, at]),
                )
            )
    for fetch, _ in pairs:
        fetch.start()
    for fetch, store in pairs:
        fetch.wait()
        store.start()
    for _, store in pairs:
        store.wait()


def turn_tables(held, dim):
    quarter = dim // 4
    freqs = 1.0 / THETA ** (np.arange(quarter) * 4.0 / dim)
    spots = np.arange(held)
    tables = []
    for place in (spots // GRID_W, spots % GRID_W):
        angles = place[:, None] * freqs
        tables.append((np.cos(angles), np.sin(angles)))
    cosine = np.concatenate([tables[0][0]] * 2 + [tables[1][0]] * 2, axis=1)
    sine = np.concatenate(
        [-tables[0][1], tables[0][1], -tables[1][1], tables[1][1]], axis=1
    )
    return jnp.asarray(cosine, jnp.float32), jnp.asarray(sine, jnp.float32)


def fused(
    query_rows,
    projected_keys,
    projected_values,
    query_gain,
    key_norm_gain,
    out_proj,
    mix_tokens,
    norm_gain,
    expert_ids,
    expert_score,
    gate_proj,
    up_proj,
    down_proj,
):
    steps, lanes = lax.axis_size("ep"), lax.axis_size("tp")
    count, width = mix_tokens.shape
    cap = count * expert_ids.shape[1] * 3 // (2 * steps)
    size = count - cap
    blocks = count // size
    wide = blocks - 1
    hidden = gate_proj.shape[2]
    length, dim = projected_keys.shape
    kind = jnp.bfloat16
    cosine, sine = turn_tables(steps * length, dim)
    anywhere = pl.BlockSpec(memory_space=pltpu.HBM)
    units = 4 * wide
    mixed, expert = pl.pallas_call(
        functools.partial(fused_kernel, steps),
        out_shape=(
            jax.ShapeDtypeStruct((length // lanes, width), kind),
            jax.ShapeDtypeStruct((count, width), kind),
        ),
        in_specs=[anywhere] * 15,
        out_specs=(anywhere, anywhere),
        scratch_shapes=[
            pltpu.VMEM((2, count), jnp.int32),
            pltpu.VMEM((2, count), jnp.float32),
            pltpu.VMEM((1, width), jnp.float32),
            pltpu.VMEM((1, dim), jnp.float32),
            pltpu.VMEM((1, dim), jnp.float32),
            pltpu.VMEM((length // lanes, width), kind),
            pltpu.VMEM((count, width), kind),
            pltpu.VMEM((4, count, count), kind),
            pltpu.VMEM((width, hidden), kind),
            pltpu.VMEM((width, hidden), kind),
            pltpu.VMEM((hidden, width), kind),
            pltpu.VMEM(out_proj.shape, kind),
            pltpu.VMEM(query_rows.shape, kind),
            pltpu.VMEM((length, dim), kind),
            pltpu.VMEM((length, dim), jnp.float32),
            pltpu.VMEM((length, dim), jnp.float32),
            pltpu.VMEM((count, width), kind),
            pltpu.VMEM((count, width), kind),
            pltpu.VMEM((blocks, size, width), kind),
            pltpu.VMEM((size * (wide - 1), 128), jnp.float32),
            pltpu.VMEM((2, size * (wide - 1), 128), jnp.float32),
            pltpu.VMEM((size, 128), jnp.float32),
            pltpu.VMEM((size, 128), jnp.float32),
            pltpu.VMEM((2, size, width), kind),
            pltpu.VMEM((2, size, width), kind),
            pltpu.VMEM((size, width), jnp.float32),
            pltpu.VMEM((blocks, 4, size, width), kind),
            pltpu.VMEM((wide, 4, size, width), kind),
            pltpu.VMEM((2, blocks, 4, size, width), kind),
            pltpu.VMEM((4 * size, hidden), kind),
            pltpu.VMEM((units, 4, size, width), kind),
            pltpu.VMEM((units, 2, size, width), kind),
            pltpu.VMEM((units, size, width), kind),
            pltpu.VMEM((units, size, width), kind),
            pltpu.VMEM((units, size, width), kind),
            pltpu.VMEM((2, wide, size, width), kind),
            pltpu.VMEM((2, wide - 1, size, width), kind),
            pltpu.VMEM((wide, size, width), kind),
            pltpu.VMEM((wide, size, width), kind),
            pltpu.VMEM((blocks, size, width), kind),
            pltpu.VMEM((count, count), jnp.float32),
            pltpu.VMEM((steps, 2, length, dim), kind),
            pltpu.VMEM(query_rows.shape, kind),
            pltpu.VMEM((lanes, length // lanes, width), kind),
            pltpu.VMEM((2, length // lanes, width), kind),
            pltpu.VMEM((length // lanes, width), kind),
            pltpu.VMEM((length // lanes, width), kind),
            pltpu.SemaphoreType.DMA((14 + blocks,)),
            pltpu.SemaphoreType.DMA((1 + width // math.gcd(width, 512),)),
        ]
        + [
            pltpu.SemaphoreType.DMA((n,))
            for n in (1, 2 * wide, 1, 2 * blocks, 1, 1)
            + (1, blocks + 2 * wide)
            + (1, units) * 3
            + (1, wide, 1, 2 * wide, 1, blocks)
            + (1, 2, 2, 2, 3, 3, 2, 3)
        ],
        compiler_params=pltpu.CompilerParams(
            collective_id=0, has_side_effects=True, vmem_limit_bytes=VMEM_LIMIT
        ),
    )(
        mix_tokens,
        expert_ids.T,
        expert_score.T,
        norm_gain.reshape(1, width),
        gate_proj.reshape(gate_proj.shape[1:]),
        up_proj.reshape(up_proj.shape[1:]),
        down_proj.reshape(down_proj.shape[1:]),
        out_proj,
        query_rows,
        projected_keys,
        projected_values,
        query_gain.reshape(1, dim),
        key_norm_gain.reshape(1, dim),
        cosine,
        sine,
    )
    return pl.pallas_call(
        deliver_kernel,
        out_shape=(
            jax.ShapeDtypeStruct(mixed.shape, kind),
            jax.ShapeDtypeStruct(expert.shape, kind),
        ),
        in_specs=[anywhere] * 2,
        out_specs=(anywhere, anywhere),
        scratch_shapes=[
            pltpu.VMEM(mixed.shape, kind),
            pltpu.VMEM(expert.shape, kind),
            pltpu.SemaphoreType.DMA((2, 2)),
        ],
    )(mixed, expert)


def fits_fused(query_rows, projected_keys, query_gain, mix_tokens, expert_ids, gate_proj):
    steps, lanes = lax.axis_size("ep"), lax.axis_size("tp")
    count, width = mix_tokens.shape
    length, dim = projected_keys.shape
    local_experts, _, hidden = gate_proj.shape
    cap = count * expert_ids.shape[1] * 3 // (2 * steps)
    blocks = 20 * steps * cap * width * 2 + 4 * width * hidden * 2
    return (
        lanes == 4
        and steps == 4
        and local_experts == 1
        and expert_ids.shape[1] == 2
        and dim == query_gain.shape[0]
        and dim % 128 == 0
        and length % 64 == 0
        and length <= 256
        and count == 128
        and cap < count
        and (count - cap) % 16 == 0
        and cap % (count - cap) == 0
        and 2 * cap > count
        and blocks < 48 * 1024 * 1024
    )


def local(
    query_rows,
    projected_keys,
    projected_values,
    query_gain,
    key_norm_gain,
    out_proj,
    mix_tokens,
    norm_gain,
    expert_ids,
    expert_score,
    gate_proj,
    up_proj,
    down_proj,
):
    simple = fits_fused(
        query_rows, projected_keys, query_gain, mix_tokens, expert_ids, gate_proj
    )
    return (fused if simple else plain_halves)(
        query_rows,
        projected_keys,
        projected_values,
        query_gain,
        key_norm_gain,
        out_proj,
        mix_tokens,
        norm_gain,
        expert_ids,
        expert_score,
        gate_proj,
        up_proj,
        down_proj,
    )


def solution(mesh):
    in_specs = (
        P(("grp", "ep"), "tp"),
        P(("grp", "ep"), "tp"),
        P(("grp", "ep"), "tp"),
        P(),
        P(),
        P("tp", None),
        P(("grp", "ep", "tp"), None),
        P(),
        P(("grp", "ep", "tp"), None),
        P(("grp", "ep", "tp"), None),
        P("ep", None, "tp"),
        P("ep", None, "tp"),
        P("ep", "tp", None),
    )
    out_specs = (P(("grp", "ep", "tp"), None), P(("grp", "ep", "tp"), None))
    return jax.shard_map(local, mesh=mesh, in_specs=in_specs, out_specs=out_specs, check_vma=False)
```
